256 devices in a mesh: sp: 32 (over z, x), tp: 8 (over y, core).
Axes of the slice: x: 4, y: 4, z: 8, core: 2. Of those that a mesh axis runs over, the one named last changes fastest.
Arguments:
- upstream: bfloat16 [8192, 2048], P('sp'), may hold values from -6 to 6
- stream: bfloat16 [8192, 2048], P('sp'), may hold values from -10 to 10
- routes: int32 [8192, 2], P('sp'), may hold values from 0 to 31, all different within a row; in each aligned block of 256 rows (0 to 255, 256 to 511, ...) at most 32 rows name the same one
- route_weights: float32 [8192, 2], P('sp'), may hold values from 0.1 to 1
- glu_value: bfloat16 [8192, 512], P('sp', 'tp'), may hold values from -6 to 6
- glu_gate: bfloat16 [8192, 512], P('sp', 'tp'), may hold values from -10 to 10
- conv_taps: float32 [31, 512], P(None, 'tp'), may hold values from -1 to 1
- conv_saved: bfloat16 [8192, 512], P('sp', 'tp'), may hold values from -600 to 600
- out_proj: bfloat16 [2048, 512], P(None, 'tp'), may hold values from -0.25 to 0.25
- expert_gate: bfloat16 [32, 2048, 2048], P('sp', None, 'tp'), may hold values from -0.125 to 0.125
- expert_up: bfloat16 [32, 2048, 2048], P('sp', None, 'tp'), may hold values from -0.125 to 0.125
- expert_down: bfloat16 [32, 2048, 2048], P('sp', 'tp'), may hold values from -0.125 to 0.125
Outputs:
- grad_stream: bfloat16 [8192, 2048], P('sp', 'tp')
- grad_value: bfloat16 [8192, 512], P('sp', 'tp')
- grad_gate: bfloat16 [8192, 512], P('sp', 'tp')
- grad_out_proj: float32 [2048, 512], P('sp', 'tp')
- grad_expert_gate: float32 [32, 2048, 2048], P('sp', None, 'tp')
- grad_expert_up: float32 [32, 2048, 2048], P('sp', None, 'tp')
- grad_expert_down: float32 [32, 2048, 2048], P('sp', 'tp')
The draws below stay inside these ranges and needn't reach their ends.
Inputs may be any that keep to these rules, and one draw needn't show every extreme that they name: `routes`: each row names 2 different experts; among the 256 rows of one index of sp no expert is named more than 32 times, a bound that some block reaches.
All inputs are finite; a program needn't handle non-finite values.
Results may differ from the reference program's by a relative error of at most 0.014.
Values may be sent and summed in bfloat16 or wider, within the bound.
A program may use at most 128 MiB of HBM per device.

```python
import math
from functools import partial
import jax
import jax.numpy as jnp
import numpy as np
from jax import lax

D = 2048
FF = 2048
CW = 512
KW = 31
TOPK = 2
TOK_DEV = 256
TOKENS = 8192
EXPERTS = 32
CAP = 32
N_SP = 32
N_TP = 8


def draw_conv_saved(key, part):
    key_values, key_rows = jax.random.split(key, 2)
    column_scale = 10.0 ** (jnp.arange(CW, dtype=jnp.float32) / CW)
    values = jnp.clip(jax.random.normal(key_values, (TOKENS, CW), jnp.float32), -4.0, 4.0)
    row_scale = jnp.exp(jax.random.uniform(key_rows, (TOKENS, 1), jnp.float32, 0.0, math.log(10.0)))
    result = values * column_scale[None, :] * row_scale
    return result.astype(jnp.bfloat16)


def raised(drawn, key, source, target, shards_of, factor):
    def block_of(axis_at):
        return (jnp.arange(drawn.shape[axis_at]) // (drawn.shape[axis_at] // shards_of)).reshape((-1,) + (1,) * (drawn.ndim - 1 - axis_at))

    first = jax.random.permutation(key, shards_of)[block_of(target)]
    other_side = (block_of(target) + shards_of // 2) % shards_of
    return jnp.where((block_of(source) == first) | (block_of(source) == other_side), factor * drawn, drawn)


def block_scale(stream_key, shape, pieces, least, largest):
    factor_of, own = 1.0, jax.random.fold_in(stream_key, 6)
    for dim, parts in pieces:
        heights = jnp.exp(jax.random.uniform(jax.random.fold_in(own, dim), (parts,), jnp.float32, least / len(pieces), largest / len(pieces)))
        factor_of = factor_of * jnp.repeat(heights, shape[dim] // parts).reshape([-1 if axis == dim else 1 for axis in range(len(shape))])
    return factor_of


def routed_block(stream_key, own, number, rows, count, top, reach, skew):
    order = jax.random.permutation(stream_key, count)
    packed, usual = load_shares(count, rows * top, reach, skew, True), load_shares(count, rows * top, reach, skew, False)
    places = jnp.arange(count)

    def named(sizes, offset_by):
        used = int((sizes > 0).sum())
        fixed = max(1, used // 4)
        moved = fixed + (places - fixed + offset_by * (used - fixed)) % max(1, count - fixed)
        return jnp.zeros((count,), jnp.int32).at[order[jnp.where(places < fixed, places, moved)]].set(jnp.asarray(sizes, jnp.int32))

    sizes = jnp.where(number % 4 == 0, named(packed, number // 4), named(usual, number - number // 4 - 1))
    mixed = jax.random.permutation(jax.random.fold_in(own, 3), count)
    source_of, receiver = mixed[0:count // 2 * 2:2], mixed[1:count // 2 * 2:2]
    slack = jnp.minimum(sizes[source_of] - 1, reach - sizes[receiver]) // 2
    slack = jnp.where((source_of == order[0]) | (receiver == order[0]) | (sizes[receiver] == 0), 0, jnp.maximum(slack, 0))
    moved = jax.random.randint(jax.random.fold_in(own, 4), (count // 2,), 0, 1 << 20) % (slack + 1)
    sizes = sizes.at[source_of].add(-moved).at[receiver].add(moved)
    items = jnp.searchsorted(jnp.cumsum(sizes), jnp.arange(rows * top), side="right").astype(jnp.int32)
    table = items.reshape(top, rows).T
    table = table[jax.random.permutation(jax.random.fold_in(own, 1), rows)]
    offset_by = jax.random.randint(jax.random.fold_in(own, 2), (rows, 1), 0, top)
    return jnp.take_along_axis(table, (jnp.arange(top)[None, :] + offset_by) % top, axis=1)


def load_shares(amount, total, most, lean, full):
    loads = [(1 << 20) // math.isqrt(standing ** lean) + 1 for standing in range(1, amount + 1)]
    largest = most if full else min(most, max(-(-total // amount), total * loads[0] // sum(loads)))
    least = 1 if total - largest >= amount - 1 else 0
    given, surplus = [largest] + [least] * (amount - 1), total - largest - least * (amount - 1)
    while surplus > 0:
        free = [i for i in range(1, amount) if given[i] < largest] or [i for i in range(1, amount) if given[i] < most]
        mass, left = sum([loads[i] for i in free]), surplus
        for i in free:
            more = min(most - given[i], max(1, left * loads[i] // mass), surplus)
            given[i] = given[i] + more
            surplus = surplus - more
    return np.array(given)


def bell_draw(rng, extent, deviation, limit, cuts=(), kind=jnp.bfloat16):
    entries = jax.random.normal(rng, extent, jnp.float32) * deviation
    if len(cuts) > 0:
        entries = block_scale(rng, extent, cuts, -0.22, 0.18) * entries
    return jnp.clip(entries, min=-limit, max=limit).astype(kind)


def heavy_noise(stream_key, shape, scale, most, cuts, heavy, kind=jnp.bfloat16):
    array = scale * jax.random.normal(stream_key, shape, jnp.float32)
    if cuts:
        array = array * block_scale(stream_key, shape, cuts, -0.22, 0.18)
    return jnp.clip(raised(array, jax.random.fold_in(stream_key, 3), *heavy), -most, most).astype(kind)


def setup_inputs(seed: int = 0) -> dict:
    seeds = jax.random.split(jax.random.key(seed), 13)
    upstream = heavy_noise(seeds[0], (TOKENS, D), 1.0, 6.0, ((0, 32),), (0, 1, 32, 2.75))
    stream = bell_draw(seeds[1], (TOKENS, D), 1.0, 10.0, ((0, 32),))
    routes_keys = jax.random.split(jax.random.fold_in(seeds[2], 1), TOKENS // TOK_DEV)
    routes_turns = jax.random.permutation(jax.random.fold_in(seeds[2], 3), TOKENS // TOK_DEV)
    routes = jax.vmap(lambda own, number: routed_block(jax.random.fold_in(seeds[2], 2), own, number, TOK_DEV, EXPERTS, TOPK, CAP, 2))(routes_keys, routes_turns).reshape((TOKENS, TOPK))
    route_weights = jnp.clip(0.1 + 0.9 * jax.random.uniform(seeds[3], (TOKENS, TOPK), jnp.float32) ** block_scale(seeds[3], (TOKENS, TOPK), ((0, 32),), -0.2, 0.2), 0.1, 1.0)
    glu_value = bell_draw(seeds[4], (TOKENS, CW), 1.0, 6.0, ((0, 32), (1, 8)))
    glu_gate = bell_draw(seeds[5], (TOKENS, CW), 2.0, 10.0, ((0, 32), (1, 8)))
    conv_taps = bell_draw(seeds[6], (KW, CW), KW ** -0.5, 1.0, ((1, 8),), jnp.float32)
    conv_saved = draw_conv_saved(jax.random.fold_in(seeds[12], 71), 0)
    out_proj = bell_draw(seeds[8], (D, CW), CW ** -0.5, 0.25, ((1, 8),))
    expert_gate = bell_draw(seeds[9], (EXPERTS, D, FF), D ** -0.5, 0.125, ((0, 32), (2, 8)))
    expert_up = bell_draw(seeds[10], (EXPERTS, D, FF), D ** -0.5, 0.125, ((0, 32), (2, 8)))
    expert_down = bell_draw(seeds[11], (EXPERTS, FF, D), FF ** -0.5, 0.125, ((0, 32), (1, 8)))
    return {"upstream": upstream, "stream": stream, "routes": routes, "route_weights": route_weights, "glu_value": glu_value, "glu_gate": glu_gate, "conv_taps": conv_taps, "conv_saved": conv_saved, "out_proj": out_proj, "expert_gate": expert_gate, "expert_up": expert_up, "expert_down": expert_down}


clamp_limit = 7.0
glu_alpha = 1.702
norm_eps = 1e-05

def contract_rows(left, right):
    return lax.dot_general(left, right, (((0,), (0,)), ((), ())), preferred_element_type=jnp.float32)

def times_transposed(left, right):
    return lax.dot_general(left, right, (((1,), (1,)), ((), ())), preferred_element_type=jnp.float32)

def block_slots(block_routes, expert_count, capacity):
    flat_routes = block_routes.reshape(-1).astype(jnp.int32)
    one_hot = (flat_routes[:, None] == jnp.arange(expert_count, dtype=jnp.int32)[None, :]).astype(jnp.int32)
    earlier = jnp.cumsum(one_hot, axis=0) - one_hot
    slot_index = lax.optimization_barrier(jnp.sum(earlier * one_hot, axis=1)).astype(jnp.int32)
    target = (flat_routes * capacity + slot_index).astype(jnp.int32)
    pair_count = flat_routes.shape[0]
    table = jnp.full((expert_count * capacity,), pair_count, jnp.int32).at[target].set(jnp.arange(pair_count, dtype=jnp.int32))
    return (target, table)

def gather_pairs(table, block_stream, block_upstream, block_weights, topk):
    token_of = table // topk
    zero_row = jnp.zeros((1, block_stream.shape[1]), jnp.bfloat16)
    stream_pad = jnp.concatenate([block_stream, zero_row], axis=0)
    upstream_pad = jnp.concatenate([block_upstream, zero_row], axis=0)
    weight_pad = jnp.concatenate([block_weights.reshape(-1), jnp.zeros((1,), jnp.float32)])
    send_rows = stream_pad[token_of]
    send_cot = (weight_pad[table][:, None] * upstream_pad[token_of].astype(jnp.float32)).astype(jnp.bfloat16)
    return (send_rows, send_cot)

def expert_backward(expert_rows, expert_cot, gate_weight, up_weight, down_weight):
    gate_pre = jnp.dot(expert_rows, gate_weight, preferred_element_type=jnp.float32)
    up_pre = jnp.dot(expert_rows, up_weight, preferred_element_type=jnp.float32)
    capped = jnp.minimum(gate_pre, clamp_limit)
    clipped = jnp.clip(up_pre, -clamp_limit, clamp_limit)
    gate_sigmoid = jax.nn.sigmoid(glu_alpha * capped)
    act = (capped * gate_sigmoid * (clipped + 1.0)).astype(jnp.bfloat16)
    grad_down = contract_rows(act, expert_cot)
    grad_act = times_transposed(expert_cot, down_weight)
    slope = gate_sigmoid + glu_alpha * capped * gate_sigmoid * (1.0 - gate_sigmoid)
    grad_gate_pre = jnp.where(gate_pre < clamp_limit, grad_act * (clipped + 1.0) * slope, 0.0).astype(jnp.bfloat16)
    grad_up_pre = jnp.where(jnp.abs(up_pre) < clamp_limit, grad_act * capped * gate_sigmoid, 0.0).astype(jnp.bfloat16)
    grad_gate = contract_rows(expert_rows, grad_gate_pre)
    grad_up = contract_rows(expert_rows, grad_up_pre)
    return (grad_gate, grad_up, grad_down, grad_gate_pre, grad_up_pre)

def one_expert(operands):
    expert_rows, expert_cot, gate_weight, up_weight, down_weight = operands
    grad_gate, grad_up, grad_down, grad_gate_pre, grad_up_pre = expert_backward(expert_rows, expert_cot, gate_weight, up_weight, down_weight)
    group_width = FF // N_TP
    gate_groups = grad_gate_pre.astype(jnp.float32).reshape(-1, N_TP, group_width)
    up_groups = grad_up_pre.astype(jnp.float32).reshape(-1, N_TP, group_width)
    gate_split = gate_weight.astype(jnp.float32).reshape(D, N_TP, group_width)
    up_split = up_weight.astype(jnp.float32).reshape(D, N_TP, group_width)
    partial_rows = jnp.einsum('rgf,dgf->grd', gate_groups, gate_split) + jnp.einsum('rgf,dgf->grd', up_groups, up_split)
    rounded = lax.optimization_barrier(partial_rows.astype(jnp.bfloat16))
    row_grad = lax.optimization_barrier(jnp.sum(rounded.astype(jnp.float32), axis=0)).astype(jnp.bfloat16)
    return (grad_gate, grad_up, grad_down, row_grad)

def take_rows(source_rows, target_rows):
    return source_rows[target_rows]

def reference(upstream, stream, routes, route_weights, glu_value, glu_gate, conv_taps, conv_saved, out_proj, expert_gate, expert_up, expert_down):
    block_routes = routes.reshape(N_SP, TOK_DEV, TOPK)
    targets, tables = jax.vmap(partial(block_slots, expert_count=EXPERTS, capacity=CAP))(block_routes)
    send_rows, send_cot = jax.vmap(partial(gather_pairs, topk=TOPK))(tables, stream.reshape(N_SP, TOK_DEV, D), upstream.reshape(N_SP, TOK_DEV, D), route_weights.reshape(N_SP, TOK_DEV, TOPK))
    expert_rows = send_rows.reshape(N_SP, EXPERTS, CAP, D).transpose(1, 0, 2, 3).reshape(EXPERTS, N_SP * CAP, D)
    expert_cot = send_cot.reshape(N_SP, EXPERTS, CAP, D).transpose(1, 0, 2, 3).reshape(EXPERTS, N_SP * CAP, D)
    grad_expert_gate, grad_expert_up, grad_expert_down, row_grads = lax.map(one_expert, (expert_rows, expert_cot, expert_gate, expert_up, expert_down))
    returned = row_grads.reshape(EXPERTS, N_SP, CAP, D).transpose(1, 0, 2, 3).reshape(N_SP, EXPERTS * CAP, D)
    pair_grads = jax.vmap(take_rows)(returned, targets)
    routed_sum = lax.optimization_barrier(jnp.sum(pair_grads.astype(jnp.float32).reshape(TOKENS, TOPK, D), axis=1))
    grad_stream = (upstream.astype(jnp.float32) + routed_sum).astype(jnp.bfloat16)
    saved_conv = conv_saved.astype(jnp.float32)
    mean_c = lax.optimization_barrier(jnp.mean(saved_conv, axis=1, keepdims=True))
    var_c = lax.optimization_barrier(jnp.mean(saved_conv * saved_conv, axis=1, keepdims=True)) - mean_c * mean_c
    inv_std = lax.rsqrt(var_c + norm_eps)
    normed = (saved_conv - mean_c) * inv_std
    norm_sigmoid = jax.nn.sigmoid(normed)
    mixed = (normed * norm_sigmoid).astype(jnp.bfloat16)
    grad_mixed = jnp.dot(grad_stream, out_proj, preferred_element_type=jnp.float32)
    grad_normed = grad_mixed * norm_sigmoid * (1.0 + normed * (1.0 - norm_sigmoid))
    first_mean = lax.optimization_barrier(jnp.mean(grad_normed, axis=1, keepdims=True))
    second_mean = lax.optimization_barrier(jnp.mean(grad_normed * normed, axis=1, keepdims=True))
    grad_conv = inv_std * (grad_normed - first_mean - normed * second_mean)
    padded = jnp.concatenate([grad_conv, jnp.zeros((KW - 1, CW), jnp.float32)], axis=0)
    grad_glu = jnp.zeros((TOKENS, CW), jnp.float32)
    for offset in range(KW):
        grad_glu = grad_glu + conv_taps[offset][None, :] * padded[offset:offset + TOKENS]
    gate_sig = jax.nn.sigmoid(glu_gate.astype(jnp.float32))
    grad_value = (grad_glu * gate_sig).astype(jnp.bfloat16)
    grad_gate = (grad_glu * glu_value.astype(jnp.float32) * gate_sig * (1.0 - gate_sig)).astype(jnp.bfloat16)
    grad_out_proj = contract_rows(grad_stream, mixed)
    return (grad_stream, grad_value, grad_gate, grad_out_proj, grad_expert_gate, grad_expert_up, grad_expert_down)
```

```python
import functools

import jax
import jax.numpy as jnp
from jax import lax
from jax.experimental import pallas as pl
from jax.experimental.pallas import tpu as pltpu
from jax.sharding import PartitionSpec as P

MESH = pl.DeviceIdType.MESH
BF16 = jnp.bfloat16
F32 = jnp.float32

CW = 512
NZ, NX, NY = 8, 4, 4
N_SP = 32
N_TP = 8
CAP = 32
TOK = 256
SL = 256
NC = 4
PER = N_SP // NC
ROWS = PER * CAP
HALF = ROWS // 2

clamp_limit = 7.0
glu_alpha = 1.702
norm_eps = 1e-05

DZ = (1, 7, 2, 6, 3, 5, 4, 0)
OWN = 28


def position_of(expert, z, x):
    dz = ((expert >> 2) - z) & 7
    dx = ((expert & 3) - x) & 3
    h = jnp.minimum(dz, 8 - dz)
    q = jnp.where(dz == 0, 7, jnp.where(dz == 4, 6, 2 * (h - 1) + jnp.where(dz > 4, 1, 0)))
    return 4 * q + dx


def dot_tn(left, right):
    return lax.dot_general(left, right, (((0,), (0,)), ((), ())), preferred_element_type=F32)


def dot_nt(left, right):
    return lax.dot_general(left, right, (((1,), (1,)), ((), ())), preferred_element_type=F32)


def dot_nn(left, right):
    return lax.dot_general(left, right, (((1,), (0,)), ((), ())), preferred_element_type=F32)


def main_kernel(
    up_hbm, st_hbm, routes_ref, weights_ref, wg_hbm, wu_hbm, wd_hbm,
    gs_ref, gg_hbm, gu_hbm, gd_hbm,
    up_v, st_v, wg, wu, wd, send, xs, onehot, part, part_in, comb, ring_in, relay, row_out, ret,
    acc_pre, ggp, gup, act_t, acc_g, acc_u, acc_d,
    load_sem, out_sem, a_snd, a_rcv, g_snd, g_rcv, r_snd, r_rcv, b_snd, b_rcv,
):
    sp = lax.axis_index("sp")
    tp = lax.axis_index("tp")
    z, x = sp // NX, sp % NX
    y, c = tp // 2, tp % 2
    fwd, bwd = ((y + 1) % NY) * 2 + c, ((y + 3) % NY) * 2 + c
    opp = ((y + 2) % NY) * 2 + c
    other = y * 2 + (1 - c)
    up_dev, down_dev, mate = (sp, fwd), (sp, bwd), (sp, other)
    oc = 1 - c
    fwd_o, bwd_o, opp_o = ((y + 1) % NY) * 2 + oc, ((y + 3) % NY) * 2 + oc, ((y + 2) % NY) * 2 + oc

    def sp_dev(p, sign):
        dz, dx = DZ[p // 4], p % 4
        if sign < 0:
            dz, dx = (NZ - dz) % NZ, (NX - dx) % NX
        return (((z + dz) % NZ) * NX + (x + dx) % NX, tp)

    column = pl.multiple_of(tp * SL, SL)
    loads = [
        pltpu.make_async_copy(st_hbm.at[:, pl.ds(column, SL)], st_v, load_sem.at[0]),
        pltpu.make_async_copy(up_hbm.at[:, pl.ds(column, SL)], up_v, load_sem.at[1]),
        pltpu.make_async_copy(wg_hbm, wg, load_sem.at[2]),
        pltpu.make_async_copy(wu_hbm, wu, load_sem.at[3]),
    ]
    for j in range(N_TP):
        loads.append(
            pltpu.make_async_copy(wd_hbm.at[:, pl.ds(j * SL, SL)], wd.at[j], load_sem.at[4 + j])
        )
    for copy in loads:
        copy.start()

    barrier = pltpu.get_barrier_semaphore()
    for p in range(N_SP):
        if p != OWN:
            pl.semaphore_signal(barrier, inc=1, device_id=sp_dev(p, 1), device_id_type=MESH)
    for dev in (up_dev, down_dev, mate):
        pl.semaphore_signal(barrier, inc=1, device_id=dev, device_id_type=MESH)

    r0, r1 = routes_ref[:, 0:1], routes_ref[:, 1:2]
    experts = lax.broadcasted_iota(jnp.int32, (TOK, N_SP), 1)
    c0 = jnp.where(r0 == experts, 1.0, 0.0).astype(F32)
    c1 = jnp.where(r1 == experts, 1.0, 0.0).astype(F32)
    tri = jnp.where(
        lax.broadcasted_iota(jnp.int32, (TOK, TOK), 1) < lax.broadcasted_iota(jnp.int32, (TOK, TOK), 0),
        1.0, 0.0,
    ).astype(BF16)
    earlier = dot_nn(tri, (c0 + c1).astype(BF16))
    slot0 = jnp.sum(earlier * c0, axis=1, keepdims=True).astype(jnp.int32)
    slot1 = jnp.sum(earlier * c1, axis=1, keepdims=True).astype(jnp.int32)
    pos0 = position_of(r0, z, x) * CAP + slot0
    pos1 = position_of(r1, z, x) * CAP + slot1
    loads[0].wait()
    loads[1].wait()
    stream = st_v[...]
    ups = up_v[...].astype(F32)
    cot0 = (weights_ref[:, 0:1] * ups).astype(BF16)
    cot1 = (weights_ref[:, 1:2] * ups).astype(BF16)
    lanes = lax.broadcasted_iota(jnp.int32, (TOK, ROWS), 1)

    def a2a(p):
        return pltpu.make_async_remote_copy(
            src_ref=send.at[p],
            dst_ref=xs.at[:, tp, pl.ds(p * CAP, CAP), :],
            send_sem=a_snd.at[p],
            recv_sem=a_rcv.at[p],
            device_id=sp_dev(p, 1),
            device_id_type=MESH,
        )

    for k in range(NC):
        s0 = jnp.where(pos0 - k * ROWS == lanes, 1.0, 0.0).astype(BF16)
        s1 = jnp.where(pos1 - k * ROWS == lanes, 1.0, 0.0).astype(BF16)
        both = s0 + s1
        onehot[k] = both
        rows = dot_tn(both, stream).astype(BF16)
        cots = (dot_tn(s0, cot0) + dot_tn(s1, cot1)).astype(BF16)
        send[k * PER:(k + 1) * PER, 0] = rows.reshape(PER, CAP, SL)
        send[k * PER:(k + 1) * PER, 1] = cots.reshape(PER, CAP, SL)
        if k == 0:
            pl.semaphore_wait(barrier, N_SP - 1 + 3)
        for p in range(k * PER, (k + 1) * PER):
            if p == OWN:
                xs[:, tp, pl.ds(p * CAP, CAP), :] = send[p]
            else:
                a2a(p).start()

    def gather(k, kind, rc, slice_at, dev):
        ref = xs.at[rc, slice_at, pl.ds(k * ROWS, ROWS), :]
        return pltpu.make_async_remote_copy(
            src_ref=ref, dst_ref=ref, send_sem=g_snd.at[k, kind], recv_sem=g_rcv.at[k, kind],
            device_id=dev, device_id_type=MESH,
        )

    plan = (
        (0, tp, up_dev), (0, tp, down_dev), (0, tp, mate),
        (1, tp, up_dev), (1, tp, down_dev), (1, tp, mate),
        (0, bwd, up_dev), (1, fwd, down_dev),
        (0, bwd, mate), (0, fwd, mate), (0, opp, mate),
        (1, fwd, mate), (1, bwd, mate), (1, opp, mate),
    )

    def spread(k, kind):
        rc, slice_at, dev = plan[kind]
        return gather(k, kind, rc, slice_at, dev)

    arrives = (bwd, fwd, other, bwd, fwd, other, opp, opp, bwd_o, fwd_o, opp_o, fwd_o, bwd_o, opp_o)
    arrives_rc = (0, 0, 0, 1, 1, 1, 0, 1, 0, 0, 0, 1, 1, 1)

    def got(k, kind):
        gather(k, kind, arrives_rc[kind], arrives[kind], mate).wait_recv()

    def stage_a(k):
        for p in range(k * PER, (k + 1) * PER):
            if p != OWN:
                a2a(p).wait_recv()
        for kind in (0, 4, 3, 1, 2, 5):
            spread(k, kind).start()

    def stage_b1(k):
        got(k, 0)
        spread(k, 6).start()
        got(k, 4)
        spread(k, 7).start()
        spread(k, 8).start()
        spread(k, 11).start()

    def stage_b2(k):
        got(k, 1)
        spread(k, 9).start()
        got(k, 3)
        spread(k, 12).start()
        got(k, 6)
        spread(k, 10).start()
        got(k, 7)
        spread(k, 13).start()

    def stage_b3(k):
        for kind in (2, 5, 8, 11, 9, 12, 10, 13):
            got(k, kind)

    def swap(k):
        return pltpu.make_async_remote_copy(
            src_ref=part.at[k, 1 - c], dst_ref=part_in.at[k],
            send_sem=r_snd.at[k, 0], recv_sem=r_rcv.at[k, 0], device_id=mate, device_id_type=MESH,
        )

    def stage_c(k):
        rows = pl.ds(k * ROWS, ROWS)
        acc_pre[...] = jnp.zeros_like(acc_pre)

        def pre(j, carry):
            r = xs[0, j, rows, :]
            acc_pre[0] += dot_nn(r, wg[j])
            acc_pre[1] += dot_nn(r, wu[j])
            acc_pre[2] += dot_nt(xs[1, j, rows, :], wd[j])
            return carry

        lax.fori_loop(0, N_TP, pre, 0)
        gate_pre, up_pre, grad_act = acc_pre[0], acc_pre[1], acc_pre[2]
        capped = jnp.minimum(gate_pre, clamp_limit)
        clipped = jnp.clip(up_pre, -clamp_limit, clamp_limit)
        sig = jax.nn.sigmoid(glu_alpha * capped)
        act = (capped * sig * (clipped + 1.0)).astype(BF16)
        slope = sig + glu_alpha * capped * sig * (1.0 - sig)
        g_gate = jnp.where(gate_pre < clamp_limit, grad_act * (clipped + 1.0) * slope, 0.0).astype(BF16)
        g_up = jnp.where(jnp.abs(up_pre) < clamp_limit, grad_act * capped * sig, 0.0).astype(BF16)
        act_t[k] = act
        ggp[k] = g_gate
        gup[k] = g_up

        def back(j, carry):
            total = dot_nt(ggp[k], wg[j]) + dot_nt(gup[k], wu[j])
            part[k, j % 2, j // 2] = total.astype(BF16)
            return carry

        lax.fori_loop(0, N_TP, back, 0)
        swap(k).start()

    def stage_w(k):
        rows = pl.ds(k * ROWS, ROWS)

        def grads(j, carry):
            r = xs[0, j, rows, :]
            g, u, d = dot_tn(r, ggp[k]), dot_tn(r, gup[k]), dot_tn(act_t[k], xs[1, j, rows, :])
            if k == 0:
                acc_g[j], acc_u[j], acc_d[j] = g, u, d
            else:
                acc_g[j] += g
                acc_u[j] += u
                acc_d[j] += d
            return carry

        lax.fori_loop(0, N_TP, grads, 0)

    lo, hi = pl.ds(0, HALF), pl.ds(HALF, HALF)

    def ring(k, kind, src, slot, dev):
        return pltpu.make_async_remote_copy(
            src_ref=src, dst_ref=ring_in.at[k, slot],
            send_sem=r_snd.at[k, kind], recv_sem=r_rcv.at[k, kind], device_id=dev, device_id_type=MESH,
        )

    def rings(k, kind):
        if kind == 0:
            return swap(k)
        if kind == 1:
            return ring(k, 1, comb.at[k, 2, lo, :], 0, down_dev)
        if kind == 2:
            return ring(k, 2, comb.at[k, 2, hi, :], 1, up_dev)
        if kind == 3:
            return ring(k, 3, comb.at[k, 1, lo, :], 2, up_dev)
        if kind == 4:
            return ring(k, 4, comb.at[k, 3, hi, :], 3, down_dev)
        if kind == 5:
            return ring(k, 5, relay.at[k, 0], 4, down_dev)
        return ring(k, 6, relay.at[k, 1], 5, up_dev)

    def stage_d(k):
        rings(k, 0).wait_recv()
        for r in (2, 1, 3, 0):
            at = (y + r) % NY
            comb[k, r] = (part[k, c, at].astype(F32) + part_in[k, at].astype(F32)).astype(BF16)
            if r == 2:
                rings(k, 1).start()
                rings(k, 2).start()
        rings(k, 3).start()
        rings(k, 4).start()

    def stage_e1(k):
        rings(k, 1).wait_recv()
        relay[k, 0] = (ring_in[k, 0].astype(F32) + comb[k, 3, lo, :].astype(F32)).astype(BF16)
        rings(k, 5).start()
        rings(k, 2).wait_recv()
        relay[k, 1] = (ring_in[k, 1].astype(F32) + comb[k, 1, hi, :].astype(F32)).astype(BF16)
        rings(k, 6).start()

    def back_copy(p):
        return pltpu.make_async_remote_copy(
            src_ref=row_out.at[p], dst_ref=ret.at[p],
            send_sem=b_snd.at[p], recv_sem=b_rcv.at[p], device_id=sp_dev(p, -1), device_id_type=MESH,
        )

    def stage_e2(k):
        for kind in (3, 4, 5, 6):
            rings(k, kind).wait_recv()
        low = comb[k, 0, lo, :].astype(F32) + ring_in[k, 2].astype(F32) + ring_in[k, 4].astype(F32)
        high = comb[k, 0, hi, :].astype(F32) + ring_in[k, 3].astype(F32) + ring_in[k, 5].astype(F32)
        at = k * PER
        row_out[at:at + PER // 2] = low.astype(BF16).reshape(PER // 2, CAP, SL)
        row_out[at + PER // 2:at + PER] = high.astype(BF16).reshape(PER // 2, CAP, SL)
        for p in range(at, at + PER):
            if p == OWN:
                ret[p] = row_out[p]
            else:
                back_copy(p).start()

    stage_a(0)
    stage_b1(0)
    stage_a(1)
    stage_b2(0)
    for copy in loads[2:]:
        copy.wait()
    stage_b3(0)
    stage_c(0)
    stage_b1(1)
    stage_a(2)
    stage_d(0)
    stage_b2(1)
    stage_b3(1)
    stage_c(1)
    stage_e1(0)
    stage_b1(2)
    stage_a(3)
    stage_d(1)
    stage_w(0)
    stage_e2(0)
    stage_b2(2)
    stage_b3(2)
    stage_c(2)
    stage_e1(1)
    stage_b1(3)
    stage_d(2)
    stage_w(1)
    stage_e2(1)
    stage_b2(3)
    stage_b3(3)
    stage_c(3)
    stage_e1(2)
    stage_d(3)
    stage_w(2)
    stage_e2(2)
    stage_e1(3)
    stage_w(3)
    outs = [
        pltpu.make_async_copy(acc_g, gg_hbm, out_sem.at[0]),
        pltpu.make_async_copy(acc_u, gu_hbm, out_sem.at[1]),
    ]
    for j in range(N_TP):
        outs.append(
            pltpu.make_async_copy(acc_d.at[j], gd_hbm.at[:, pl.ds(j * SL, SL)], out_sem.at[2 + j])
        )
    for copy in outs:
        copy.start()
    stage_e2(3)
    total = up_v[...].astype(F32)
    for k in range(NC):
        for p in range(k * PER, (k + 1) * PER):
            if p != OWN:
                back_copy(p).wait_recv()
        total = total + dot_nn(onehot[k], ret[k * PER:(k + 1) * PER].reshape(ROWS, SL))
    gs_ref[...] = total.astype(BF16)

    for p in range(N_SP):
        if p != OWN:
            a2a(p).wait_send()
            back_copy(p).wait_send()
    for k in range(NC):
        for kind in range(14):
            spread(k, kind).wait_send()
        for kind in range(7):
            rings(k, kind).wait_send()
    for copy in outs:
        copy.wait()


def main_call(upstream, stream, routes, route_weights, wg, wu, wd):
    any_spec = pl.BlockSpec(memory_space=pl.ANY)
    vmem = pl.BlockSpec(memory_space=pltpu.VMEM)
    flops = 2 * N_SP * CAP * 2048 * 256 * 8
    return pl.pallas_call(
        main_kernel,
        out_shape=(
            jax.ShapeDtypeStruct((TOK, SL), BF16),
            jax.ShapeDtypeStruct((N_TP, SL, SL), F32),
            jax.ShapeDtypeStruct((N_TP, SL, SL), F32),
            jax.ShapeDtypeStruct((SL, N_TP * SL), F32),
        ),
        in_specs=[any_spec, any_spec, vmem, vmem, any_spec, any_spec, any_spec],
        out_specs=(vmem, any_spec, any_spec, any_spec),
        scratch_shapes=[
            pltpu.VMEM((TOK, SL), BF16),
            pltpu.VMEM((TOK, SL), BF16),
            pltpu.VMEM((N_TP, SL, SL), BF16),
            pltpu.VMEM((N_TP, SL, SL), BF16),
            pltpu.VMEM((N_TP, SL, SL), BF16),
            pltpu.VMEM((N_SP, 2, CAP, SL), BF16),
            pltpu.VMEM((2, N_TP, N_SP * CAP, SL), BF16),
            pltpu.VMEM((NC, TOK, ROWS), BF16),
            pltpu.VMEM((NC, 2, NY, ROWS, SL), BF16),
            pltpu.VMEM((NC, NY, ROWS, SL), BF16),
            pltpu.VMEM((NC, NY, ROWS, SL), BF16),
            pltpu.VMEM((NC, 6, HALF, SL), BF16),
            pltpu.VMEM((NC, 2, HALF, SL), BF16),
            pltpu.VMEM((N_SP, CAP, SL), BF16),
            pltpu.VMEM((N_SP, CAP, SL), BF16),
            pltpu.VMEM((3, ROWS, SL), F32),
            pltpu.VMEM((NC, ROWS, SL), BF16),
            pltpu.VMEM((NC, ROWS, SL), BF16),
            pltpu.VMEM((NC, ROWS, SL), BF16),
            pltpu.VMEM((N_TP, SL, SL), F32),
            pltpu.VMEM((N_TP, SL, SL), F32),
            pltpu.VMEM((N_TP, SL, SL), F32),
            pltpu.SemaphoreType.DMA((12,)),
            pltpu.SemaphoreType.DMA((10,)),
            pltpu.SemaphoreType.DMA((N_SP,)),
            pltpu.SemaphoreType.DMA((N_SP,)),
            pltpu.SemaphoreType.DMA((NC, 14)),
            pltpu.SemaphoreType.DMA((NC, 14)),
            pltpu.SemaphoreType.DMA((NC, 7)),
            pltpu.SemaphoreType.DMA((NC, 7)),
            pltpu.SemaphoreType.DMA((N_SP,)),
            pltpu.SemaphoreType.DMA((N_SP,)),
        ],
        compiler_params=pltpu.CompilerParams(
            collective_id=0, has_side_effects=True, vmem_limit_bytes=56 * 1024 * 1024
        ),
        cost_estimate=pl.CostEstimate(flops=flops, bytes_accessed=16 << 20, transcendentals=0),
        name="routed_experts",
    )(upstream, stream, routes, route_weights, wg, wu, wd)


def copy_for_each(shard, axis):
    size = lax.axis_size(axis)
    return lax.all_to_all(
        jnp.broadcast_to(shard[None], (size, *shard.shape)), axis, 0, 0, tiled=True
    )


def laid_out(tiles, dim):
    tiles = jnp.moveaxis(tiles, 0, dim)
    shape = tiles.shape
    return tiles.reshape(*shape[:dim], shape[dim] * shape[dim + 1], *shape[dim + 2 :])


def gather_directly(shard, axis, dim):
    tiles = copy_for_each(shard, axis)
    return laid_out(tiles, dim)


def taken_together(shard, axis):
    return copy_for_each(shard, axis).sum(axis=0)


def packed_total(arrays, axis):
    ends = [0]
    for a in arrays:
        ends.append(ends[-1] + a.size)
    so_far = taken_together(jnp.concatenate([a.ravel() for a in arrays]), axis)
    return tuple((so_far[b:e].reshape(a.shape) for a, b, e in zip(arrays, ends, ends[1:])))


def passed_along(shard, axis, by):
    size = lax.axis_size(axis)
    pairs = [(i, i + by) for i in range(size) if 0 <= i + by < size]
    return lax.ppermute(shard, axis, pairs)


def in_blocks(shard, dim, size):
    before, after = (shard.shape[:dim], shard.shape[dim + 1 :])
    return jnp.moveaxis(shard.reshape(*before, size, -1, *after), dim, 0)


def sum_at_owner(shard, axis, dim):
    tiles = in_blocks(shard, dim, lax.axis_size(axis))
    arrived = lax.all_to_all(tiles, axis, split_axis=0, concat_axis=0, tiled=True)
    return arrived.sum(axis=0)


def contract_rows(left, right):
    return lax.dot_general(
        left, right, (((0,), (0,)), ((), ())), preferred_element_type=jnp.float32
    )


def on_device(
    upstream,
    stream,
    routes,
    route_weights,
    glu_value,
    glu_gate,
    conv_taps,
    conv_saved,
    out_proj,
    expert_gate,
    expert_up,
    expert_down,
):
    tok_count = upstream.shape[0]
    grad_stream, grad_gate_w, grad_up_w, grad_down_w = main_call(
        upstream, stream, routes, route_weights,
        expert_gate.reshape(N_TP, SL, SL), expert_up.reshape(N_TP, SL, SL), expert_down[0],
    )
    grad_gate_w = grad_gate_w.reshape(N_TP * SL, SL)
    grad_up_w = grad_up_w.reshape(N_TP * SL, SL)
    full_grad = gather_directly(grad_stream, "tp", 1)
    saved_conv = conv_saved.astype(jnp.float32)
    total_sum, square_sum = packed_total(
        (jnp.sum(saved_conv, axis=1), jnp.sum(saved_conv * saved_conv, axis=1)), "tp"
    )
    mean_c = (total_sum / CW)[:, None]
    var_c = (square_sum / CW)[:, None] - mean_c * mean_c
    inv_std = lax.rsqrt(var_c + norm_eps)
    normed = (saved_conv - mean_c) * inv_std
    norm_sigmoid = jax.nn.sigmoid(normed)
    mixed = (normed * norm_sigmoid).astype(jnp.bfloat16)
    grad_mixed = jnp.dot(full_grad, out_proj, preferred_element_type=jnp.float32)
    grad_normed = grad_mixed * norm_sigmoid * (1.0 + normed * (1.0 - norm_sigmoid))
    first_sum, second_sum = packed_total(
        (jnp.sum(grad_normed, axis=1), jnp.sum(grad_normed * normed, axis=1)), "tp"
    )
    grad_conv = inv_std * (
        grad_normed - (first_sum / CW)[:, None] - normed * (second_sum / CW)[:, None]
    )
    kernel_width = conv_taps.shape[0]
    rim_rows = passed_along(grad_conv[: kernel_width - 1], "sp", -1)
    padded = jnp.concatenate([grad_conv, rim_rows], axis=0)
    grad_glu = jnp.zeros_like(grad_conv)
    for offset in range(kernel_width):
        grad_glu = grad_glu + conv_taps[offset][None, :] * padded[offset : offset + tok_count]
    gate_sig = jax.nn.sigmoid(glu_gate.astype(jnp.float32))
    grad_value = (grad_glu * gate_sig).astype(jnp.bfloat16)
    grad_gate = (grad_glu * glu_value.astype(jnp.float32) * gate_sig * (1.0 - gate_sig)).astype(
        jnp.bfloat16
    )
    grad_out_proj = sum_at_owner(contract_rows(full_grad, mixed), "sp", 0)
    return (
        grad_stream,
        grad_value,
        grad_gate,
        grad_out_proj,
        grad_gate_w[None],
        grad_up_w[None],
        grad_down_w[None],
    )


def solution(mesh):
    in_specs = (
        P("sp", None),
        P("sp", None),
        P("sp", None),
        P("sp", None),
        P("sp", "tp"),
        P("sp", "tp"),
        P(None, "tp"),
        P("sp", "tp"),
        P(None, "tp"),
        P("sp", None, "tp"),
        P("sp", None, "tp"),
        P("sp", "tp", None),
    )
    out_specs = (
        P("sp", "tp"),
        P("sp", "tp"),
        P("sp", "tp"),
        P("sp", "tp"),
        P("sp", None, "tp"),
        P("sp", None, "tp"),
        P("sp", "tp", None),
    )
    return jax.shard_map(
        on_device, mesh=mesh, in_specs=in_specs, out_specs=out_specs, check_vma=False
    )
```

```python
import jax
import jax.numpy as jnp
from jax import lax
from jax.experimental import pallas as pl
from jax.experimental.pallas import tpu as pltpu
from jax.sharding import PartitionSpec as P

MESH = pl.DeviceIdType.MESH
BF16 = jnp.bfloat16
F32 = jnp.float32

CW = 512
NZ, NX, NY = 8, 4, 4
N_SP = 32
N_TP = 8
CAP = 32
TOK = 256
SL = 256
NC = 4
PER = N_SP // NC
ROWS = PER * CAP
HALF = ROWS // 2

clamp_limit = 7.0
glu_alpha = 1.702
norm_eps = 1e-05

DZ = (1, 7, 2, 6, 3, 5, 4, 0)
OWN = 28
CH = 64
KW = 31


def position_of(expert, z, x):
    dz = ((expert >> 2) - z) & 7
    dx = ((expert & 3) - x) & 3
    h = jnp.minimum(dz, 8 - dz)
    q = jnp.where(dz == 0, 7, jnp.where(dz == 4, 6, 2 * (h - 1) + jnp.where(dz > 4, 1, 0)))
    return 4 * q + dx


def dot_tn(left, right):
    return lax.dot_general(left, right, (((0,), (0,)), ((), ())), preferred_element_type=F32)


def dot_nt(left, right):
    return lax.dot_general(left, right, (((1,), (1,)), ((), ())), preferred_element_type=F32)


def dot_nn(left, right):
    return lax.dot_general(left, right, (((1,), (0,)), ((), ())), preferred_element_type=F32)


def main_kernel(
    up_hbm, st_hbm, routes_hbm, weights_hbm, wg_hbm, wu_hbm, wd_hbm,
    value_hbm, gate_hbm, taps_hbm, conv_hbm, proj_hbm,
    gs_ref, gv_ref, gq_ref, go_ref, acc_g, acc_u, acc_d,
    up_v, st_v, routes_v, weights_v, wg, wu, wd, send, xs, onehot, part, part_in, comb, ring_in, relay,
    row_out, ret, acc_pre, ggp, gup, act_t,
    value_v, gate_v, taps_v, conv_all, proj_all, hh, hn, mix, stat,
    pm, pm_in, pm_out, pm_got, sums, sums_in, conv_grad, gt, gt_in, gt_out, gt_got,
    load_sem, a_snd, a_rcv, g_snd, g_rcv, r_snd, r_rcv, b_snd, b_rcv,
    e_snd, e_rcv, p_snd, p_rcv, s_snd, s_rcv, h_snd, h_rcv, o_snd, o_rcv, f_snd, f_rcv,
):
    sp = lax.axis_index("sp")
    tp = lax.axis_index("tp")
    z, x = sp // NX, sp % NX
    y, c = tp // 2, tp % 2
    fwd, bwd = ((y + 1) % NY) * 2 + c, ((y + 3) % NY) * 2 + c
    opp = ((y + 2) % NY) * 2 + c
    other = y * 2 + (1 - c)
    up_dev, down_dev, mate = (sp, fwd), (sp, bwd), (sp, other)
    oc = 1 - c
    fwd_o, bwd_o, opp_o = ((y + 1) % NY) * 2 + oc, ((y + 3) % NY) * 2 + oc, ((y + 2) % NY) * 2 + oc

    def sp_dev(p, sign):
        dz, dx = DZ[p // 4], p % 4
        if sign < 0:
            dz, dx = (NZ - dz) % NZ, (NX - dx) % NX
        return (((z + dz) % NZ) * NX + (x + dx) % NX, tp)

    column = pl.multiple_of(tp * SL, SL)
    loads = [
        pltpu.make_async_copy(st_hbm.at[:, pl.ds(column, SL)], st_v, load_sem.at[0]),
        pltpu.make_async_copy(up_hbm.at[:, pl.ds(column, SL)], up_v, load_sem.at[1]),
        pltpu.make_async_copy(routes_hbm, routes_v, load_sem.at[2]),
        pltpu.make_async_copy(weights_hbm, weights_v, load_sem.at[3]),
    ]
    late = [
        pltpu.make_async_copy(wg_hbm, wg, load_sem.at[4]),
        pltpu.make_async_copy(wu_hbm, wu, load_sem.at[5]),
    ]
    for j in range(N_TP):
        late.append(
            pltpu.make_async_copy(wd_hbm.at[:, pl.ds(j * SL, SL)], wd.at[j], load_sem.at[6 + j])
        )
    tail_loads = [
        pltpu.make_async_copy(value_hbm, value_v, load_sem.at[14]),
        pltpu.make_async_copy(gate_hbm, gate_v, load_sem.at[15]),
        pltpu.make_async_copy(taps_hbm, taps_v, load_sem.at[16]),
        pltpu.make_async_copy(conv_hbm, conv_all.at[tp], load_sem.at[17]),
        pltpu.make_async_copy(proj_hbm.at[:, pl.ds(column, SL)], proj_all.at[tp], load_sem.at[18]),
    ]
    for copy in loads + late + tail_loads:
        copy.start()

    barrier = pltpu.get_barrier_semaphore()
    for p in range(N_SP):
        if p != OWN:
            pl.semaphore_signal(barrier, inc=1, device_id=sp_dev(p, 1), device_id_type=MESH)
    peers = [(sp, (tp + r) % N_TP) for r in range(1, N_TP)]
    for dev in peers:
        pl.semaphore_signal(barrier, inc=1, device_id=dev, device_id_type=MESH)
    owners = [(tp * NX + a, sp // NX) for a in range(NX)]
    for a in range(NX):

        @pl.when((sp // NX != tp) | (sp % NX != a))
        def _(a=a):
            pl.semaphore_signal(barrier, inc=1, device_id=owners[a], device_id_type=MESH)

    for copy in loads:
        copy.wait()
    packed = jnp.concatenate(
        [routes_v[...].astype(F32), weights_v[...], jnp.zeros((4, TOK), F32)], axis=0
    ).T
    r0, r1 = packed[:, 0:1].astype(jnp.int32), packed[:, 1:2].astype(jnp.int32)
    experts = lax.broadcasted_iota(jnp.int32, (TOK, N_SP), 1)
    c0 = jnp.where(r0 == experts, 1.0, 0.0).astype(F32)
    c1 = jnp.where(r1 == experts, 1.0, 0.0).astype(F32)
    tri = jnp.where(
        lax.broadcasted_iota(jnp.int32, (TOK, TOK), 1) < lax.broadcasted_iota(jnp.int32, (TOK, TOK), 0),
        1.0, 0.0,
    ).astype(BF16)
    earlier = dot_nn(tri, (c0 + c1).astype(BF16))
    slot0 = jnp.sum(earlier * c0, axis=1, keepdims=True).astype(jnp.int32)
    slot1 = jnp.sum(earlier * c1, axis=1, keepdims=True).astype(jnp.int32)
    pos0 = position_of(r0, z, x) * CAP + slot0
    pos1 = position_of(r1, z, x) * CAP + slot1
    stream = st_v[...]
    ups = up_v[...].astype(F32)
    cot0 = (packed[:, 2:3] * ups).astype(BF16)
    cot1 = (packed[:, 3:4] * ups).astype(BF16)
    lanes = lax.broadcasted_iota(jnp.int32, (TOK, ROWS), 1)

    def a2a(p):
        return pltpu.make_async_remote_copy(
            src_ref=send.at[p],
            dst_ref=xs.at[:, tp, pl.ds(p * CAP, CAP), :],
            send_sem=a_snd.at[p],
            recv_sem=a_rcv.at[p],
            device_id=sp_dev(p, 1),
            device_id_type=MESH,
        )

    def share(r, what):
        at = pl.multiple_of(((tp + r) % N_TP) * SL, SL)
        src = conv_hbm if what == 0 else proj_hbm.at[:, pl.ds(at, SL)]
        dst = conv_all.at[tp] if what == 0 else proj_all.at[tp]
        return pltpu.make_async_remote_copy(
            src_ref=src, dst_ref=dst, send_sem=e_snd.at[what, r - 1], recv_sem=e_rcv.at[what, r - 1],
            device_id=peers[r - 1], device_id_type=MESH,
        )

    for k in range(NC):
        s0 = jnp.where(pos0 - k * ROWS == lanes, 1.0, 0.0).astype(BF16)
        s1 = jnp.where(pos1 - k * ROWS == lanes, 1.0, 0.0).astype(BF16)
        both = s0 + s1
        onehot[k] = both
        rows = dot_tn(both, stream).astype(BF16)
        cots = (dot_tn(s0, cot0) + dot_tn(s1, cot1)).astype(BF16)
        send[k * PER:(k + 1) * PER, 0] = rows.reshape(PER, CAP, SL)
        send[k * PER:(k + 1) * PER, 1] = cots.reshape(PER, CAP, SL)
        if k == 0:
            @pl.when(sp // NX == tp)
            def _():
                pl.semaphore_wait(barrier, N_SP + N_TP + NX - 3)

            @pl.when(sp // NX != tp)
            def _():
                pl.semaphore_wait(barrier, N_SP + N_TP + NX - 2)

            for r in range(1, N_TP):
                share(r, 0).start()
                share(r, 1).start()
        for p in range(k * PER, (k + 1) * PER):
            if p == OWN:
                xs[:, tp, pl.ds(p * CAP, CAP), :] = send[p]
            else:
                a2a(p).start()

    def gather(k, kind, rc, slice_at, dev):
        ref = xs.at[rc, slice_at, pl.ds(k * ROWS, ROWS), :]
        return pltpu.make_async_remote_copy(
            src_ref=ref, dst_ref=ref, send_sem=g_snd.at[k, kind], recv_sem=g_rcv.at[k, kind],
            device_id=dev, device_id_type=MESH,
        )

    plan = (
        (0, tp, up_dev), (0, tp, down_dev), (0, tp, mate),
        (1, tp, up_dev), (1, tp, down_dev), (1, tp, mate),
        (0, bwd, up_dev), (1, fwd, down_dev),
        (0, bwd, mate), (0, fwd, mate), (0, opp, mate),
        (1, fwd, mate), (1, bwd, mate), (1, opp, mate),
    )

    def spread(k, kind):
        rc, slice_at, dev = plan[kind]
        return gather(k, kind, rc, slice_at, dev)

    arrives = (bwd, fwd, other, bwd, fwd, other, opp, opp, bwd_o, fwd_o, opp_o, fwd_o, bwd_o, opp_o)
    arrives_rc = (0, 0, 0, 1, 1, 1, 0, 1, 0, 0, 0, 1, 1, 1)

    def got(k, kind):
        gather(k, kind, arrives_rc[kind], arrives[kind], mate).wait_recv()

    def stage_a(k):
        for p in range(k * PER, (k + 1) * PER):
            if p != OWN:
                a2a(p).wait_recv()
        for kind in (0, 4, 3, 1, 2, 5):
            spread(k, kind).start()

    def stage_b1(k):
        got(k, 0)
        spread(k, 6).start()
        got(k, 4)
        spread(k, 7).start()
        spread(k, 8).start()
        spread(k, 11).start()

    def stage_b2(k):
        got(k, 1)
        spread(k, 9).start()
        got(k, 3)
        spread(k, 12).start()
        got(k, 6)
        spread(k, 10).start()
        got(k, 7)
        spread(k, 13).start()

    def stage_b3(k):
        for kind in (2, 5, 8, 11, 9, 12, 10, 13):
            got(k, kind)

    def swap(k):
        return pltpu.make_async_remote_copy(
            src_ref=part.at[k, 1 - c], dst_ref=part_in.at[k],
            send_sem=r_snd.at[k, 0], recv_sem=r_rcv.at[k, 0], device_id=mate, device_id_type=MESH,
        )

    def stage_c(k):
        rows = pl.ds(k * ROWS, ROWS)
        acc_pre[...] = jnp.zeros_like(acc_pre)

        def pre(j, carry):
            r = xs[0, j, rows, :]
            acc_pre[0] += dot_nn(r, wg[j])
            acc_pre[1] += dot_nn(r, wu[j])
            acc_pre[2] += dot_nt(xs[1, j, rows, :], wd[j])
            return carry

        lax.fori_loop(0, N_TP, pre, 0)
        gate_pre, up_pre, grad_act = acc_pre[0], acc_pre[1], acc_pre[2]
        capped = jnp.minimum(gate_pre, clamp_limit)
        clipped = jnp.clip(up_pre, -clamp_limit, clamp_limit)
        sig = jax.nn.sigmoid(glu_alpha * capped)
        act = (capped * sig * (clipped + 1.0)).astype(BF16)
        slope = sig + glu_alpha * capped * sig * (1.0 - sig)
        g_gate = jnp.where(gate_pre < clamp_limit, grad_act * (clipped + 1.0) * slope, 0.0).astype(BF16)
        g_up = jnp.where(jnp.abs(up_pre) < clamp_limit, grad_act * capped * sig, 0.0).astype(BF16)
        act_t[k] = act
        ggp[k] = g_gate
        gup[k] = g_up

        def back(j, carry):
            total = dot_nt(ggp[k], wg[j]) + dot_nt(gup[k], wu[j])
            part[k, j % 2, j // 2] = total.astype(BF16)
            return carry

        lax.fori_loop(0, N_TP, back, 0)
        swap(k).start()

    def stage_w(k):
        rows = pl.ds(k * ROWS, ROWS)

        def grads(j, carry):
            r = xs[0, j, rows, :]
            at = pl.ds(pl.multiple_of(j * SL, SL), SL)
            g, u, d = dot_tn(r, ggp[k]), dot_tn(r, gup[k]), dot_tn(act_t[k], xs[1, j, rows, :])
            if k == 0:
                acc_g[j], acc_u[j], acc_d[:, at] = g, u, d
            else:
                acc_g[j] += g
                acc_u[j] += u
                acc_d[:, at] += d
            return carry

        lax.fori_loop(0, N_TP, grads, 0)

    lo, hi = pl.ds(0, HALF), pl.ds(HALF, HALF)

    def ring(k, kind, src, slot, dev):
        return pltpu.make_async_remote_copy(
            src_ref=src, dst_ref=ring_in.at[k, slot],
            send_sem=r_snd.at[k, kind], recv_sem=r_rcv.at[k, kind], device_id=dev, device_id_type=MESH,
        )

    def rings(k, kind):
        if kind == 0:
            return swap(k)
        if kind == 1:
            return ring(k, 1, comb.at[k, 2, lo, :], 0, down_dev)
        if kind == 2:
            return ring(k, 2, comb.at[k, 2, hi, :], 1, up_dev)
        if kind == 3:
            return ring(k, 3, comb.at[k, 1, lo, :], 2, up_dev)
        if kind == 4:
            return ring(k, 4, comb.at[k, 3, hi, :], 3, down_dev)
        if kind == 5:
            return ring(k, 5, relay.at[k, 0], 4, down_dev)
        return ring(k, 6, relay.at[k, 1], 5, up_dev)

    def stage_d(k):
        rings(k, 0).wait_recv()
        for r in (2, 1, 3, 0):
            at = (y + r) % NY
            comb[k, r] = (part[k, c, at].astype(F32) + part_in[k, at].astype(F32)).astype(BF16)
            if r == 2:
                rings(k, 1).start()
                rings(k, 2).start()
        rings(k, 3).start()
        rings(k, 4).start()

    def stage_e1(k):
        rings(k, 1).wait_recv()
        relay[k, 0] = (ring_in[k, 0].astype(F32) + comb[k, 3, lo, :].astype(F32)).astype(BF16)
        rings(k, 5).start()
        rings(k, 2).wait_recv()
        relay[k, 1] = (ring_in[k, 1].astype(F32) + comb[k, 1, hi, :].astype(F32)).astype(BF16)
        rings(k, 6).start()

    def back_copy(p):
        return pltpu.make_async_remote_copy(
            src_ref=row_out.at[p], dst_ref=ret.at[p],
            send_sem=b_snd.at[p], recv_sem=b_rcv.at[p], device_id=sp_dev(p, -1), device_id_type=MESH,
        )

    def stage_e2(k):
        for kind in (3, 4, 5, 6):
            rings(k, kind).wait_recv()
        low = comb[k, 0, lo, :].astype(F32) + ring_in[k, 2].astype(F32) + ring_in[k, 4].astype(F32)
        high = comb[k, 0, hi, :].astype(F32) + ring_in[k, 3].astype(F32) + ring_in[k, 5].astype(F32)
        at = k * PER
        row_out[at:at + PER // 2] = low.astype(BF16).reshape(PER // 2, CAP, SL)
        row_out[at + PER // 2:at + PER] = high.astype(BF16).reshape(PER // 2, CAP, SL)
        for p in range(at, at + PER):
            if p == OWN:
                ret[p] = row_out[p]
            else:
                back_copy(p).start()

    def stage_n():
        for copy in tail_loads:
            copy.wait()
        for r in range(1, N_TP):
            share(r, 0).wait_recv()
            share(r, 1).wait_recv()
        total, square = jnp.zeros((1, TOK), F32), jnp.zeros((1, TOK), F32)
        for k in range(N_TP):
            v = conv_all[k].astype(F32)
            total = total + jnp.sum(v, axis=0, keepdims=True)
            square = square + jnp.sum(v * v, axis=0, keepdims=True)
        mean = total / CW
        inv = lax.rsqrt(square / CW - mean * mean + norm_eps)
        stat[0:1, :] = mean
        stat[1:2, :] = inv
        for k in range(N_TP):
            n = (conv_all[k].astype(F32) - mean) * inv
            sig = jax.nn.sigmoid(n)
            slope = sig * (1.0 + n * (1.0 - sig))
            mix[k] = (n * sig).astype(BF16)
            hh[k] = slope
            hn[k] = slope * n

    stage_a(0)
    stage_b1(0)
    stage_a(1)
    stage_b2(0)
    for copy in late:
        copy.wait()
    stage_b3(0)
    stage_c(0)
    stage_b1(1)
    stage_a(2)
    stage_d(0)
    stage_n()
    stage_b2(1)
    stage_b3(1)
    stage_c(1)
    stage_e1(0)
    stage_b1(2)
    stage_a(3)
    stage_d(1)
    stage_w(0)
    stage_e2(0)
    stage_b2(2)
    stage_b3(2)
    stage_c(2)
    stage_e1(1)
    stage_b1(3)
    stage_d(2)
    stage_w(1)
    stage_e2(1)
    stage_b2(3)
    stage_b3(3)
    stage_c(3)
    stage_e1(2)
    stage_d(3)
    stage_w(2)
    stage_e2(2)
    stage_e1(3)
    stage_e2(3)
    stage_w(3)
    total = up_v[...].astype(F32)
    for k in range(NC):
        for p in range(k * PER, (k + 1) * PER):
            if p != OWN:
                back_copy(p).wait_recv()
        total = total + dot_nn(onehot[k], ret[k * PER:(k + 1) * PER].reshape(ROWS, SL))
    grads = total.astype(BF16)
    gs_ref[...] = grads

    prod = dot_nt(proj_all[...].reshape(CW, SL), grads)
    sums[0:1, :] = jnp.sum(prod * hh[...].reshape(CW, TOK), axis=0, keepdims=True)
    sums[1:2, :] = jnp.sum(prod * hn[...].reshape(CW, TOK), axis=0, keepdims=True)
    for k in range(N_TP):
        pm[k % 2, k // 2] = prod[k * CH:(k + 1) * CH].astype(BF16)

    def pm_copy(r):
        if r == 0:
            src, dst, dev = pm.at[1 - c], pm_in, mate
        else:
            src, dst, dev = pm_out.at[r - 1], pm_got.at[r - 1], (sp, ((y + r) % NY) * 2 + c)
        return pltpu.make_async_remote_copy(
            src_ref=src, dst_ref=dst, send_sem=p_snd.at[r], recv_sem=p_rcv.at[r],
            device_id=dev, device_id_type=MESH,
        )

    def sum_copy(r):
        return pltpu.make_async_remote_copy(
            src_ref=sums, dst_ref=sums_in.at[r - 1], send_sem=s_snd.at[r - 1], recv_sem=s_rcv.at[r - 1],
            device_id=peers[r - 1], device_id_type=MESH,
        )

    pm_copy(0).start()
    for r in range(1, N_TP):
        sum_copy(r).start()

    gt[...] = dot_nn(mix[...].reshape(CW, TOK), grads).astype(BF16).reshape(N_SP, CW // N_SP, SL)

    def gt_copy(p):
        dev = sp_dev(p, 1)
        return pltpu.make_async_remote_copy(
            src_ref=gt.at[dev[0]], dst_ref=gt_in.at[p], send_sem=o_snd.at[p], recv_sem=o_rcv.at[p],
            device_id=dev, device_id_type=MESH,
        )

    for p in range(N_SP):
        if p != OWN:
            gt_copy(p).start()

    pm_copy(0).wait_recv()
    for r in (2, 1, 3):
        at = (y + r) % NY
        pm_out[r - 1] = (pm[c, at].astype(F32) + pm_in[at].astype(F32)).astype(BF16)
        pm_copy(r).start()
    mixed_grad = pm[c, y].astype(F32) + pm_in[y].astype(F32)
    first, second = sums[0:1, :], sums[1:2, :]
    for r in range(1, N_TP):
        sum_copy(r).wait_recv()
        first = first + sums_in[r - 1, 0:1, :]
        second = second + sums_in[r - 1, 1:2, :]
    for r in (1, 3, 2):
        pm_copy(r).wait_recv()
        mixed_grad = mixed_grad + pm_got[r - 1].astype(F32)
    mean, inv = stat[0:1, :], stat[1:2, :]
    normed = (conv_all[tp].astype(F32) - mean) * inv
    grad_normed = mixed_grad * hh[tp]
    conv_grad[:, 0:TOK] = inv * (grad_normed - first / CW - normed * (second / CW))
    halo = pltpu.make_async_remote_copy(
        src_ref=conv_grad.at[:, pl.ds(0, 128)], dst_ref=conv_grad.at[:, pl.ds(TOK, 128)],
        send_sem=h_snd, recv_sem=h_rcv, device_id=((sp + N_SP - 1) % N_SP, tp), device_id_type=MESH,
    )
    halo.start()

    owned = gt[sp].astype(F32)
    for p in range(N_SP):
        if p != OWN:
            gt_copy(p).wait_recv()
            owned = owned + gt_in[p].astype(F32)
    gt_out[0] = owned[:, 0:128]
    gt_out[1] = owned[:, 128:256]
    part_at = sp % NX

    def owner_copy(a, slot):
        return pltpu.make_async_remote_copy(
            src_ref=gt_out.at[a // 2], dst_ref=gt_got.at[slot], send_sem=f_snd.at[a], recv_sem=f_rcv.at[slot],
            device_id=owners[a], device_id_type=MESH,
        )

    for a in range(NX):
        mine = (sp // NX == tp) & (part_at == a)

        @pl.when(mine)
        def _(a=a):
            gt_got[a] = gt_out[a // 2]

        @pl.when(jnp.logical_not(mine))
        def _(a=a):
            owner_copy(a, part_at).start()

    halo.wait_recv()
    tail = conv_grad[:, TOK:TOK + 128]
    wide = jnp.concatenate([conv_grad[:, 0:TOK], jnp.where(sp == N_SP - 1, 0.0, tail)], axis=1)
    taps_t = jnp.concatenate([taps_v[...], jnp.zeros((1, CH), F32)], axis=0).T
    glu = taps_t[:, 0:1] * wide[:, 0:TOK]
    for offset in range(1, KW):
        glu = glu + taps_t[:, offset:offset + 1] * pltpu.roll(wide, TOK + 128 - offset, 1)[:, 0:TOK]
    gate_sig = jax.nn.sigmoid(gate_v[...].astype(F32))
    gv_ref[...] = (glu * gate_sig).astype(BF16)
    gq_ref[...] = (glu * value_v[...].astype(F32) * gate_sig * (1.0 - gate_sig)).astype(BF16)

    for a in range(NX):
        mine = (sp // NX == tp) & (part_at == a)

        @pl.when(jnp.logical_not(mine))
        def _(a=a):
            owner_copy(a, a).wait_recv()
            owner_copy(a, part_at).wait_send()

    got_t = gt_got[...].reshape(CH, 128).T
    go_ref[...] = jnp.where(part_at % 2 == 0, got_t[0:CH, :], got_t[CH:2 * CH, :])

    for p in range(N_SP):
        if p != OWN:
            a2a(p).wait_send()
            back_copy(p).wait_send()
            gt_copy(p).wait_send()
    for k in range(NC):
        for kind in range(14):
            spread(k, kind).wait_send()
        for kind in range(7):
            rings(k, kind).wait_send()
    for r in range(NY):
        pm_copy(r).wait_send()
    for r in range(1, N_TP):
        sum_copy(r).wait_send()
        share(r, 0).wait_send()
        share(r, 1).wait_send()
    halo.wait_send()


def main_call(*operands):
    any_spec = pl.BlockSpec(memory_space=pl.ANY)
    vmem = pl.BlockSpec(memory_space=pltpu.VMEM)
    flops = 2 * N_SP * CAP * 2048 * 256 * 8
    V = pltpu.VMEM
    D = pltpu.SemaphoreType.DMA
    return pl.pallas_call(
        main_kernel,
        out_shape=(
            jax.ShapeDtypeStruct((TOK, SL), BF16),
            jax.ShapeDtypeStruct((CH, TOK), BF16),
            jax.ShapeDtypeStruct((CH, TOK), BF16),
            jax.ShapeDtypeStruct((CH, CH), F32),
            jax.ShapeDtypeStruct((N_TP, SL, SL), F32),
            jax.ShapeDtypeStruct((N_TP, SL, SL), F32),
            jax.ShapeDtypeStruct((SL, N_TP * SL), F32),
        ),
        in_specs=[any_spec] * 12,
        out_specs=(vmem,) * 7,
        scratch_shapes=[
            V((TOK, SL), BF16),
            V((TOK, SL), BF16),
            V((2, TOK), jnp.int32),
            V((2, TOK), F32),
            V((N_TP, SL, SL), BF16),
            V((N_TP, SL, SL), BF16),
            V((N_TP, SL, SL), BF16),
            V((N_SP, 2, CAP, SL), BF16),
            V((2, N_TP, N_SP * CAP, SL), BF16),
            V((NC, TOK, ROWS), BF16),
            V((NC, 2, NY, ROWS, SL), BF16),
            V((NC, NY, ROWS, SL), BF16),
            V((NC, NY, ROWS, SL), BF16),
            V((NC, 6, HALF, SL), BF16),
            V((NC, 2, HALF, SL), BF16),
            V((N_SP, CAP, SL), BF16),
            V((N_SP, CAP, SL), BF16),
            V((3, ROWS, SL), F32),
            V((NC, ROWS, SL), BF16),
            V((NC, ROWS, SL), BF16),
            V((NC, ROWS, SL), BF16),
            V((CH, TOK), BF16),
            V((CH, TOK), BF16),
            V((KW, CH), F32),
            V((N_TP, CH, TOK), BF16),
            V((N_TP, CH, SL), BF16),
            V((N_TP, CH, TOK), F32),
            V((N_TP, CH, TOK), F32),
            V((N_TP, CH, TOK), BF16),
            V((8, TOK), F32),
            V((2, NY, CH, TOK), BF16),
            V((NY, CH, TOK), BF16),
            V((NY - 1, CH, TOK), BF16),
            V((NY - 1, CH, TOK), BF16),
            V((8, TOK), F32),
            V((N_TP - 1, 8, TOK), F32),
            V((CH, TOK + 128), F32),
            V((N_SP, CW // N_SP, SL), BF16),
            V((N_SP, CW // N_SP, SL), BF16),
            V((2, CW // N_SP, 128), F32),
            V((NX, CW // N_SP, 128), F32),
            D((19,)),
            D((N_SP,)),
            D((N_SP,)),
            D((NC, 14)),
            D((NC, 14)),
            D((NC, 7)),
            D((NC, 7)),
            D((N_SP,)),
            D((N_SP,)),
            D((2, N_TP - 1)),
            D((2, N_TP - 1)),
            D((NY,)),
            D((NY,)),
            D((N_TP - 1,)),
            D((N_TP - 1,)),
            D,
            D,
            D((N_SP,)),
            D((N_SP,)),
            D((NX,)),
            D((NX,)),
        ],
        compiler_params=pltpu.CompilerParams(
            collective_id=0, has_side_effects=True, vmem_limit_bytes=60 * 1024 * 1024
        ),
        cost_estimate=pl.CostEstimate(flops=flops, bytes_accessed=16 << 20, transcendentals=0),
        name="routed_experts",
    )(*operands)


def on_device(
    upstream,
    stream,
    routes,
    route_weights,
    glu_value,
    glu_gate,
    conv_taps,
    conv_saved,
    out_proj,
    expert_gate,
    expert_up,
    expert_down,
):
    grad_stream, grad_value, grad_gate, grad_out_proj, grad_gate_w, grad_up_w, grad_down_w = main_call(
        upstream, stream, routes.T, route_weights.T,
        expert_gate.reshape(N_TP, SL, SL), expert_up.reshape(N_TP, SL, SL), expert_down[0],
        glu_value.T, glu_gate.T, conv_taps, conv_saved.T, out_proj.T,
    )
    return (
        grad_stream,
        grad_value.T,
        grad_gate.T,
        grad_out_proj,
        grad_gate_w.reshape(1, N_TP * SL, SL),
        grad_up_w.reshape(1, N_TP * SL, SL),
        grad_down_w[None],
    )


def solution(mesh):
    in_specs = (
        P("sp", None),
        P("sp", None),
        P("sp", None),
        P("sp", None),
        P("sp", "tp"),
        P("sp", "tp"),
        P(None, "tp"),
        P("sp", "tp"),
        P(None, "tp"),
        P("sp", None, "tp"),
        P("sp", None, "tp"),
        P("sp", "tp", None),
    )
    out_specs = (
        P("sp", "tp"),
        P("sp", "tp"),
        P("sp", "tp"),
        P("sp", "tp"),
        P("sp", None, "tp"),
        P("sp", None, "tp"),
        P("sp", "tp", None),
    )
    return jax.shard_map(
        on_device, mesh=mesh, in_specs=in_specs, out_specs=out_specs, check_vma=False
    )
```

```python
import jax
import jax.numpy as jnp
from jax import lax
from jax.experimental import pallas as pl
from jax.experimental.pallas import tpu as pltpu
from jax.sharding import PartitionSpec as P

MESH = pl.DeviceIdType.MESH
BF16 = jnp.bfloat16
F32 = jnp.float32

CW = 512
NZ, NX, NY = 8, 4, 4
N_SP = 32
N_TP = 8
CAP = 32
TOK = 256
SL = 256
CHUNKS = ((0, 4), (4, 8), (12, 8), (20, 8), (28, 4))
NC = len(CHUNKS)
MAX = 8 * CAP

clamp_limit = 7.0
glu_alpha = 1.702
norm_eps = 1e-05

OFFSETS = (
    ((0, 0), (1, 0), (7, 0), (0, 1))
    + ((0, 2), (0, 3), (1, 2), (7, 2), (2, 0), (6, 0), (2, 2), (6, 2))
    + tuple((dz, dx) for dz in (4, 5) for dx in range(4))
    + ((3, 0), (3, 1), (3, 2), (3, 3), (2, 1), (6, 1), (2, 3), (6, 3))
    + ((1, 1), (7, 1), (1, 3), (7, 3))
)
OWN = 0
G_SLOT = (0, 1, 6, 2, 3, 6, 4, 5, 6, 6, 6, 6, 6, 6)
CH = 64
KW = 31


def dot_tn(left, right):
    return lax.dot_general(left, right, (((0,), (0,)), ((), ())), preferred_element_type=F32)


def dot_nt(left, right):
    return lax.dot_general(left, right, (((1,), (1,)), ((), ())), preferred_element_type=F32)


def dot_nn(left, right):
    return lax.dot_general(left, right, (((1,), (0,)), ((), ())), preferred_element_type=F32)


def main_kernel(
    up_hbm, st_hbm, routes_hbm, weights_hbm, wg_hbm, wu_hbm, wd_hbm,
    value_hbm, gate_hbm, taps_hbm, conv_hbm, proj_hbm,
    gs_out, gv_out, gq_out, go_out, gg_out, gu_out, gd_out,
    gs_ref, gv_ref, gq_ref, go_ref, acc_g, acc_u, acc_d,
    up_v, st_v, routes_v, weights_v, wg, wu, wd, send, xs, onehot, part, part_in, comb, ring_in, relay,
    row_out, ret, ggp, gup, act,
    value_v, gate_v, taps_v, conv_all, proj_all, hh, hn, mix, stat,
    pm, pm_in, pm_out, pm_got, sums, sums_in, conv_grad, gt, gt_in, gt_out, gt_got,
    far_sem, load_sem, out_sem, a_snd, a_rcv, g_snd, g_rcv, r_snd, r_rcv, b_snd, b_rcv,
    e_snd, e_rcv, j_snd, j_rcv, k_snd, k_rcv, p_snd, p_rcv, s_snd, s_rcv, h_snd, h_rcv, o_snd, o_rcv, f_snd, f_rcv,
):
    sp = lax.axis_index("sp")
    tp = lax.axis_index("tp")
    z, x = sp // NX, sp % NX
    y, c = tp // 2, tp % 2
    fwd, bwd = ((y + 1) % NY) * 2 + c, ((y + 3) % NY) * 2 + c
    opp = ((y + 2) % NY) * 2 + c
    other = y * 2 + (1 - c)
    up_dev, down_dev, mate = (sp, fwd), (sp, bwd), (sp, other)
    oc = 1 - c
    fwd_o, bwd_o, opp_o = ((y + 1) % NY) * 2 + oc, ((y + 3) % NY) * 2 + oc, ((y + 2) % NY) * 2 + oc

    def sp_dev(p, sign):
        dz, dx = OFFSETS[p]
        if sign < 0:
            dz, dx = (NZ - dz) % NZ, (NX - dx) % NX
        return (((z + dz) % NZ) * NX + (x + dx) % NX, tp)

    def whole(ref, sem):
        pltpu.make_async_copy(ref, ref, sem).wait()

    chunk_of = [k for k, (_, count) in enumerate(CHUNKS) for _ in range(count)]
    column = pl.multiple_of(tp * SL, SL)
    quarter = pl.ds(pl.multiple_of(x * (CH // NX), CH // NX), CH // NX)
    loads = [
        pltpu.make_async_copy(st_hbm.at[:, pl.ds(column, SL)], st_v, load_sem.at[0]),
        pltpu.make_async_copy(up_hbm.at[:, pl.ds(column, SL)], up_v, load_sem.at[1]),
        pltpu.make_async_copy(routes_hbm, routes_v, load_sem.at[2]),
        pltpu.make_async_copy(weights_hbm, weights_v, load_sem.at[3]),
    ]
    late = [
        pltpu.make_async_copy(wg_hbm, wg, load_sem.at[4]),
        pltpu.make_async_copy(wu_hbm, wu, load_sem.at[5]),
    ]
    for j in range(N_TP):
        late.append(
            pltpu.make_async_copy(wd_hbm.at[:, pl.ds(j * SL, SL)], wd.at[j], load_sem.at[6])
        )
    tail_loads = [
        pltpu.make_async_copy(value_hbm, value_v, load_sem.at[7]),
        pltpu.make_async_copy(gate_hbm, gate_v, load_sem.at[8]),
        pltpu.make_async_copy(taps_hbm, taps_v, load_sem.at[9]),
        pltpu.make_async_copy(conv_hbm, conv_all.at[tp], load_sem.at[10]),
        pltpu.make_async_copy(
            proj_hbm.at[quarter, pl.ds(column, SL)], proj_all.at[tp, quarter], load_sem.at[11]
        ),
    ]
    for copy in loads + late + tail_loads:
        copy.start()

    barrier = pltpu.get_barrier_semaphore()
    peers = [(sp, (tp + r) % N_TP) for r in range(1, N_TP)]
    near = [p for p in range(N_SP) if p != OWN and OFFSETS[p][0] in (0, 1, NZ - 1)]
    for dev in [sp_dev(p, 1) for p in near] + peers:
        pl.semaphore_signal(barrier, inc=1, device_id=dev, device_id_type=MESH)
    owners = [(tp * NX + a, sp // NX) for a in range(NX)]
    above, below = (((z + 1) % NZ) * NX + x, tp), (((z + NZ - 1) % NZ) * NX + x, tp)

    for copy in loads:
        copy.wait()
    packed = jnp.concatenate(
        [routes_v[...].astype(F32), weights_v[...], jnp.zeros((4, TOK), F32)], axis=0
    ).T
    r0, r1 = packed[:, 0:1].astype(jnp.int32), packed[:, 1:2].astype(jnp.int32)
    experts = lax.broadcasted_iota(jnp.int32, (TOK, N_SP), 1)
    c0 = jnp.where(r0 == experts, 1.0, 0.0).astype(F32)
    c1 = jnp.where(r1 == experts, 1.0, 0.0).astype(F32)
    tri = jnp.where(
        lax.broadcasted_iota(jnp.int32, (TOK, TOK), 1) < lax.broadcasted_iota(jnp.int32, (TOK, TOK), 0),
        1.0, 0.0,
    ).astype(BF16)
    expert = lax.broadcasted_iota(jnp.int32, (8, N_SP), 1)
    offset_of = (((expert >> 2) - z) & (NZ - 1)) * NX + (((expert & 3) - x) & (NX - 1))
    first_slot = jnp.zeros((8, N_SP), F32)
    for p, (dz, dx) in enumerate(OFFSETS):
        first_slot = first_slot + jnp.where(offset_of == dz * NX + dx, float(p * CAP), 0.0)
    slots = dot_nn(tri, (c0 + c1).astype(BF16)) + first_slot[0:1, :]
    pos0 = jnp.sum(slots * c0, axis=1, keepdims=True).astype(jnp.int32)
    pos1 = jnp.sum(slots * c1, axis=1, keepdims=True).astype(jnp.int32)
    stream = st_v[...]
    ups = up_v[...].astype(F32)
    cot0 = (packed[:, 2:3] * ups).astype(BF16)
    cot1 = (packed[:, 3:4] * ups).astype(BF16)

    def a2a(p):
        return pltpu.make_async_remote_copy(
            src_ref=send.at[p],
            dst_ref=xs.at[:, tp, pl.ds(p * CAP, CAP), :],
            send_sem=a_snd,
            recv_sem=a_rcv.at[chunk_of[p]],
            device_id=sp_dev(p, 1),
            device_id_type=MESH,
        )

    conv_plan = ((tp, up_dev), (tp, down_dev), (tp, (sp, opp)), (tp, mate), (bwd, mate), (fwd, mate), (opp, mate))
    conv_arrives = (bwd, fwd, opp, other, bwd_o, fwd_o, opp_o)

    def conv_copy(kind, arriving=False):
        at, dev = conv_plan[kind]
        if arriving:
            at = conv_arrives[kind]
        return pltpu.make_async_remote_copy(
            src_ref=conv_hbm if kind < 4 else conv_all.at[at], dst_ref=conv_all.at[at],
            send_sem=e_snd, recv_sem=e_rcv.at[kind], device_id=dev, device_id_type=MESH,
        )

    def proj_copy(r):
        at = pl.multiple_of(((tp + r) % N_TP) * SL, SL)
        return pltpu.make_async_remote_copy(
            src_ref=proj_hbm.at[quarter, pl.ds(at, SL)], dst_ref=proj_all.at[tp, quarter],
            send_sem=j_snd, recv_sem=j_rcv, device_id=peers[r - 1], device_id_type=MESH,
        )

    def quarter_copy(d):
        return pltpu.make_async_remote_copy(
            src_ref=proj_all.at[:, quarter, :], dst_ref=proj_all.at[:, quarter, :],
            send_sem=k_snd, recv_sem=k_rcv,
            device_id=(z * NX + (x + d) % NX, tp), device_id_type=MESH,
        )

    def stage_s(k):
        start, count = CHUNKS[k]
        width = count * CAP
        lanes = lax.broadcasted_iota(jnp.int32, (TOK, width), 1) + start * CAP
        s0 = jnp.where(pos0 == lanes, 1.0, 0.0).astype(BF16)
        s1 = jnp.where(pos1 == lanes, 1.0, 0.0).astype(BF16)
        both = s0 + s1
        onehot[:, start * CAP:start * CAP + width] = both
        rows = dot_tn(both, stream).astype(BF16)
        cots = (dot_tn(s0, cot0) + dot_tn(s1, cot1)).astype(BF16)
        send[start:start + count, 0] = rows.reshape(count, CAP, SL)
        send[start:start + count, 1] = cots.reshape(count, CAP, SL)

    def stage_go(k):
        start, count = CHUNKS[k]
        for p in range(start, start + count):
            if p == OWN:
                xs[:, tp, pl.ds(p * CAP, CAP), :] = send[p]
            else:
                a2a(p).start()

    def farther(step):
        for dev in (above, below):
            pl.semaphore_signal(far_sem.at[step], inc=1, device_id=dev, device_id_type=MESH)

    def stage_f(step):
        pl.semaphore_wait(far_sem.at[step], 2)
        if step < 2:
            farther(step + 1)

    stage_s(0)
    pl.semaphore_wait(barrier, len(near) + N_TP - 1)
    farther(0)
    stage_go(0)
    for kind in range(4):
        conv_copy(kind).start()
    for r in range(1, N_TP):
        proj_copy(r).start()
    stage_s(1)
    stage_f(0)
    stage_go(1)
    stage_s(2)
    stage_f(1)
    stage_s(3)
    stage_f(2)
    stage_s(4)

    def gather(k, kind, rc, slice_at, dev):
        start, count = CHUNKS[k]
        ref = xs.at[rc, slice_at, pl.ds(start * CAP, count * CAP), :]
        return pltpu.make_async_remote_copy(
            src_ref=ref, dst_ref=ref, send_sem=g_snd, recv_sem=g_rcv.at[k, G_SLOT[kind]],
            device_id=dev, device_id_type=MESH,
        )

    plan = (
        (0, tp, up_dev), (0, tp, down_dev), (0, tp, mate),
        (1, tp, up_dev), (1, tp, down_dev), (1, tp, mate),
        (0, bwd, up_dev), (1, fwd, down_dev),
        (0, bwd, mate), (0, fwd, mate), (0, opp, mate),
        (1, fwd, mate), (1, bwd, mate), (1, opp, mate),
    )

    def spread(k, kind):
        rc, slice_at, dev = plan[kind]
        return gather(k, kind, rc, slice_at, dev)

    arrives = (bwd, fwd, other, bwd, fwd, other, opp, opp, bwd_o, fwd_o, opp_o, fwd_o, bwd_o, opp_o)
    arrives_rc = (0, 0, 0, 1, 1, 1, 0, 1, 0, 0, 0, 1, 1, 1)

    def got(k, kind):
        gather(k, kind, arrives_rc[kind], arrives[kind], mate).wait_recv()

    def stage_a(k):
        start, count = CHUNKS[k]
        begin = max(start, 1)
        whole(xs.at[:, tp, pl.ds(begin * CAP, (start + count - begin) * CAP), :], a_rcv.at[k])
        for kind in (0, 4, 3, 1, 2, 5):
            spread(k, kind).start()

    def stage_b1(k):
        got(k, 0)
        spread(k, 6).start()
        got(k, 4)
        spread(k, 7).start()
        spread(k, 8).start()
        spread(k, 11).start()

    def stage_b2(k):
        got(k, 1)
        spread(k, 9).start()
        got(k, 3)
        spread(k, 12).start()
        got(k, 6)
        spread(k, 10).start()
        got(k, 7)
        spread(k, 13).start()

    def stage_b3(k):
        start, count = CHUNKS[k]
        whole(xs.at[:, pl.ds(0, NY), pl.ds(start * CAP, count * CAP), :], g_rcv.at[k, 6])

    def swap(k):
        return pltpu.make_async_remote_copy(
            src_ref=part.at[k, 1 - c, :, pl.ds(0, CHUNKS[k][1] * CAP), :],
            dst_ref=part_in.at[k, :, pl.ds(0, CHUNKS[k][1] * CAP), :],
            send_sem=r_snd, recv_sem=r_rcv.at[k, 0], device_id=mate, device_id_type=MESH,
        )

    def stage_c(k):
        start, count = CHUNKS[k]
        size = count * CAP
        rows = pl.ds(start * CAP, size)
        gate_pre = jnp.zeros((size, SL), F32)
        up_pre = jnp.zeros((size, SL), F32)
        grad_act = jnp.zeros((size, SL), F32)
        for j in range(N_TP):
            r = xs[0, j, rows, :]
            gate_pre = gate_pre + dot_nn(r, wg[j])
            up_pre = up_pre + dot_nn(r, wu[j])
            grad_act = grad_act + dot_nt(xs[1, j, rows, :], wd[j])
        capped = jnp.minimum(gate_pre, clamp_limit)
        clipped = jnp.clip(up_pre, -clamp_limit, clamp_limit)
        sig = jax.nn.sigmoid(glu_alpha * capped)
        act[rows, :] = (capped * sig * (clipped + 1.0)).astype(BF16)
        slope = sig + glu_alpha * capped * sig * (1.0 - sig)
        g_gate = jnp.where(gate_pre < clamp_limit, grad_act * (clipped + 1.0) * slope, 0.0).astype(BF16)
        g_up = jnp.where(jnp.abs(up_pre) < clamp_limit, grad_act * capped * sig, 0.0).astype(BF16)
        ggp[rows, :] = g_gate
        gup[rows, :] = g_up
        for j in range(N_TP):
            total = dot_nt(g_gate, wg[j]) + dot_nt(g_up, wu[j])
            part[k, j % 2, j // 2, 0:size] = total.astype(BF16)
        swap(k).start()

    def stage_w(start, stop):
        rows = pl.ds(start, stop - start)

        def grads(j, carry):
            r = xs[0, j, rows, :]
            at = pl.ds(pl.multiple_of(j * SL, SL), SL)
            g, u = dot_tn(r, ggp[rows, :]), dot_tn(r, gup[rows, :])
            d = dot_tn(act[rows, :], xs[1, j, rows, :])
            if start == 0:
                acc_g[j], acc_u[j], acc_d[:, at] = g, u, d
            else:
                acc_g[j] += g
                acc_u[j] += u
                acc_d[:, at] += d
            return carry

        lax.fori_loop(0, N_TP, grads, 0)

    def halves(k):
        half = CHUNKS[k][1] * CAP // 2
        return pl.ds(0, half), pl.ds(half, half)

    def ring(k, kind, src, slot, dev):
        return pltpu.make_async_remote_copy(
            src_ref=src, dst_ref=ring_in.at[k, slot, halves(k)[0], :],
            send_sem=r_snd, recv_sem=r_rcv.at[k, kind], device_id=dev, device_id_type=MESH,
        )

    def rings(k, kind):
        lo, hi = halves(k)
        if kind == 0:
            return swap(k)
        if kind == 1:
            return ring(k, 1, comb.at[k, 2, lo, :], 0, down_dev)
        if kind == 2:
            return ring(k, 2, comb.at[k, 2, hi, :], 1, up_dev)
        if kind == 3:
            return ring(k, 3, comb.at[k, 1, lo, :], 2, up_dev)
        if kind == 4:
            return ring(k, 4, comb.at[k, 3, hi, :], 3, down_dev)
        if kind == 5:
            return ring(k, 5, relay.at[k, 0, lo, :], 4, down_dev)
        return ring(k, 6, relay.at[k, 1, lo, :], 5, up_dev)

    def stage_d(k):
        rings(k, 0).wait_recv()
        size = CHUNKS[k][1] * CAP
        for r in (2, 1, 3, 0):
            at = (y + r) % NY
            both = part[k, c, at, 0:size].astype(F32) + part_in[k, at, 0:size].astype(F32)
            comb[k, r, 0:size] = both.astype(BF16)
            if r == 2:
                rings(k, 1).start()
                rings(k, 2).start()
        rings(k, 3).start()
        rings(k, 4).start()

    def stage_e1(k):
        rings(k, 1).wait_recv()
        lo, hi = halves(k)
        relay[k, 0, lo, :] = (ring_in[k, 0, lo, :].astype(F32) + comb[k, 3, lo, :].astype(F32)).astype(BF16)
        rings(k, 5).start()
        rings(k, 2).wait_recv()
        relay[k, 1, lo, :] = (ring_in[k, 1, lo, :].astype(F32) + comb[k, 1, hi, :].astype(F32)).astype(BF16)
        rings(k, 6).start()

    def back_copy(p):
        return pltpu.make_async_remote_copy(
            src_ref=row_out.at[p], dst_ref=ret.at[p],
            send_sem=b_snd, recv_sem=b_rcv.at[chunk_of[p]], device_id=sp_dev(p, -1), device_id_type=MESH,
        )

    def stage_e2(k):
        for kind in (3, 4, 5, 6):
            rings(k, kind).wait_recv()
        lo, hi = halves(k)
        low = comb[k, 0, lo, :].astype(F32) + ring_in[k, 2, lo, :].astype(F32) + ring_in[k, 4, lo, :].astype(F32)
        high = comb[k, 0, hi, :].astype(F32) + ring_in[k, 3, lo, :].astype(F32) + ring_in[k, 5, lo, :].astype(F32)
        at, count = CHUNKS[k]
        row_out[at:at + count // 2] = low.astype(BF16).reshape(count // 2, CAP, SL)
        row_out[at + count // 2:at + count] = high.astype(BF16).reshape(count // 2, CAP, SL)
        for p in range(at, at + count):
            if p == OWN:
                ret[p] = row_out[p]
            else:
                back_copy(p).start()

    def stage_m():
        for copy in tail_loads:
            copy.wait()
        for kind in range(3):
            conv_copy(kind, True).wait_recv()
            conv_copy(kind + 4).start()
        whole(proj_all.at[pl.ds(0, N_TP - 1), pl.ds(0, CH // NX), :], j_rcv)
        for d in range(1, NX):
            quarter_copy(d).start()

    def stage_n():
        for kind in range(3, 7):
            conv_copy(kind, True).wait_recv()
        total, square = jnp.zeros((1, TOK), F32), jnp.zeros((1, TOK), F32)
        for k in range(N_TP):
            v = conv_all[k].astype(F32)
            total = total + jnp.sum(v, axis=0, keepdims=True)
            square = square + jnp.sum(v * v, axis=0, keepdims=True)
        mean = total / CW
        inv = lax.rsqrt(square / CW - mean * mean + norm_eps)
        stat[0:1, :] = mean
        stat[1:2, :] = inv
        for k in range(N_TP):
            n = (conv_all[k].astype(F32) - mean) * inv
            sig = jax.nn.sigmoid(n)
            slope = sig * (1.0 + n * (1.0 - sig))
            mix[k] = (n * sig).astype(BF16)
            hh[k] = slope
            hn[k] = slope * n

    stage_a(0)
    stage_go(2)
    stage_b1(0)
    stage_a(1)
    stage_go(3)
    stage_go(4)
    stage_b2(0)
    late[0].wait()
    late[1].wait()
    whole(wd, load_sem.at[6])
    stage_b3(0)
    stage_c(0)
    stage_b1(1)
    stage_d(0)
    stage_a(2)
    stage_m()
    stage_b2(1)
    stage_e1(0)
    stage_b3(1)
    stage_c(1)
    stage_b1(2)
    stage_d(1)
    stage_a(3)
    stage_e2(0)
    stage_n()
    stage_b2(2)
    stage_e1(1)
    stage_b3(2)
    stage_c(2)
    stage_b1(3)
    stage_d(2)
    stage_a(4)
    stage_e2(1)
    stage_w(0, 384)
    stage_b2(3)
    stage_e1(2)
    stage_b3(3)
    stage_c(3)
    stage_b1(4)
    stage_d(3)
    stage_e2(2)
    stage_w(384, 640)
    stage_b2(4)
    stage_e1(3)
    stage_b3(4)
    stage_c(4)
    stage_e2(3)
    stage_d(4)
    stage_w(640, 896)
    stage_e1(4)
    stage_w(896, 1024)
    stage_e2(4)
    outs = [
        pltpu.make_async_copy(acc_g, gg_out, out_sem.at[4]),
        pltpu.make_async_copy(acc_u, gu_out, out_sem.at[5]),
        pltpu.make_async_copy(acc_d, gd_out, out_sem.at[6]),
    ]
    for copy in outs:
        copy.start()
    total = up_v[...].astype(F32)
    for start, count in CHUNKS:
        begin = max(start, 1)
        whole(ret.at[pl.ds(begin, start + count - begin)], b_rcv.at[chunk_of[start]])
        picked = onehot[:, start * CAP:(start + count) * CAP]
        total = total + dot_nn(picked, ret[start:start + count].reshape(count * CAP, SL))
    grads = total.astype(BF16)
    gs_ref[...] = grads

    whole(proj_all.at[:, pl.ds(0, 3 * CH // NX), :], k_rcv)
    prod = dot_nt(proj_all[...].reshape(CW, SL), grads)
    sums[0:1, :] = jnp.sum(prod * hh[...].reshape(CW, TOK), axis=0, keepdims=True)
    sums[1:2, :] = jnp.sum(prod * hn[...].reshape(CW, TOK), axis=0, keepdims=True)
    for k in range(N_TP):
        pm[k % 2, k // 2] = prod[k * CH:(k + 1) * CH].astype(BF16)

    def pm_copy(r):
        if r == 0:
            src, dst, dev = pm.at[1 - c], pm_in, mate
        else:
            src, dst, dev = pm_out.at[r - 1], pm_got.at[r - 1], (sp, ((y + r) % NY) * 2 + c)
        return pltpu.make_async_remote_copy(
            src_ref=src, dst_ref=dst, send_sem=p_snd, recv_sem=p_rcv.at[r],
            device_id=dev, device_id_type=MESH,
        )

    def sum_copy(r):
        return pltpu.make_async_remote_copy(
            src_ref=sums, dst_ref=sums_in.at[r - 1], send_sem=s_snd, recv_sem=s_rcv,
            device_id=peers[r - 1], device_id_type=MESH,
        )

    pm_copy(0).start()
    for r in range(1, N_TP):
        sum_copy(r).start()

    gt[...] = dot_nn(mix[...].reshape(CW, TOK), grads).astype(BF16).reshape(N_SP, CW // N_SP, SL)

    def gt_copy(p):
        dev = sp_dev(p, 1)
        return pltpu.make_async_remote_copy(
            src_ref=gt.at[dev[0]], dst_ref=gt_in.at[p], send_sem=o_snd, recv_sem=o_rcv,
            device_id=dev, device_id_type=MESH,
        )

    for p in range(N_SP):
        if p != OWN:
            gt_copy(p).start()

    pm_copy(0).wait_recv()
    for r in (2, 1, 3):
        at = (y + r) % NY
        pm_out[r - 1] = (pm[c, at].astype(F32) + pm_in[at].astype(F32)).astype(BF16)
        pm_copy(r).start()
    mixed_grad = pm[c, y].astype(F32) + pm_in[y].astype(F32)
    first, second = sums[0:1, :], sums[1:2, :]
    whole(sums_in, s_rcv)
    for r in range(1, N_TP):
        first = first + sums_in[r - 1, 0:1, :]
        second = second + sums_in[r - 1, 1:2, :]
    for r in (1, 3, 2):
        pm_copy(r).wait_recv()
        mixed_grad = mixed_grad + pm_got[r - 1].astype(F32)
    mean, inv = stat[0:1, :], stat[1:2, :]
    normed = (conv_all[tp].astype(F32) - mean) * inv
    grad_normed = mixed_grad * hh[tp]
    conv_grad[:, 0:TOK] = inv * (grad_normed - first / CW - normed * (second / CW))
    halo = pltpu.make_async_remote_copy(
        src_ref=conv_grad.at[:, pl.ds(0, 128)], dst_ref=conv_grad.at[:, pl.ds(TOK, 128)],
        send_sem=h_snd, recv_sem=h_rcv, device_id=((sp + N_SP - 1) % N_SP, tp), device_id_type=MESH,
    )
    halo.start()

    owned = gt[sp].astype(F32)
    whole(gt_in.at[pl.ds(1, N_SP - 1)], o_rcv)
    for p in range(N_SP):
        if p != OWN:
            owned = owned + gt_in[p].astype(F32)
    gt_out[0] = owned[:, 0:128]
    gt_out[1] = owned[:, 128:256]
    part_at = sp % NX

    def owner_copy(a, slot):
        return pltpu.make_async_remote_copy(
            src_ref=gt_out.at[a // 2], dst_ref=gt_got.at[slot], send_sem=f_snd.at[a], recv_sem=f_rcv.at[slot],
            device_id=owners[a], device_id_type=MESH,
        )

    for a in range(NX):
        mine = (sp // NX == tp) & (part_at == a)

        @pl.when(mine)
        def _(a=a):
            gt_got[a] = gt_out[a // 2]

        @pl.when(jnp.logical_not(mine))
        def _(a=a):
            owner_copy(a, part_at).start()

    halo.wait_recv()
    tail = conv_grad[:, TOK:TOK + 128]
    wide = jnp.concatenate([conv_grad[:, 0:TOK], jnp.where(sp == N_SP - 1, 0.0, tail)], axis=1)
    taps_t = jnp.concatenate([taps_v[...], jnp.zeros((1, CH), F32)], axis=0).T
    glu = taps_t[:, 0:1] * wide[:, 0:TOK]
    for offset in range(1, KW):
        glu = glu + taps_t[:, offset:offset + 1] * pltpu.roll(wide, TOK + 128 - offset, 1)[:, 0:TOK]
    gate_sig = jax.nn.sigmoid(gate_v[...].astype(F32))
    gv_ref[...] = (glu * gate_sig).astype(BF16)
    gq_ref[...] = (glu * value_v[...].astype(F32) * gate_sig * (1.0 - gate_sig)).astype(BF16)

    for a in range(NX):
        mine = (sp // NX == tp) & (part_at == a)

        @pl.when(jnp.logical_not(mine))
        def _(a=a):
            owner_copy(a, a).wait_recv()
            owner_copy(a, part_at).wait_send()

    got_t = gt_got[...].reshape(CH, 128).T
    go_ref[...] = jnp.where(part_at % 2 == 0, got_t[0:CH, :], got_t[CH:2 * CH, :])

    outs.extend([
        pltpu.make_async_copy(gs_ref, gs_out, out_sem.at[0]),
        pltpu.make_async_copy(gv_ref, gv_out, out_sem.at[1]),
        pltpu.make_async_copy(gq_ref, gq_out, out_sem.at[2]),
        pltpu.make_async_copy(go_ref, go_out, out_sem.at[3]),
    ])
    for copy in outs[3:]:
        copy.start()
    whole(send.at[pl.ds(1, N_SP - 1)], a_snd)
    whole(row_out.at[pl.ds(1, N_SP - 1)], b_snd)
    whole(gt_in.at[pl.ds(1, N_SP - 1)], o_snd)
    whole(xs.at[:, pl.ds(0, 7)], g_snd)
    whole(xs.at[0, pl.ds(0, 7)], r_snd)
    whole(conv_all.at[pl.ds(0, 7)], p_snd)
    whole(sums_in, s_snd)
    whole(proj_all.at[pl.ds(0, N_TP - 1), pl.ds(0, CH // NX), :], j_snd)
    whole(proj_all.at[:, pl.ds(0, 3 * CH // NX), :], k_snd)
    whole(conv_all.at[pl.ds(0, 7)], e_snd)
    for copy in outs:
        copy.wait()
    halo.wait_send()


RESULTS = (
    ((TOK, SL), BF16),
    ((CH, TOK), BF16),
    ((CH, TOK), BF16),
    ((CH, CH), F32),
    ((N_TP, SL, SL), F32),
    ((N_TP, SL, SL), F32),
    ((SL, N_TP * SL), F32),
)


def store_kernel(*refs):
    n = len(RESULTS)
    sems = refs[-1]
    copies = [pltpu.make_async_copy(refs[i], refs[n + i], sems.at[i]) for i in range(n)]
    for copy in copies:
        copy.start()
    for copy in copies:
        copy.wait()


def store_call(*results):
    return pl.pallas_call(
        store_kernel,
        out_shape=tuple(jax.ShapeDtypeStruct(shape, dtype) for shape, dtype in RESULTS),
        in_specs=[pl.BlockSpec(memory_space=pltpu.VMEM)] * len(RESULTS),
        out_specs=(pl.BlockSpec(memory_space=pl.ANY),) * len(RESULTS),
        scratch_shapes=[pltpu.SemaphoreType.DMA((len(RESULTS),))],
        compiler_params=pltpu.CompilerParams(vmem_limit_bytes=2 * 1024 * 1024),
        name="store_results",
    )(*(pltpu.with_memory_space_constraint(r, pltpu.VMEM) for r in results))


def main_call(*operands):
    any_spec = pl.BlockSpec(memory_space=pltpu.HBM)
    flops = 2 * N_SP * CAP * 2048 * 256 * 8
    V = pltpu.VMEM
    D = pltpu.SemaphoreType.DMA
    return pl.pallas_call(
        main_kernel,
        out_shape=tuple(V(shape, dtype) for shape, dtype in RESULTS),
        in_specs=[any_spec] * 12,
        out_specs=(pl.BlockSpec(memory_space=pl.ANY),) * 7,
        scratch_shapes=[V(shape, dtype) for shape, dtype in RESULTS] + [
            V((TOK, SL), BF16),
            V((TOK, SL), BF16),
            V((2, TOK), jnp.int32),
            V((2, TOK), F32),
            V((N_TP, SL, SL), BF16),
            V((N_TP, SL, SL), BF16),
            V((N_TP, SL, SL), BF16),
            V((N_SP, 2, CAP, SL), BF16),
            V((2, N_TP, N_SP * CAP, SL), BF16),
            V((TOK, N_SP * CAP), BF16),
            V((NC, 2, NY, MAX, SL), BF16),
            V((NC, NY, MAX, SL), BF16),
            V((NC, NY, MAX, SL), BF16),
            V((NC, 6, MAX // 2, SL), BF16),
            V((NC, 2, MAX // 2, SL), BF16),
            V((N_SP, CAP, SL), BF16),
            V((N_SP, CAP, SL), BF16),
            V((N_SP * CAP, SL), BF16),
            V((N_SP * CAP, SL), BF16),
            V((N_SP * CAP, SL), BF16),
            V((CH, TOK), BF16),
            V((CH, TOK), BF16),
            V((KW, CH), F32),
            V((N_TP, CH, TOK), BF16),
            V((N_TP, CH, SL), BF16),
            V((N_TP, CH, TOK), F32),
            V((N_TP, CH, TOK), F32),
            V((N_TP, CH, TOK), BF16),
            V((8, TOK), F32),
            V((2, NY, CH, TOK), BF16),
            V((NY, CH, TOK), BF16),
            V((NY - 1, CH, TOK), BF16),
            V((NY - 1, CH, TOK), BF16),
            V((8, TOK), F32),
            V((N_TP - 1, 8, TOK), F32),
            V((CH, TOK + 128), F32),
            V((N_SP, CW // N_SP, SL), BF16),
            V((N_SP, CW // N_SP, SL), BF16),
            V((2, CW // N_SP, 128), F32),
            V((NX, CW // N_SP, 128), F32),
            pltpu.SemaphoreType.REGULAR((3,)),
            D((12,)),
            D((7,)),
            D,
            D((NC,)),
            D,
            D((NC, 7)),
            D,
            D((NC, 7)),
            D,
            D((NC,)),
            D,
            D((7,)),
            D,
            D,
            D,
            D,
            D,
            D((NY,)),
            D,
            D,
            D,
            D,
            D,
            D,
            D((NX,)),
            D((NX,)),
        ],
        compiler_params=pltpu.CompilerParams(
            collective_id=0, has_side_effects=True, vmem_limit_bytes=54 * 1024 * 1024
        ),
        cost_estimate=pl.CostEstimate(flops=flops, bytes_accessed=16 << 20, transcendentals=0),
        name="routed_experts",
    )(*operands)


def on_device(
    upstream,
    stream,
    routes,
    route_weights,
    glu_value,
    glu_gate,
    conv_taps,
    conv_saved,
    out_proj,
    expert_gate,
    expert_up,
    expert_down,
):
    grad_stream, grad_value, grad_gate, grad_out_proj, grad_gate_w, grad_up_w, grad_down_w = store_call(*main_call(
        upstream, stream, routes.T, route_weights.T,
        expert_gate.reshape(N_TP, SL, SL), expert_up.reshape(N_TP, SL, SL), expert_down[0],
        glu_value.T, glu_gate.T, conv_taps, conv_saved.T, out_proj.T,
    ))
    return (
        grad_stream,
        grad_value.T,
        grad_gate.T,
        grad_out_proj,
        grad_gate_w.reshape(1, N_TP * SL, SL),
        grad_up_w.reshape(1, N_TP * SL, SL),
        grad_down_w[None],
    )


def solution(mesh):
    in_specs = (
        P("sp", None),
        P("sp", None),
        P("sp", None),
        P("sp", None),
        P("sp", "tp"),
        P("sp", "tp"),
        P(None, "tp"),
        P("sp", "tp"),
        P(None, "tp"),
        P("sp", None, "tp"),
        P("sp", None, "tp"),
        P("sp", "tp", None),
    )
    out_specs = (
        P("sp", "tp"),
        P("sp", "tp"),
        P("sp", "tp"),
        P("sp", "tp"),
        P("sp", None, "tp"),
        P("sp", None, "tp"),
        P("sp", "tp", None),
    )
    return jax.shard_map(
        on_device, mesh=mesh, in_specs=in_specs, out_specs=out_specs, check_vma=False
    )
```

```python
import jax
import jax.numpy as jnp
from jax import lax
from jax.experimental import pallas as pl
from jax.experimental.pallas import tpu as pltpu
from jax.sharding import PartitionSpec as P

MESH = pl.DeviceIdType.MESH
BF16 = jnp.bfloat16
F32 = jnp.float32

CW = 512
NZ, NX, NY = 8, 4, 4
N_SP = 32
N_TP = 8
CAP = 32
TOK = 256
SL = 256
CHUNKS = ((0, 4), (4, 8), (12, 8), (20, 8), (28, 4))
NC = len(CHUNKS)
MAX = 8 * CAP

clamp_limit = 7.0
glu_alpha = 1.702
norm_eps = 1e-05

OFFSETS = (
    ((0, 0), (1, 0), (7, 0), (0, 1))
    + ((0, 3), (0, 2), (1, 1), (7, 1), (1, 3), (7, 3), (2, 0), (6, 0))
    + ((3, 0), (5, 0), (3, 1), (5, 1), (3, 2), (5, 2), (3, 3), (5, 3))
    + ((4, 0), (4, 1), (4, 2), (4, 3), (1, 2), (7, 2), (2, 2), (6, 2))
    + ((2, 1), (6, 1), (2, 3), (6, 3))
)
DIRECT = (0, 4)
SECOND = {p: i for i, p in enumerate(p for k in DIRECT for p in range(CHUNKS[k][0], sum(CHUNKS[k])))}
OWN = 0


def far_first(positions):
    hops = lambda p: min(OFFSETS[p][0], 8 - OFFSETS[p][0]) + min(OFFSETS[p][1], 4 - OFFSETS[p][1])
    return sorted(positions, key=lambda p: (-hops(p), p))


G_SLOT = (0, 1, 6, 2, 3, 6, 4, 5, 6, 6, 6, 6, 6, 6)
CH = 64
KW = 31


def dot_tn(left, right):
    return lax.dot_general(left, right, (((0,), (0,)), ((), ())), preferred_element_type=F32)


def dot_nt(left, right):
    return lax.dot_general(left, right, (((1,), (1,)), ((), ())), preferred_element_type=F32)


def dot_nn(left, right):
    return lax.dot_general(left, right, (((1,), (0,)), ((), ())), preferred_element_type=F32)


def main_kernel(
    up_hbm, st_hbm, routes_hbm, weights_hbm, wg_hbm, wu_hbm, wd_hbm,
    value_hbm, gate_hbm, taps_hbm, conv_hbm, proj_hbm,
    gs_out, gv_out, gq_out, go_out, gg_out, gu_out, gd_out,
    gs_ref, gv_ref, gq_ref, go_ref, acc_g, acc_u, acc_d,
    up_v, st_v, up_o, st_o, routes_v, weights_v, wg, wu, wd, send, send_o, xs, onehot, part, part_in, comb, ring_in, relay,
    row_out, ret, ggp, gup, act,
    value_v, gate_v, taps_v, conv_all, proj_all, hh, hn, mix, stat,
    pm, pm_in, pm_out, pm_got, sums, sums_in, conv_grad, gt, gt_in, gt_out, gt_got,
    far_sem, load_sem, out_sem, a_snd, a_rcv, g_snd, g_rcv, r_snd, r_rcv, b_snd, b_rcv,
    e_snd, e_rcv, j_snd, j_rcv, k_snd, k_rcv, p_snd, p_rcv, s_snd, s_rcv, h_snd, h_rcv, o_snd, o_rcv, f_snd, f_rcv,
):
    sp = lax.axis_index("sp")
    tp = lax.axis_index("tp")
    z, x = sp // NX, sp % NX
    y, c = tp // 2, tp % 2
    fwd, bwd = ((y + 1) % NY) * 2 + c, ((y + 3) % NY) * 2 + c
    opp = ((y + 2) % NY) * 2 + c
    other = y * 2 + (1 - c)
    up_dev, down_dev, mate = (sp, fwd), (sp, bwd), (sp, other)
    oc = 1 - c
    fwd_o, bwd_o, opp_o = ((y + 1) % NY) * 2 + oc, ((y + 3) % NY) * 2 + oc, ((y + 2) % NY) * 2 + oc

    def sp_dev(p, sign):
        dz, dx = OFFSETS[p]
        if sign < 0:
            dz, dx = (NZ - dz) % NZ, (NX - dx) % NX
        return (((z + dz) % NZ) * NX + (x + dx) % NX, tp)

    def whole(ref, sem):
        pltpu.make_async_copy(ref, ref, sem).wait()

    chunk_of = [k for k, (_, count) in enumerate(CHUNKS) for _ in range(count)]
    column = pl.multiple_of(tp * SL, SL)
    column_o = pl.multiple_of(opp * SL, SL)
    quarter = pl.ds(pl.multiple_of(x * (CH // NX), CH // NX), CH // NX)
    loads = [
        pltpu.make_async_copy(st_hbm.at[:, pl.ds(column, SL)], st_v, load_sem.at[0]),
        pltpu.make_async_copy(up_hbm.at[:, pl.ds(column, SL)], up_v, load_sem.at[1]),
        pltpu.make_async_copy(st_hbm.at[:, pl.ds(column_o, SL)], st_o, load_sem.at[12]),
        pltpu.make_async_copy(up_hbm.at[:, pl.ds(column_o, SL)], up_o, load_sem.at[13]),
        pltpu.make_async_copy(routes_hbm, routes_v, load_sem.at[2]),
        pltpu.make_async_copy(weights_hbm, weights_v, load_sem.at[3]),
    ]
    late = [
        pltpu.make_async_copy(wg_hbm, wg, load_sem.at[4]),
        pltpu.make_async_copy(wu_hbm, wu, load_sem.at[5]),
    ]
    for j in range(N_TP):
        late.append(
            pltpu.make_async_copy(wd_hbm.at[:, pl.ds(j * SL, SL)], wd.at[j], load_sem.at[6])
        )
    tail_loads = [
        pltpu.make_async_copy(value_hbm, value_v, load_sem.at[7]),
        pltpu.make_async_copy(gate_hbm, gate_v, load_sem.at[8]),
        pltpu.make_async_copy(taps_hbm, taps_v, load_sem.at[9]),
        pltpu.make_async_copy(conv_hbm, conv_all.at[tp], load_sem.at[10]),
        pltpu.make_async_copy(
            proj_hbm.at[quarter, pl.ds(column, SL)], proj_all.at[tp, quarter], load_sem.at[11]
        ),
    ]
    barrier = pltpu.get_barrier_semaphore()
    peers = [(sp, (tp + r) % N_TP) for r in range(1, N_TP)]
    near = [p for p in range(N_SP) if p != OWN and OFFSETS[p][0] in (0, 1, NZ - 1)]
    for dev in [sp_dev(p, 1) for p in near] + peers:
        pl.semaphore_signal(barrier, inc=1, device_id=dev, device_id_type=MESH)
    for copy in loads:
        copy.start()
    for copy in late + tail_loads:
        copy.start()
    above, below = (((z + 1) % NZ) * NX + x, tp), (((z + NZ - 1) % NZ) * NX + x, tp)

    for copy in loads:
        copy.wait()
    packed = jnp.concatenate(
        [routes_v[...].astype(F32), weights_v[...], jnp.zeros((4, TOK), F32)], axis=0
    ).T
    r0, r1 = packed[:, 0:1].astype(jnp.int32), packed[:, 1:2].astype(jnp.int32)
    experts = lax.broadcasted_iota(jnp.int32, (TOK, N_SP), 1)
    c0 = jnp.where(r0 == experts, 1.0, 0.0).astype(F32)
    c1 = jnp.where(r1 == experts, 1.0, 0.0).astype(F32)
    tri = jnp.where(
        lax.broadcasted_iota(jnp.int32, (TOK, TOK), 1) < lax.broadcasted_iota(jnp.int32, (TOK, TOK), 0),
        1.0, 0.0,
    ).astype(BF16)
    expert = lax.broadcasted_iota(jnp.int32, (8, N_SP), 1)
    offset_of = (((expert >> 2) - z) & (NZ - 1)) * NX + (((expert & 3) - x) & (NX - 1))
    first_slot = jnp.zeros((8, N_SP), F32)
    for p, (dz, dx) in enumerate(OFFSETS):
        first_slot = first_slot + jnp.where(offset_of == dz * NX + dx, float(p * CAP), 0.0)
    slots = dot_nn(tri, (c0 + c1).astype(BF16)) + first_slot[0:1, :]
    pos0 = jnp.sum(slots * c0, axis=1, keepdims=True).astype(jnp.int32)
    pos1 = jnp.sum(slots * c1, axis=1, keepdims=True).astype(jnp.int32)
    stream = st_v[...]
    ups = up_v[...].astype(F32)
    cot0 = (packed[:, 2:3] * ups).astype(BF16)
    cot1 = (packed[:, 3:4] * ups).astype(BF16)
    stream_o = st_o[...]
    ups_o = up_o[...].astype(F32)
    cot0_o = (packed[:, 2:3] * ups_o).astype(BF16)
    cot1_o = (packed[:, 3:4] * ups_o).astype(BF16)

    def a2a(p):
        return pltpu.make_async_remote_copy(
            src_ref=send.at[p],
            dst_ref=xs.at[:, tp, pl.ds(p * CAP, CAP), :],
            send_sem=a_snd.at[0],
            recv_sem=a_rcv.at[chunk_of[p]],
            device_id=sp_dev(p, 1),
            device_id_type=MESH,
        )

    def a2a_o(p):
        return pltpu.make_async_remote_copy(
            src_ref=send_o.at[SECOND[p]],
            dst_ref=xs.at[:, opp, pl.ds(p * CAP, CAP), :],
            send_sem=a_snd.at[1],
            recv_sem=a_rcv.at[chunk_of[p]],
            device_id=sp_dev(p, 1),
            device_id_type=MESH,
        )

    conv_plan = ((tp, up_dev), (tp, down_dev), (tp, (sp, opp)), (tp, mate), (bwd, mate), (fwd, mate), (opp, mate))
    conv_arrives = (bwd, fwd, opp, other, bwd_o, fwd_o, opp_o)

    def conv_copy(kind, arriving=False):
        at, dev = conv_plan[kind]
        if arriving:
            at = conv_arrives[kind]
        return pltpu.make_async_remote_copy(
            src_ref=conv_hbm if kind < 4 else conv_all.at[at], dst_ref=conv_all.at[at],
            send_sem=e_snd, recv_sem=e_rcv.at[kind], device_id=dev, device_id_type=MESH,
        )

    def proj_copy(r):
        at = pl.multiple_of(((tp + r) % N_TP) * SL, SL)
        return pltpu.make_async_remote_copy(
            src_ref=proj_hbm.at[quarter, pl.ds(at, SL)], dst_ref=proj_all.at[tp, quarter],
            send_sem=j_snd, recv_sem=j_rcv, device_id=peers[r - 1], device_id_type=MESH,
        )

    def quarter_copy(d):
        return pltpu.make_async_remote_copy(
            src_ref=proj_all.at[:, quarter, :], dst_ref=proj_all.at[:, quarter, :],
            send_sem=k_snd, recv_sem=k_rcv,
            device_id=(z * NX + (x + d) % NX, tp), device_id_type=MESH,
        )

    def stage_s(k):
        start, count = CHUNKS[k]
        width = count * CAP
        lanes = lax.broadcasted_iota(jnp.int32, (TOK, width), 1) + start * CAP
        s0 = jnp.where(pos0 == lanes, 1.0, 0.0).astype(BF16)
        s1 = jnp.where(pos1 == lanes, 1.0, 0.0).astype(BF16)
        both = s0 + s1
        onehot[:, start * CAP:start * CAP + width] = both
        rows = dot_tn(both, stream).astype(BF16)
        cots = (dot_tn(s0, cot0) + dot_tn(s1, cot1)).astype(BF16)
        send[start:start + count, 0] = rows.reshape(count, CAP, SL)
        send[start:start + count, 1] = cots.reshape(count, CAP, SL)
        if k in DIRECT:
            at = SECOND[start]
            rows = dot_tn(both, stream_o).astype(BF16)
            cots = (dot_tn(s0, cot0_o) + dot_tn(s1, cot1_o)).astype(BF16)
            send_o[at:at + count, 0] = rows.reshape(count, CAP, SL)
            send_o[at:at + count, 1] = cots.reshape(count, CAP, SL)

    def stage_go(k):
        start, count = CHUNKS[k]
        for p in range(start, start + count):
            if p == OWN:
                xs[:, tp, pl.ds(p * CAP, CAP), :] = send[p]
                xs[:, opp, pl.ds(p * CAP, CAP), :] = send_o[SECOND[p]]
            else:
                a2a(p).start()
                if k in DIRECT:
                    a2a_o(p).start()

    def farther(step):
        for dev in (above, below):
            pl.semaphore_signal(far_sem.at[step], inc=1, device_id=dev, device_id_type=MESH)

    def stage_f(step):
        pl.semaphore_wait(far_sem.at[step], 2)
        if step < 2:
            farther(step + 1)

    stage_s(0)
    stage_s(1)
    pl.semaphore_wait(barrier, len(near) + N_TP - 1)
    farther(0)
    stage_go(0)
    for kind in range(4):
        conv_copy(kind).start()
    for r in range(1, N_TP):
        proj_copy(r).start()
    stage_f(0)
    stage_go(1)
    stage_s(2)
    stage_f(1)
    stage_go(2)

    def gather(k, kind, rc, slice_at, dev):
        start, count = CHUNKS[k]
        ref = xs.at[rc, slice_at, pl.ds(start * CAP, count * CAP), :]
        return pltpu.make_async_remote_copy(
            src_ref=ref, dst_ref=ref, send_sem=g_snd.at[1 if k in DIRECT else 0], recv_sem=g_rcv.at[k, G_SLOT[kind]],
            device_id=dev, device_id_type=MESH,
        )

    plan = (
        (0, tp, up_dev), (0, tp, down_dev), (0, tp, mate),
        (1, tp, up_dev), (1, tp, down_dev), (1, tp, mate),
        (0, bwd, up_dev), (1, fwd, down_dev),
        (0, bwd, mate), (0, fwd, mate), (0, opp, mate),
        (1, fwd, mate), (1, bwd, mate), (1, opp, mate),
    )

    def spread(k, kind):
        rc, slice_at, dev = plan[kind]
        return gather(k, kind, rc, slice_at, dev)

    arrives = (bwd, fwd, other, bwd, fwd, other, opp, opp, bwd_o, fwd_o, opp_o, fwd_o, bwd_o, opp_o)
    arrives_rc = (0, 0, 0, 1, 1, 1, 0, 1, 0, 0, 0, 1, 1, 1)

    def got(k, kind):
        gather(k, kind, arrives_rc[kind], arrives[kind], mate).wait_recv()

    def stage_a(k):
        start, count = CHUNKS[k]
        begin = max(start, 1)
        slices = 2 if k in DIRECT else 1
        whole(xs.at[:, pl.ds(0, slices), pl.ds(begin * CAP, (start + count - begin) * CAP), :], a_rcv.at[k])
        for kind in (0, 4, 3, 1, 2, 5) + ((10, 13) if k in DIRECT else ()):
            spread(k, kind).start()

    def stage_b1(k):
        got(k, 0)
        if k not in DIRECT:
            spread(k, 6).start()
        got(k, 4)
        if k not in DIRECT:
            spread(k, 7).start()
        spread(k, 8).start()
        spread(k, 11).start()

    def stage_b2(k):
        got(k, 1)
        spread(k, 9).start()
        got(k, 3)
        spread(k, 12).start()
        if k not in DIRECT:
            got(k, 6)
            spread(k, 10).start()
            got(k, 7)
            spread(k, 13).start()

    def stage_b3(k):
        start, count = CHUNKS[k]
        whole(xs.at[:, pl.ds(0, NY), pl.ds(start * CAP, count * CAP), :], g_rcv.at[k, 6])

    def swap(k):
        return pltpu.make_async_remote_copy(
            src_ref=part.at[k, 1 - c, :, pl.ds(0, CHUNKS[k][1] * CAP), :],
            dst_ref=part_in.at[k, :, pl.ds(0, CHUNKS[k][1] * CAP), :],
            send_sem=r_snd, recv_sem=r_rcv.at[k, 0], device_id=mate, device_id_type=MESH,
        )

    def stage_c(k):
        start, count = CHUNKS[k]
        size = count * CAP
        rows = pl.ds(start * CAP, size)
        gate_pre = jnp.zeros((size, SL), F32)
        up_pre = jnp.zeros((size, SL), F32)
        grad_act = jnp.zeros((size, SL), F32)
        for j in range(N_TP):
            r = xs[0, j, rows, :]
            gate_pre = gate_pre + dot_nn(r, wg[j])
            up_pre = up_pre + dot_nn(r, wu[j])
            grad_act = grad_act + dot_nt(xs[1, j, rows, :], wd[j])
        capped = jnp.minimum(gate_pre, clamp_limit)
        clipped = jnp.clip(up_pre, -clamp_limit, clamp_limit)
        sig = jax.nn.sigmoid(glu_alpha * capped)
        act[rows, :] = (capped * sig * (clipped + 1.0)).astype(BF16)
        slope = sig + glu_alpha * capped * sig * (1.0 - sig)
        g_gate = jnp.where(gate_pre < clamp_limit, grad_act * (clipped + 1.0) * slope, 0.0).astype(BF16)
        g_up = jnp.where(jnp.abs(up_pre) < clamp_limit, grad_act * capped * sig, 0.0).astype(BF16)
        ggp[rows, :] = g_gate
        gup[rows, :] = g_up
        for i in range(N_TP):
            core, at = (1 - c, i) if i < NY else (c, i - NY)
            total = dot_nt(g_gate, wg[2 * at + core]) + dot_nt(g_up, wu[2 * at + core])
            part[k, core, at, 0:size] = total.astype(BF16)
            if i == NY - 1:
                swap(k).start()

    def stage_w(start, stop):
        rows = pl.ds(start, stop - start)

        def grads(j, carry):
            r = xs[0, j, rows, :]
            at = pl.ds(pl.multiple_of(j * SL, SL), SL)
            g, u = dot_tn(r, ggp[rows, :]), dot_tn(r, gup[rows, :])
            d = dot_tn(act[rows, :], xs[1, j, rows, :])
            if start == 0:
                acc_g[j], acc_u[j], acc_d[:, at] = g, u, d
            else:
                acc_g[j] += g
                acc_u[j] += u
                acc_d[:, at] += d
            return carry

        lax.fori_loop(0, N_TP, grads, 0)

    def halves(k):
        half = CHUNKS[k][1] * CAP // 2
        return pl.ds(0, half), pl.ds(half, half)

    def ring(k, kind, src, slot, dev):
        return pltpu.make_async_remote_copy(
            src_ref=src, dst_ref=ring_in.at[k, slot, halves(k)[0], :],
            send_sem=r_snd, recv_sem=r_rcv.at[k, min(kind, 3)], device_id=dev, device_id_type=MESH,
        )

    def rings(k, kind):
        lo, hi = halves(k)
        if kind == 0:
            return swap(k)
        if kind == 1:
            return ring(k, 1, comb.at[k, 2, lo, :], 0, down_dev)
        if kind == 2:
            return ring(k, 2, comb.at[k, 2, hi, :], 1, up_dev)
        if kind == 3:
            return ring(k, 3, comb.at[k, 1, lo, :], 2, up_dev)
        if kind == 4:
            return ring(k, 4, comb.at[k, 3, hi, :], 3, down_dev)
        if kind == 5:
            return ring(k, 5, relay.at[k, 0, lo, :], 4, down_dev)
        return ring(k, 6, relay.at[k, 1, lo, :], 5, up_dev)

    def stage_d(k):
        rings(k, 0).wait_recv()
        size = CHUNKS[k][1] * CAP
        for r in (2, 1, 3, 0):
            at = (y + r) % NY
            both = part[k, c, at, 0:size].astype(F32) + part_in[k, at, 0:size].astype(F32)
            comb[k, r, 0:size] = both.astype(BF16)
            if r == 2:
                rings(k, 1).start()
                rings(k, 2).start()
        rings(k, 3).start()
        rings(k, 4).start()

    def stage_e1(k):
        rings(k, 1).wait_recv()
        lo, hi = halves(k)
        relay[k, 0, lo, :] = (ring_in[k, 0, lo, :].astype(F32) + comb[k, 3, lo, :].astype(F32)).astype(BF16)
        rings(k, 5).start()
        rings(k, 2).wait_recv()
        relay[k, 1, lo, :] = (ring_in[k, 1, lo, :].astype(F32) + comb[k, 1, hi, :].astype(F32)).astype(BF16)
        rings(k, 6).start()

    def back_copy(p):
        return pltpu.make_async_remote_copy(
            src_ref=row_out.at[p], dst_ref=ret.at[p],
            send_sem=b_snd, recv_sem=b_rcv.at[chunk_of[p]], device_id=sp_dev(p, -1), device_id_type=MESH,
        )

    def stage_e2(k):
        lo, hi = halves(k)
        whole(ring_in.at[k, pl.ds(2, 4), lo, :], r_rcv.at[k, 3])
        low = comb[k, 0, lo, :].astype(F32) + ring_in[k, 2, lo, :].astype(F32) + ring_in[k, 4, lo, :].astype(F32)
        high = comb[k, 0, hi, :].astype(F32) + ring_in[k, 3, lo, :].astype(F32) + ring_in[k, 5, lo, :].astype(F32)
        at, count = CHUNKS[k]
        row_out[at:at + count // 2] = low.astype(BF16).reshape(count // 2, CAP, SL)
        row_out[at + count // 2:at + count] = high.astype(BF16).reshape(count // 2, CAP, SL)
        for p in far_first(range(at, at + count)):
            if p == OWN:
                ret[p] = row_out[p]
            else:
                back_copy(p).start()

    def stage_m():
        for copy in tail_loads:
            copy.wait()
        for kind in range(3):
            conv_copy(kind, True).wait_recv()
            conv_copy(kind + 4).start()
        whole(proj_all.at[pl.ds(0, N_TP - 1), pl.ds(0, CH // NX), :], j_rcv)
        for d in range(1, NX):
            quarter_copy(d).start()

    def stage_n():
        for kind in range(3, 7):
            conv_copy(kind, True).wait_recv()
        total, square = jnp.zeros((1, TOK), F32), jnp.zeros((1, TOK), F32)
        for k in range(N_TP):
            v = conv_all[k].astype(F32)
            total = total + jnp.sum(v, axis=0, keepdims=True)
            square = square + jnp.sum(v * v, axis=0, keepdims=True)
        mean = total / CW
        inv = lax.rsqrt(square / CW - mean * mean + norm_eps)
        stat[0:1, :] = mean
        stat[1:2, :] = inv
        for k in range(N_TP):
            n = (conv_all[k].astype(F32) - mean) * inv
            sig = jax.nn.sigmoid(n)
            slope = sig * (1.0 + n * (1.0 - sig))
            mix[k] = (n * sig).astype(BF16)
            hh[k] = slope
            hn[k] = slope * n

    stage_a(0)
    stage_s(3)
    stage_f(2)
    stage_s(4)
    stage_a(1)
    stage_go(3)
    stage_go(4)
    stage_b1(0)
    stage_b2(0)
    late[0].wait()
    late[1].wait()
    whole(wd, load_sem.at[6])
    stage_b3(0)
    stage_c(0)
    stage_b1(1)
    stage_d(0)
    stage_a(2)
    stage_m()
    stage_b2(1)
    stage_b3(1)
    stage_c(1)
    stage_e1(0)
    stage_b1(2)
    stage_d(1)
    stage_a(3)
    stage_e2(0)
    stage_n()
    stage_w(0, 384)
    stage_b2(2)
    stage_b3(2)
    stage_c(2)
    stage_e1(1)
    stage_b1(3)
    stage_d(2)
    stage_a(4)
    stage_w(384, 640)
    stage_e2(1)
    stage_b2(3)
    stage_b3(3)
    stage_c(3)
    stage_b1(4)
    stage_e1(2)
    stage_d(3)
    stage_b2(4)
    stage_b3(4)
    stage_c(4)
    stage_e2(2)
    stage_e1(3)
    stage_d(4)
    stage_w(640, 896)
    stage_e1(4)
    stage_e2(3)
    stage_e2(4)
    stage_w(896, 1024)
    outs = [
        pltpu.make_async_copy(acc_g, gg_out, out_sem.at[4]),
        pltpu.make_async_copy(acc_u, gu_out, out_sem.at[5]),
        pltpu.make_async_copy(acc_d, gd_out, out_sem.at[6]),
    ]
    for copy in outs:
        copy.start()
    total = up_v[...].astype(F32)
    for start, count in CHUNKS:
        begin = max(start, 1)
        whole(ret.at[pl.ds(begin, start + count - begin)], b_rcv.at[chunk_of[start]])
        picked = onehot[:, start * CAP:(start + count) * CAP]
        total = total + dot_nn(picked, ret[start:start + count].reshape(count * CAP, SL))
    grads = total.astype(BF16)
    gs_ref[...] = grads

    outer = dot_nn(mix[...].reshape(CW, TOK), grads).reshape(N_TP, 2, CH // 2, SL)
    low_half = lax.broadcasted_iota(jnp.int32, (CW // 2, 128), 1) < CH
    for g in range(2):
        upper = outer[:, 0, :, 128 * g:128 * g + 128].reshape(CW // 2, 128)
        lower = outer[:, 1, :, 128 * g:128 * g + 128].reshape(CW // 2, 128)
        even = jnp.where(low_half, upper, pltpu.roll(lower, CH, 1))
        odd = jnp.where(low_half, pltpu.roll(upper, CH, 1), lower)
        gt[:, 2 * g] = even.astype(BF16).reshape(N_TP, CH // 2, 128)
        gt[:, 2 * g + 1] = odd.astype(BF16).reshape(N_TP, CH // 2, 128)
    def gt_copy(p):
        dev = sp_dev(p, 1)
        return pltpu.make_async_remote_copy(
            src_ref=gt.at[dev[0] // NX, dev[0] % NX], dst_ref=gt_in.at[p], send_sem=o_snd, recv_sem=o_rcv,
            device_id=dev, device_id_type=MESH,
        )

    for p in far_first(range(N_SP)):
        if p != OWN:
            gt_copy(p).start()

    whole(proj_all.at[:, pl.ds(0, 3 * CH // NX), :], k_rcv)
    prod = dot_nt(proj_all[...].reshape(CW, SL), grads)
    sums[0:1, :] = jnp.sum(prod * hh[...].reshape(CW, TOK), axis=0, keepdims=True)
    sums[1:2, :] = jnp.sum(prod * hn[...].reshape(CW, TOK), axis=0, keepdims=True)
    for k in range(N_TP):
        pm[k % 2, k // 2] = prod[k * CH:(k + 1) * CH].astype(BF16)

    def pm_copy(r):
        if r == 0:
            src, dst, dev = pm.at[1 - c], pm_in, mate
        else:
            src, dst, dev = pm_out.at[r - 1], pm_got.at[r - 1], (sp, ((y + r) % NY) * 2 + c)
        return pltpu.make_async_remote_copy(
            src_ref=src, dst_ref=dst, send_sem=p_snd, recv_sem=p_rcv.at[r],
            device_id=dev, device_id_type=MESH,
        )

    def sum_copy(r):
        return pltpu.make_async_remote_copy(
            src_ref=sums, dst_ref=sums_in.at[r - 1], send_sem=s_snd, recv_sem=s_rcv,
            device_id=peers[r - 1], device_id_type=MESH,
        )

    pm_copy(0).start()
    for r in range(1, N_TP):
        sum_copy(r).start()

    pm_copy(0).wait_recv()
    for r in (2, 1, 3):
        at = (y + r) % NY
        pm_out[r - 1] = (pm[c, at].astype(F32) + pm_in[at].astype(F32)).astype(BF16)
        pm_copy(r).start()
    mixed_grad = pm[c, y].astype(F32) + pm_in[y].astype(F32)
    first, second = sums[0:1, :], sums[1:2, :]
    whole(sums_in, s_rcv)
    for r in range(1, N_TP):
        first = first + sums_in[r - 1, 0:1, :]
        second = second + sums_in[r - 1, 1:2, :]
    for r in (1, 3, 2):
        pm_copy(r).wait_recv()
        mixed_grad = mixed_grad + pm_got[r - 1].astype(F32)
    mean, inv = stat[0:1, :], stat[1:2, :]
    normed = (conv_all[tp].astype(F32) - mean) * inv
    grad_normed = mixed_grad * hh[tp]
    conv_grad[:, 0:TOK] = inv * (grad_normed - first / CW - normed * (second / CW))
    halo = pltpu.make_async_remote_copy(
        src_ref=conv_grad.at[:, pl.ds(0, 128)], dst_ref=conv_grad.at[:, pl.ds(TOK, 128)],
        send_sem=h_snd, recv_sem=h_rcv, device_id=((sp + N_SP - 1) % N_SP, tp), device_id_type=MESH,
    )
    halo.start()

    whole(gt_in.at[pl.ds(1, N_SP - 1)], o_rcv)
    owned = gt[z, x].astype(F32)
    for p in range(N_SP):
        if p != OWN:
            owned = owned + gt_in[p].astype(F32)
    gt_out[...] = owned
    here = z == tp
    owner_copy = pltpu.make_async_remote_copy(
        src_ref=gt_out, dst_ref=gt_got, send_sem=f_snd, recv_sem=f_rcv,
        device_id=(tp * NX + x, z), device_id_type=MESH,
    )

    @pl.when(here)
    def _():
        gt_got[...] = gt_out[...]

    @pl.when(jnp.logical_not(here))
    def _():
        owner_copy.start()

    halo.wait_recv()
    tail = conv_grad[:, TOK:TOK + 128]
    wide = jnp.concatenate([conv_grad[:, 0:TOK], jnp.where(sp == N_SP - 1, 0.0, tail)], axis=1)
    taps_t = jnp.concatenate([taps_v[...], jnp.zeros((1, CH), F32)], axis=0).T
    glu = taps_t[:, 0:1] * wide[:, 0:TOK]
    for offset in range(1, KW):
        glu = glu + taps_t[:, offset:offset + 1] * pltpu.roll(wide, TOK + 128 - offset, 1)[:, 0:TOK]
    gate_sig = jax.nn.sigmoid(gate_v[...].astype(F32))
    gv_ref[...] = (glu * gate_sig).astype(BF16)
    gq_ref[...] = (glu * value_v[...].astype(F32) * gate_sig * (1.0 - gate_sig)).astype(BF16)

    @pl.when(jnp.logical_not(here))
    def _():
        owner_copy.wait_recv()
        owner_copy.wait_send()

    got_t = gt_got[...].T
    go_ref[:, 0:CH // 2] = got_t[0:CH]
    go_ref[:, CH // 2:CH] = got_t[CH:2 * CH]
    outs.extend([
        pltpu.make_async_copy(gs_ref, gs_out, out_sem.at[0]),
        pltpu.make_async_copy(gv_ref, gv_out, out_sem.at[1]),
        pltpu.make_async_copy(gq_ref, gq_out, out_sem.at[2]),
        pltpu.make_async_copy(go_ref, go_out, out_sem.at[3]),
    ])
    for copy in outs[3:]:
        copy.start()
    whole(send.at[pl.ds(1, N_SP - 1)], a_snd.at[0])
    whole(send_o.at[pl.ds(1, len(SECOND) - 1)], a_snd.at[1])
    whole(row_out.at[pl.ds(1, N_SP - 1)], b_snd)
    whole(gt_in.at[pl.ds(1, N_SP - 1)], o_snd)

    whole(xs.at[:, pl.ds(0, 7), pl.ds(0, 768), :], g_snd.at[0])
    whole(xs.at[0, pl.ds(0, 3)], g_snd.at[1])
    whole(xs.at[0, pl.ds(0, 7)], r_snd)
    whole(conv_all.at[pl.ds(0, 7)], p_snd)
    whole(sums_in, s_snd)
    whole(proj_all.at[pl.ds(0, N_TP - 1), pl.ds(0, CH // NX), :], j_snd)
    whole(proj_all.at[:, pl.ds(0, 3 * CH // NX), :], k_snd)
    whole(conv_all.at[pl.ds(0, 7)], e_snd)
    for copy in outs:
        copy.wait()
    halo.wait_send()


RESULTS = (
    ((TOK, SL), BF16),
    ((CH, TOK), BF16),
    ((CH, TOK), BF16),
    ((CH, CH), F32),
    ((N_TP, SL, SL), F32),
    ((N_TP, SL, SL), F32),
    ((SL, N_TP * SL), F32),
)


def store_kernel(*refs):
    n = len(RESULTS)
    sems = refs[-1]
    copies = [pltpu.make_async_copy(refs[i], refs[n + i], sems.at[i]) for i in range(n)]
    for copy in copies:
        copy.start()
    for copy in copies:
        copy.wait()


def store_call(*results):
    return pl.pallas_call(
        store_kernel,
        out_shape=tuple(jax.ShapeDtypeStruct(shape, dtype) for shape, dtype in RESULTS),
        in_specs=[pl.BlockSpec(memory_space=pltpu.VMEM)] * len(RESULTS),
        out_specs=(pl.BlockSpec(memory_space=pl.ANY),) * len(RESULTS),
        scratch_shapes=[pltpu.SemaphoreType.DMA((len(RESULTS),))],
        compiler_params=pltpu.CompilerParams(vmem_limit_bytes=2 * 1024 * 1024),
        name="store_results",
    )(*(pltpu.with_memory_space_constraint(r, pltpu.VMEM) for r in results))


def main_call(*operands):
    any_spec = pl.BlockSpec(memory_space=pltpu.HBM)
    flops = 2 * N_SP * CAP * 2048 * 256 * 8
    V = pltpu.VMEM
    D = pltpu.SemaphoreType.DMA
    return pl.pallas_call(
        main_kernel,
        out_shape=tuple(V(shape, dtype) for shape, dtype in RESULTS),
        in_specs=[any_spec] * 12,
        out_specs=(pl.BlockSpec(memory_space=pl.ANY),) * 7,
        scratch_shapes=[V(shape, dtype) for shape, dtype in RESULTS] + [
            V((TOK, SL), BF16),
            V((TOK, SL), BF16),
            V((TOK, SL), BF16),
            V((TOK, SL), BF16),
            V((2, TOK), jnp.int32),
            V((2, TOK), F32),
            V((N_TP, SL, SL), BF16),
            V((N_TP, SL, SL), BF16),
            V((N_TP, SL, SL), BF16),
            V((N_SP, 2, CAP, SL), BF16),
            V((len(SECOND), 2, CAP, SL), BF16),
            V((2, N_TP, N_SP * CAP, SL), BF16),
            V((TOK, N_SP * CAP), BF16),
            V((NC, 2, NY, MAX, SL), BF16),
            V((NC, NY, MAX, SL), BF16),
            V((NC, NY, MAX, SL), BF16),
            V((NC, 6, MAX // 2, SL), BF16),
            V((NC, 2, MAX // 2, SL), BF16),
            V((N_SP, CAP, SL), BF16),
            V((N_SP, CAP, SL), BF16),
            V((N_SP * CAP, SL), BF16),
            V((N_SP * CAP, SL), BF16),
            V((N_SP * CAP, SL), BF16),
            V((CH, TOK), BF16),
            V((CH, TOK), BF16),
            V((KW, CH), F32),
            V((N_TP, CH, TOK), BF16),
            V((N_TP, CH, SL), BF16),
            V((N_TP, CH, TOK), F32),
            V((N_TP, CH, TOK), F32),
            V((N_TP, CH, TOK), BF16),
            V((8, TOK), F32),
            V((2, NY, CH, TOK), BF16),
            V((NY, CH, TOK), BF16),
            V((NY - 1, CH, TOK), BF16),
            V((NY - 1, CH, TOK), BF16),
            V((8, TOK), F32),
            V((N_TP - 1, 8, TOK), F32),
            V((CH, TOK + 128), F32),
            V((N_TP, NX, CH // 2, 128), BF16),
            V((N_SP, CH // 2, 128), BF16),
            V((CH // 2, 128), F32),
            V((CH // 2, 128), F32),
            pltpu.SemaphoreType.REGULAR((3,)),
            D((14,)),
            D((7,)),
            D((2,)),
            D((NC,)),
            D((2,)),
            D((NC, 7)),
            D,
            D((NC, 7)),
            D,
            D((NC,)),
            D,
            D((7,)),
            D,
            D,
            D,
            D,
            D,
            D((NY,)),
            D,
            D,
            D,
            D,
            D,
            D,
            D,
            D,
        ],
        compiler_params=pltpu.CompilerParams(
            collective_id=0, has_side_effects=True, vmem_limit_bytes=54 * 1024 * 1024
        ),
        cost_estimate=pl.CostEstimate(flops=flops, bytes_accessed=16 << 20, transcendentals=0),
        name="routed_experts",
    )(*operands)


def on_device(
    upstream,
    stream,
    routes,
    route_weights,
    glu_value,
    glu_gate,
    conv_taps,
    conv_saved,
    out_proj,
    expert_gate,
    expert_up,
    expert_down,
):
    grad_stream, grad_value, grad_gate, grad_out_proj, grad_gate_w, grad_up_w, grad_down_w = store_call(*main_call(
        upstream, stream, routes.T, route_weights.T,
        expert_gate.reshape(N_TP, SL, SL), expert_up.reshape(N_TP, SL, SL), expert_down[0],
        glu_value.T, glu_gate.T, conv_taps, conv_saved.T, out_proj.T,
    ))
    return (
        grad_stream,
        grad_value.T,
        grad_gate.T,
        grad_out_proj,
        grad_gate_w.reshape(1, N_TP * SL, SL),
        grad_up_w.reshape(1, N_TP * SL, SL),
        grad_down_w[None],
    )


def solution(mesh):
    in_specs = (
        P("sp", None),
        P("sp", None),
        P("sp", None),
        P("sp", None),
        P("sp", "tp"),
        P("sp", "tp"),
        P(None, "tp"),
        P("sp", "tp"),
        P(None, "tp"),
        P("sp", None, "tp"),
        P("sp", None, "tp"),
        P("sp", "tp", None),
    )
    out_specs = (
        P("sp", "tp"),
        P("sp", "tp"),
        P("sp", "tp"),
        P("sp", "tp"),
        P("sp", None, "tp"),
        P("sp", None, "tp"),
        P("sp", "tp", None),
    )
    return jax.shard_map(
        on_device, mesh=mesh, in_specs=in_specs, out_specs=out_specs, check_vma=False
    )
```

```python
import jax
import jax.numpy as jnp
from jax import lax
from jax.experimental import pallas as pl
from jax.experimental.pallas import tpu as pltpu
from jax.sharding import PartitionSpec as P

MESH = pl.DeviceIdType.MESH
BF16 = jnp.bfloat16
F32 = jnp.float32

CW = 512
NZ, NX, NY = 8, 4, 4
N_SP = 32
N_TP = 8
CAP = 32
TOK = 256
SL = 256
CHUNKS = ((0, 4), (4, 8), (12, 8), (20, 8), (28, 4))
NC = len(CHUNKS)
MAX = 8 * CAP

clamp_limit = 7.0
glu_alpha = 1.702
norm_eps = 1e-05

OFFSETS = (
    ((0, 0), (1, 0), (7, 0), (0, 1))
    + ((0, 3), (0, 2), (1, 1), (7, 1), (1, 3), (7, 3), (2, 0), (6, 0))
    + ((3, 0), (5, 0), (3, 1), (5, 1), (3, 2), (5, 2), (3, 3), (5, 3))
    + ((4, 0), (4, 1), (4, 2), (4, 3), (1, 2), (7, 2), (2, 2), (6, 2))
    + ((2, 1), (6, 1), (2, 3), (6, 3))
)
DIRECT = (0, 3, 4)
SECOND = {p: i for i, p in enumerate(p for k in DIRECT for p in range(CHUNKS[k][0], sum(CHUNKS[k])))}
OWN = 0


def far_first(positions):
    hops = lambda p: min(OFFSETS[p][0], 8 - OFFSETS[p][0]) + min(OFFSETS[p][1], 4 - OFFSETS[p][1])
    return sorted(positions, key=lambda p: (-hops(p), p))


G_SLOT = (0, 1, 3, 1, 0, 3, 2, 2, 3, 3, 3, 3, 3, 3)
CH = 64
KW = 31


def dot_tn(left, right):
    return lax.dot_general(left, right, (((0,), (0,)), ((), ())), preferred_element_type=F32)


def dot_nt(left, right):
    return lax.dot_general(left, right, (((1,), (1,)), ((), ())), preferred_element_type=F32)


def dot_nn(left, right):
    return lax.dot_general(left, right, (((1,), (0,)), ((), ())), preferred_element_type=F32)


def main_kernel(
    up_hbm, st_hbm, routes_hbm, weights_hbm, wg_hbm, wu_hbm, wd_hbm,
    value_hbm, gate_hbm, taps_hbm, conv_hbm, proj_hbm,
    gs_out, gv_out, gq_out, go_out, gg_out, gu_out, gd_out,
    gs_ref, gv_ref, gq_ref, go_ref, acc_g, acc_u, acc_d,
    up_v, st_v, up_o, st_o, routes_v, weights_v, wg, wu, wd, send, send_o, xs, onehot, part, part_in, comb, ring_in, relay,
    row_out, ret, ggp, gup, act,
    value_v, gate_v, taps_v, conv_all, proj_all, hh, hn, mix, stat,
    pm, pm_in, pm_out, pm_got, sums, sums_in, conv_grad, gt, gt_in, gt_out, gt_got,
    far_sem, load_sem, out_sem, a_snd, a_rcv, ao_rcv, g_snd, g_rcv, r_snd, r_rcv, b_snd, b_rcv,
    e_snd, e_rcv, j_snd, j_rcv, k_snd, k_rcv, p_snd, p_rcv, s_snd, s_rcv, h_snd, h_rcv, o_snd, o_rcv, f_snd, f_rcv,
):
    sp = lax.axis_index("sp")
    tp = lax.axis_index("tp")
    z, x = sp // NX, sp % NX
    y, c = tp // 2, tp % 2
    fwd, bwd = ((y + 1) % NY) * 2 + c, ((y + 3) % NY) * 2 + c
    opp = ((y + 2) % NY) * 2 + c
    other = y * 2 + (1 - c)
    up_dev, down_dev, mate = (sp, fwd), (sp, bwd), (sp, other)
    oc = 1 - c
    fwd_o, bwd_o, opp_o = ((y + 1) % NY) * 2 + oc, ((y + 3) % NY) * 2 + oc, ((y + 2) % NY) * 2 + oc

    def sp_dev(p, sign):
        dz, dx = OFFSETS[p]
        if sign < 0:
            dz, dx = (NZ - dz) % NZ, (NX - dx) % NX
        return (((z + dz) % NZ) * NX + (x + dx) % NX, tp)

    def whole(ref, sem):
        pltpu.make_async_copy(ref, ref, sem).wait()

    chunk_of = [k for k, (_, count) in enumerate(CHUNKS) for _ in range(count)]
    column = pl.multiple_of(tp * SL, SL)
    column_o = pl.multiple_of(opp * SL, SL)
    quarter = pl.ds(pl.multiple_of(x * (CH // NX), CH // NX), CH // NX)
    loads = [
        pltpu.make_async_copy(st_hbm.at[:, pl.ds(column, SL)], st_v, load_sem.at[0]),
        pltpu.make_async_copy(up_hbm.at[:, pl.ds(column, SL)], up_v, load_sem.at[1]),
        pltpu.make_async_copy(st_hbm.at[:, pl.ds(column_o, SL)], st_o, load_sem.at[12]),
        pltpu.make_async_copy(up_hbm.at[:, pl.ds(column_o, SL)], up_o, load_sem.at[13]),
        pltpu.make_async_copy(routes_hbm, routes_v, load_sem.at[2]),
        pltpu.make_async_copy(weights_hbm, weights_v, load_sem.at[3]),
    ]
    late = [
        pltpu.make_async_copy(wg_hbm, wg, load_sem.at[4]),
        pltpu.make_async_copy(wu_hbm, wu, load_sem.at[5]),
    ]
    for j in range(N_TP):
        late.append(
            pltpu.make_async_copy(wd_hbm.at[:, pl.ds(j * SL, SL)], wd.at[j], load_sem.at[6])
        )
    tail_loads = [
        pltpu.make_async_copy(value_hbm, value_v, load_sem.at[7]),
        pltpu.make_async_copy(gate_hbm, gate_v, load_sem.at[8]),
        pltpu.make_async_copy(taps_hbm, taps_v, load_sem.at[9]),
        pltpu.make_async_copy(conv_hbm, conv_all.at[tp], load_sem.at[10]),
        pltpu.make_async_copy(
            proj_hbm.at[quarter, pl.ds(column, SL)], proj_all.at[tp, quarter], load_sem.at[11]
        ),
    ]
    barrier = pltpu.get_barrier_semaphore()
    peers = [(sp, (tp + r) % N_TP) for r in range(1, N_TP)]
    near = [p for p in range(N_SP) if p != OWN and OFFSETS[p][0] in (0, 1, NZ - 1)]
    for dev in [sp_dev(p, 1) for p in near] + peers:
        pl.semaphore_signal(barrier, inc=1, device_id=dev, device_id_type=MESH)
    for copy in loads:
        copy.start()
    for copy in late + tail_loads:
        copy.start()
    above, below = (((z + 1) % NZ) * NX + x, tp), (((z + NZ - 1) % NZ) * NX + x, tp)

    for copy in loads:
        copy.wait()
    packed = jnp.concatenate(
        [routes_v[...].astype(F32), weights_v[...], jnp.zeros((4, TOK), F32)], axis=0
    ).T
    r0, r1 = packed[:, 0:1].astype(jnp.int32), packed[:, 1:2].astype(jnp.int32)
    experts = lax.broadcasted_iota(jnp.int32, (TOK, N_SP), 1)
    c0 = jnp.where(r0 == experts, 1.0, 0.0).astype(F32)
    c1 = jnp.where(r1 == experts, 1.0, 0.0).astype(F32)
    tri = jnp.where(
        lax.broadcasted_iota(jnp.int32, (TOK, TOK), 1) < lax.broadcasted_iota(jnp.int32, (TOK, TOK), 0),
        1.0, 0.0,
    ).astype(BF16)
    expert = lax.broadcasted_iota(jnp.int32, (8, N_SP), 1)
    offset_of = (((expert >> 2) - z) & (NZ - 1)) * NX + (((expert & 3) - x) & (NX - 1))
    first_slot = jnp.zeros((8, N_SP), F32)
    for p, (dz, dx) in enumerate(OFFSETS):
        first_slot = first_slot + jnp.where(offset_of == dz * NX + dx, float(p * CAP), 0.0)
    slots = dot_nn(tri, (c0 + c1).astype(BF16)) + first_slot[0:1, :]
    pos0 = jnp.sum(slots * c0, axis=1, keepdims=True).astype(jnp.int32)
    pos1 = jnp.sum(slots * c1, axis=1, keepdims=True).astype(jnp.int32)
    stream = st_v[...]
    ups = up_v[...].astype(F32)
    cot0 = (packed[:, 2:3] * ups).astype(BF16)
    cot1 = (packed[:, 3:4] * ups).astype(BF16)
    stream_o = st_o[...]
    ups_o = up_o[...].astype(F32)
    cot0_o = (packed[:, 2:3] * ups_o).astype(BF16)
    cot1_o = (packed[:, 3:4] * ups_o).astype(BF16)

    def a2a(p):
        return pltpu.make_async_remote_copy(
            src_ref=send.at[p],
            dst_ref=xs.at[:, tp, pl.ds(p * CAP, CAP), :],
            send_sem=a_snd.at[0],
            recv_sem=a_rcv.at[chunk_of[p]],
            device_id=sp_dev(p, 1),
            device_id_type=MESH,
        )

    def a2a_o(p):
        return pltpu.make_async_remote_copy(
            src_ref=send_o.at[SECOND[p]],
            dst_ref=xs.at[:, opp, pl.ds(p * CAP, CAP), :],
            send_sem=a_snd.at[1],
            recv_sem=ao_rcv.at[chunk_of[p]],
            device_id=sp_dev(p, 1),
            device_id_type=MESH,
        )

    conv_plan = ((tp, up_dev), (tp, down_dev), (tp, (sp, opp)), (tp, mate), (bwd, mate), (fwd, mate), (opp, mate))
    conv_arrives = (bwd, fwd, opp, other, bwd_o, fwd_o, opp_o)

    def conv_copy(kind, arriving=False):
        at, dev = conv_plan[kind]
        if arriving:
            at = conv_arrives[kind]
        return pltpu.make_async_remote_copy(
            src_ref=conv_hbm if kind < 4 else conv_all.at[at], dst_ref=conv_all.at[at],
            send_sem=e_snd, recv_sem=e_rcv.at[kind], device_id=dev, device_id_type=MESH,
        )

    def proj_copy(r):
        at = pl.multiple_of(((tp + r) % N_TP) * SL, SL)
        return pltpu.make_async_remote_copy(
            src_ref=proj_hbm.at[quarter, pl.ds(at, SL)], dst_ref=proj_all.at[tp, quarter],
            send_sem=j_snd, recv_sem=j_rcv, device_id=peers[r - 1], device_id_type=MESH,
        )

    def quarter_copy(d):
        return pltpu.make_async_remote_copy(
            src_ref=proj_all.at[:, quarter, :], dst_ref=proj_all.at[:, quarter, :],
            send_sem=k_snd, recv_sem=k_rcv,
            device_id=(z * NX + (x + d) % NX, tp), device_id_type=MESH,
        )

    def stage_s(k):
        start, count = CHUNKS[k]
        width = count * CAP
        lanes = lax.broadcasted_iota(jnp.int32, (TOK, width), 1) + start * CAP
        s0 = jnp.where(pos0 == lanes, 1.0, 0.0).astype(BF16)
        s1 = jnp.where(pos1 == lanes, 1.0, 0.0).astype(BF16)
        both = s0 + s1
        onehot[:, start * CAP:start * CAP + width] = both
        rows = dot_tn(both, stream).astype(BF16)
        cots = (dot_tn(s0, cot0) + dot_tn(s1, cot1)).astype(BF16)
        send[start:start + count, 0] = rows.reshape(count, CAP, SL)
        send[start:start + count, 1] = cots.reshape(count, CAP, SL)
        if k in DIRECT:
            at = SECOND[start]
            rows = dot_tn(both, stream_o).astype(BF16)
            cots = (dot_tn(s0, cot0_o) + dot_tn(s1, cot1_o)).astype(BF16)
            send_o[at:at + count, 0] = rows.reshape(count, CAP, SL)
            send_o[at:at + count, 1] = cots.reshape(count, CAP, SL)

    def stage_go(k):
        start, count = CHUNKS[k]
        for p in range(start, start + count):
            if p == OWN:
                xs[:, tp, pl.ds(p * CAP, CAP), :] = send[p]
                xs[:, opp, pl.ds(p * CAP, CAP), :] = send_o[SECOND[p]]
            else:
                a2a(p).start()

    def stage_ox(k):
        start, count = CHUNKS[k]
        for p in range(max(start, 1), start + count):
            a2a_o(p).start()

    def farther(step):
        for dev in (above, below):
            pl.semaphore_signal(far_sem.at[step], inc=1, device_id=dev, device_id_type=MESH)

    def stage_f(step):
        pl.semaphore_wait(far_sem.at[step], 2)
        if step < 2:
            farther(step + 1)

    stage_s(0)
    stage_s(1)
    pl.semaphore_wait(barrier, len(near) + N_TP - 1)
    farther(0)
    stage_go(0)
    stage_ox(0)
    for kind in range(4):
        conv_copy(kind).start()
    for r in range(1, N_TP):
        proj_copy(r).start()
    stage_f(0)
    stage_go(1)
    stage_s(2)
    stage_f(1)

    @pl.when(c == 0)
    def _():
        stage_go(2)


    def gather(k, kind, rc, slice_at, dev):
        start, count = CHUNKS[k]
        ref = xs.at[rc, slice_at, pl.ds(start * CAP, count * CAP), :]
        return pltpu.make_async_remote_copy(
            src_ref=ref, dst_ref=ref, send_sem=g_snd.at[1 if k in DIRECT else 0], recv_sem=g_rcv.at[k, G_SLOT[kind]],
            device_id=dev, device_id_type=MESH,
        )

    plan = (
        (0, tp, up_dev), (0, tp, down_dev), (0, tp, mate),
        (1, tp, up_dev), (1, tp, down_dev), (1, tp, mate),
        (0, bwd, up_dev), (1, fwd, down_dev),
        (0, bwd, mate), (0, fwd, mate), (0, opp, mate),
        (1, fwd, mate), (1, bwd, mate), (1, opp, mate),
    )

    def spread(k, kind):
        rc, slice_at, dev = plan[kind]
        return gather(k, kind, rc, slice_at, dev)

    def both(k, slot):
        start, count = CHUNKS[k]
        whole(xs.at[:, tp, pl.ds(start * CAP, count * CAP), :], g_rcv.at[k, slot])

    def stage_a(k):
        start, count = CHUNKS[k]
        begin = max(start, 1)
        whole(xs.at[:, tp, pl.ds(begin * CAP, (start + count - begin) * CAP), :], a_rcv.at[k])
        for kind in (0, 4, 3, 1, 2, 5):
            spread(k, kind).start()

    def opposite(k):
        start, count = CHUNKS[k]
        begin = max(start, 1)
        whole(xs.at[:, opp, pl.ds(begin * CAP, (start + count - begin) * CAP), :], ao_rcv.at[k])
        spread(k, 10).start()
        spread(k, 13).start()

    def stage_b1(k):
        both(k, 0)
        for kind in (8, 11) if k in DIRECT else (6, 7, 8, 11):
            spread(k, kind).start()

    def stage_b2(k):
        both(k, 1)
        spread(k, 9).start()
        spread(k, 12).start()
        if k in DIRECT:
            opposite(k)
        else:
            both(k, 2)
            spread(k, 10).start()
            spread(k, 13).start()

    def stage_b3(k):
        start, count = CHUNKS[k]
        whole(xs.at[:, pl.ds(0, NY), pl.ds(start * CAP, count * CAP), :], g_rcv.at[k, 3])

    def swap(k):
        return pltpu.make_async_remote_copy(
            src_ref=part.at[k, 1 - c, :, pl.ds(0, CHUNKS[k][1] * CAP), :],
            dst_ref=part_in.at[k, :, pl.ds(0, CHUNKS[k][1] * CAP), :],
            send_sem=r_snd, recv_sem=r_rcv.at[k, 0], device_id=mate, device_id_type=MESH,
        )

    def stage_c(k):
        start, count = CHUNKS[k]
        size = count * CAP
        rows = pl.ds(start * CAP, size)
        gate_pre = jnp.zeros((size, SL), F32)
        up_pre = jnp.zeros((size, SL), F32)
        grad_act = jnp.zeros((size, SL), F32)
        for j in range(N_TP):
            r = xs[0, j, rows, :]
            gate_pre = gate_pre + dot_nn(r, wg[j])
            up_pre = up_pre + dot_nn(r, wu[j])
            grad_act = grad_act + dot_nt(xs[1, j, rows, :], wd[j])
        capped = jnp.minimum(gate_pre, clamp_limit)
        clipped = jnp.clip(up_pre, -clamp_limit, clamp_limit)
        sig = jax.nn.sigmoid(glu_alpha * capped)
        act[rows, :] = (capped * sig * (clipped + 1.0)).astype(BF16)
        slope = sig + glu_alpha * capped * sig * (1.0 - sig)
        g_gate = jnp.where(gate_pre < clamp_limit, grad_act * (clipped + 1.0) * slope, 0.0).astype(BF16)
        g_up = jnp.where(jnp.abs(up_pre) < clamp_limit, grad_act * capped * sig, 0.0).astype(BF16)
        ggp[rows, :] = g_gate
        gup[rows, :] = g_up
        for i in range(N_TP):
            core, at = (1 - c, i) if i < NY else (c, i - NY)
            total = dot_nt(g_gate, wg[2 * at + core]) + dot_nt(g_up, wu[2 * at + core])
            part[k, core, at, 0:size] = total.astype(BF16)
            if i == NY - 1:
                swap(k).start()

    def stage_w(start, stop):
        rows = pl.ds(start, stop - start)

        def grads(j, carry):
            r = xs[0, j, rows, :]
            at = pl.ds(pl.multiple_of(j * SL, SL), SL)
            g, u = dot_tn(r, ggp[rows, :]), dot_tn(r, gup[rows, :])
            d = dot_tn(act[rows, :], xs[1, j, rows, :])
            if start == 0:
                acc_g[j], acc_u[j], acc_d[:, at] = g, u, d
            else:
                acc_g[j] += g
                acc_u[j] += u
                acc_d[:, at] += d
            return carry

        lax.fori_loop(0, N_TP, grads, 0)

    def halves(k):
        half = CHUNKS[k][1] * CAP // 2
        return pl.ds(0, half), pl.ds(half, half)

    def ring(k, kind, src, slot, dev):
        return pltpu.make_async_remote_copy(
            src_ref=src, dst_ref=ring_in.at[k, slot, halves(k)[0], :],
            send_sem=r_snd, recv_sem=r_rcv.at[k, min(kind, 3)], device_id=dev, device_id_type=MESH,
        )

    def rings(k, kind):
        lo, hi = halves(k)
        if kind == 0:
            return swap(k)
        if kind == 1:
            return ring(k, 1, comb.at[k, 2, lo, :], 0, down_dev)
        if kind == 2:
            return ring(k, 2, comb.at[k, 2, hi, :], 1, up_dev)
        if kind == 3:
            return ring(k, 3, comb.at[k, 1, lo, :], 2, up_dev)
        if kind == 4:
            return ring(k, 4, comb.at[k, 3, hi, :], 3, down_dev)
        if kind == 5:
            return ring(k, 5, relay.at[k, 0, lo, :], 4, down_dev)
        return ring(k, 6, relay.at[k, 1, lo, :], 5, up_dev)

    def stage_d(k):
        rings(k, 0).wait_recv()
        size = CHUNKS[k][1] * CAP
        for r in (2, 1, 3, 0):
            at = (y + r) % NY
            both = part[k, c, at, 0:size].astype(F32) + part_in[k, at, 0:size].astype(F32)
            comb[k, r, 0:size] = both.astype(BF16)
            if r == 2:
                rings(k, 1).start()
                rings(k, 2).start()
        rings(k, 3).start()
        rings(k, 4).start()

    def stage_e1(k):
        rings(k, 1).wait_recv()
        lo, hi = halves(k)
        relay[k, 0, lo, :] = (ring_in[k, 0, lo, :].astype(F32) + comb[k, 3, lo, :].astype(F32)).astype(BF16)
        rings(k, 5).start()
        rings(k, 2).wait_recv()
        relay[k, 1, lo, :] = (ring_in[k, 1, lo, :].astype(F32) + comb[k, 1, hi, :].astype(F32)).astype(BF16)
        rings(k, 6).start()

    def back_copy(p):
        return pltpu.make_async_remote_copy(
            src_ref=row_out.at[p], dst_ref=ret.at[p],
            send_sem=b_snd, recv_sem=b_rcv.at[chunk_of[p]], device_id=sp_dev(p, -1), device_id_type=MESH,
        )

    def stage_e2(k):
        lo, hi = halves(k)
        whole(ring_in.at[k, pl.ds(2, 4), lo, :], r_rcv.at[k, 3])
        low = comb[k, 0, lo, :].astype(F32) + ring_in[k, 2, lo, :].astype(F32) + ring_in[k, 4, lo, :].astype(F32)
        high = comb[k, 0, hi, :].astype(F32) + ring_in[k, 3, lo, :].astype(F32) + ring_in[k, 5, lo, :].astype(F32)
        at, count = CHUNKS[k]
        row_out[at:at + count // 2] = low.astype(BF16).reshape(count // 2, CAP, SL)
        row_out[at + count // 2:at + count] = high.astype(BF16).reshape(count // 2, CAP, SL)
        for p in far_first(range(at, at + count)):
            if p == OWN:
                ret[p] = row_out[p]
            else:
                back_copy(p).start()

    def stage_m():
        for copy in tail_loads:
            copy.wait()
        for kind in range(3):
            conv_copy(kind, True).wait_recv()
            conv_copy(kind + 4).start()
        whole(proj_all.at[pl.ds(0, N_TP - 1), pl.ds(0, CH // NX), :], j_rcv)
        for d in range(1, NX):
            quarter_copy(d).start()

    def stage_n():
        for kind in range(3, 7):
            conv_copy(kind, True).wait_recv()
        total, square = jnp.zeros((1, TOK), F32), jnp.zeros((1, TOK), F32)
        for k in range(N_TP):
            v = conv_all[k].astype(F32)
            total = total + jnp.sum(v, axis=0, keepdims=True)
            square = square + jnp.sum(v * v, axis=0, keepdims=True)
        mean = total / CW
        inv = lax.rsqrt(square / CW - mean * mean + norm_eps)
        stat[0:1, :] = mean
        stat[1:2, :] = inv
        for k in range(N_TP):
            n = (conv_all[k].astype(F32) - mean) * inv
            sig = jax.nn.sigmoid(n)
            slope = sig * (1.0 + n * (1.0 - sig))
            mix[k] = (n * sig).astype(BF16)
            hh[k] = slope
            hn[k] = slope * n

    stage_a(0)
    stage_s(3)
    stage_f(2)
    stage_s(4)
    stage_a(1)

    @pl.when(c == 0)
    def _():
        stage_go(3)
        stage_go(4)
        stage_ox(4)

    @pl.when(c == 1)
    def _():
        stage_go(2)

    stage_b1(0)
    stage_b2(0)
    late[0].wait()
    late[1].wait()
    whole(wd, load_sem.at[6])
    stage_b3(0)
    stage_c(0)
    stage_b1(1)
    stage_d(0)
    stage_a(2)

    @pl.when(c == 1)
    def _():
        stage_go(3)
        stage_go(4)
        stage_ox(4)

    stage_m()
    stage_b2(1)
    stage_b3(1)
    stage_c(1)
    stage_e1(0)
    stage_b1(2)
    stage_d(1)
    stage_a(3)
    stage_ox(3)
    stage_e2(0)
    stage_n()
    stage_w(0, 384)
    stage_b2(2)
    stage_b3(2)
    stage_c(2)
    stage_e1(1)
    stage_b1(3)
    stage_d(2)
    stage_a(4)
    stage_w(384, 640)
    stage_e2(1)
    stage_b2(3)
    stage_b3(3)
    stage_c(3)
    stage_b1(4)
    stage_e1(2)
    stage_d(3)
    stage_b2(4)
    stage_b3(4)
    stage_c(4)
    stage_e2(2)
    stage_e1(3)
    stage_d(4)
    stage_w(640, 896)
    stage_e1(4)
    stage_e2(3)
    stage_e2(4)
    stage_w(896, 1024)
    outs = [
        pltpu.make_async_copy(acc_g, gg_out, out_sem.at[4]),
        pltpu.make_async_copy(acc_u, gu_out, out_sem.at[5]),
        pltpu.make_async_copy(acc_d, gd_out, out_sem.at[6]),
    ]
    for copy in outs:
        copy.start()
    total = up_v[...].astype(F32)
    for start, count in CHUNKS:
        begin = max(start, 1)
        whole(ret.at[pl.ds(begin, start + count - begin)], b_rcv.at[chunk_of[start]])
        picked = onehot[:, start * CAP:(start + count) * CAP]
        total = total + dot_nn(picked, ret[start:start + count].reshape(count * CAP, SL))
    grads = total.astype(BF16)
    gs_ref[...] = grads

    outer = dot_nn(mix[...].reshape(CW, TOK), grads).reshape(N_TP, 2, CH // 2, SL)
    low_half = lax.broadcasted_iota(jnp.int32, (CW // 2, 128), 1) < CH
    for g in range(2):
        upper = outer[:, 0, :, 128 * g:128 * g + 128].reshape(CW // 2, 128)
        lower = outer[:, 1, :, 128 * g:128 * g + 128].reshape(CW // 2, 128)
        even = jnp.where(low_half, upper, pltpu.roll(lower, CH, 1))
        odd = jnp.where(low_half, pltpu.roll(upper, CH, 1), lower)
        gt[:, 2 * g] = even.astype(BF16).reshape(N_TP, CH // 2, 128)
        gt[:, 2 * g + 1] = odd.astype(BF16).reshape(N_TP, CH // 2, 128)
    def block_at(height):
        ahead = (height - tp + NZ) % NZ
        return 2 * ((y + ahead // 2 + 2) % NY) + ahead % 2

    def gt_copy(p):
        dev = sp_dev(p, 1)
        return pltpu.make_async_remote_copy(
            src_ref=gt.at[block_at(dev[0] // NX), dev[0] % NX], dst_ref=gt_in.at[p], send_sem=o_snd, recv_sem=o_rcv,
            device_id=dev, device_id_type=MESH,
        )

    for p in far_first(range(N_SP)):
        if p != OWN:
            gt_copy(p).start()

    whole(proj_all.at[:, pl.ds(0, 3 * CH // NX), :], k_rcv)
    prod = dot_nt(proj_all[...].reshape(CW, SL), grads)
    sums[0:1, :] = jnp.sum(prod * hh[...].reshape(CW, TOK), axis=0, keepdims=True)
    sums[1:2, :] = jnp.sum(prod * hn[...].reshape(CW, TOK), axis=0, keepdims=True)
    for k in range(N_TP):
        pm[k % 2, k // 2] = prod[k * CH:(k + 1) * CH].astype(BF16)

    def pm_copy(r):
        if r == 0:
            src, dst, dev = pm.at[1 - c], pm_in, mate
        else:
            src, dst, dev = pm_out.at[r - 1], pm_got.at[r - 1], (sp, ((y + r) % NY) * 2 + c)
        return pltpu.make_async_remote_copy(
            src_ref=src, dst_ref=dst, send_sem=p_snd, recv_sem=p_rcv.at[r],
            device_id=dev, device_id_type=MESH,
        )

    def sum_copy(r):
        return pltpu.make_async_remote_copy(
            src_ref=sums, dst_ref=sums_in.at[r - 1], send_sem=s_snd, recv_sem=s_rcv,
            device_id=peers[r - 1], device_id_type=MESH,
        )

    pm_copy(0).start()
    for r in range(1, N_TP):
        sum_copy(r).start()

    pm_copy(0).wait_recv()
    for r in (2, 1, 3):
        at = (y + r) % NY
        pm_out[r - 1] = (pm[c, at].astype(F32) + pm_in[at].astype(F32)).astype(BF16)
        pm_copy(r).start()
    mixed_grad = pm[c, y].astype(F32) + pm_in[y].astype(F32)
    first, second = sums[0:1, :], sums[1:2, :]
    whole(sums_in, s_rcv)
    for r in range(1, N_TP):
        first = first + sums_in[r - 1, 0:1, :]
        second = second + sums_in[r - 1, 1:2, :]
    for r in (1, 3, 2):
        pm_copy(r).wait_recv()
        mixed_grad = mixed_grad + pm_got[r - 1].astype(F32)
    mean, inv = stat[0:1, :], stat[1:2, :]
    normed = (conv_all[tp].astype(F32) - mean) * inv
    grad_normed = mixed_grad * hh[tp]
    conv_grad[:, 0:TOK] = inv * (grad_normed - first / CW - normed * (second / CW))
    halo = pltpu.make_async_remote_copy(
        src_ref=conv_grad.at[:, pl.ds(0, 128)], dst_ref=conv_grad.at[:, pl.ds(TOK, 128)],
        send_sem=h_snd, recv_sem=h_rcv, device_id=((sp + N_SP - 1) % N_SP, tp), device_id_type=MESH,
    )
    halo.start()

    whole(gt_in.at[pl.ds(1, N_SP - 1)], o_rcv)
    owned = gt[block_at(z), x].astype(F32)
    for p in range(N_SP):
        if p != OWN:
            owned = owned + gt_in[p].astype(F32)
    gt_out[...] = owned
    owner_copy = pltpu.make_async_remote_copy(
        src_ref=gt_out, dst_ref=gt_got, send_sem=f_snd, recv_sem=f_rcv,
        device_id=(tp * NX + x, block_at(z)), device_id_type=MESH,
    )
    owner_copy.start()

    halo.wait_recv()
    tail = conv_grad[:, TOK:TOK + 128]
    wide = jnp.concatenate([conv_grad[:, 0:TOK], jnp.where(sp == N_SP - 1, 0.0, tail)], axis=1)
    taps_t = jnp.concatenate([taps_v[...], jnp.zeros((1, CH), F32)], axis=0).T
    glu = taps_t[:, 0:1] * wide[:, 0:TOK]
    for offset in range(1, KW):
        glu = glu + taps_t[:, offset:offset + 1] * pltpu.roll(wide, TOK + 128 - offset, 1)[:, 0:TOK]
    gate_sig = jax.nn.sigmoid(gate_v[...].astype(F32))
    gv_ref[...] = (glu * gate_sig).astype(BF16)
    gq_ref[...] = (glu * value_v[...].astype(F32) * gate_sig * (1.0 - gate_sig)).astype(BF16)

    owner_copy.wait_recv()
    owner_copy.wait_send()
    got_t = gt_got[...].T
    go_ref[:, 0:CH // 2] = got_t[0:CH]
    go_ref[:, CH // 2:CH] = got_t[CH:2 * CH]
    outs.extend([
        pltpu.make_async_copy(gs_ref, gs_out, out_sem.at[0]),
        pltpu.make_async_copy(gv_ref, gv_out, out_sem.at[1]),
        pltpu.make_async_copy(gq_ref, gq_out, out_sem.at[2]),
        pltpu.make_async_copy(go_ref, go_out, out_sem.at[3]),
    ])
    for copy in outs[3:]:
        copy.start()
    whole(send.at[pl.ds(1, N_SP - 1)], a_snd.at[0])
    whole(send_o.at[pl.ds(1, len(SECOND) - 1)], a_snd.at[1])
    whole(row_out.at[pl.ds(1, N_SP - 1)], b_snd)
    whole(gt_in.at[pl.ds(1, N_SP - 1)], o_snd)

    whole(xs.at[:, pl.ds(0, 7), pl.ds(0, 512), :], g_snd.at[0])
    whole(xs.at[:, pl.ds(0, 6), pl.ds(0, 512), :], g_snd.at[1])
    whole(xs.at[0, pl.ds(0, 7)], r_snd)
    whole(conv_all.at[pl.ds(0, 7)], p_snd)
    whole(sums_in, s_snd)
    whole(proj_all.at[pl.ds(0, N_TP - 1), pl.ds(0, CH // NX), :], j_snd)
    whole(proj_all.at[:, pl.ds(0, 3 * CH // NX), :], k_snd)
    whole(conv_all.at[pl.ds(0, 7)], e_snd)
    for copy in outs:
        copy.wait()
    halo.wait_send()


RESULTS = (
    ((TOK, SL), BF16),
    ((CH, TOK), BF16),
    ((CH, TOK), BF16),
    ((CH, CH), F32),
    ((N_TP, SL, SL), F32),
    ((N_TP, SL, SL), F32),
    ((SL, N_TP * SL), F32),
)


def store_kernel(*refs):
    n = len(RESULTS)
    sems = refs[-1]
    copies = [pltpu.make_async_copy(refs[i], refs[n + i], sems.at[i]) for i in range(n)]
    for copy in copies:
        copy.start()
    for copy in copies:
        copy.wait()


def store_call(*results):
    return pl.pallas_call(
        store_kernel,
        out_shape=tuple(jax.ShapeDtypeStruct(shape, dtype) for shape, dtype in RESULTS),
        in_specs=[pl.BlockSpec(memory_space=pltpu.VMEM)] * len(RESULTS),
        out_specs=(pl.BlockSpec(memory_space=pl.ANY),) * len(RESULTS),
        scratch_shapes=[pltpu.SemaphoreType.DMA((len(RESULTS),))],
        compiler_params=pltpu.CompilerParams(vmem_limit_bytes=2 * 1024 * 1024),
        name="store_results",
    )(*(pltpu.with_memory_space_constraint(r, pltpu.VMEM) for r in results))


def main_call(*operands):
    any_spec = pl.BlockSpec(memory_space=pltpu.HBM)
    flops = 2 * N_SP * CAP * 2048 * 256 * 8
    V = pltpu.VMEM
    D = pltpu.SemaphoreType.DMA
    return pl.pallas_call(
        main_kernel,
        out_shape=tuple(V(shape, dtype) for shape, dtype in RESULTS),
        in_specs=[any_spec] * 12,
        out_specs=(pl.BlockSpec(memory_space=pl.ANY),) * 7,
        scratch_shapes=[V(shape, dtype) for shape, dtype in RESULTS] + [
            V((TOK, SL), BF16),
            V((TOK, SL), BF16),
            V((TOK, SL), BF16),
            V((TOK, SL), BF16),
            V((2, TOK), jnp.int32),
            V((2, TOK), F32),
            V((N_TP, SL, SL), BF16),
            V((N_TP, SL, SL), BF16),
            V((N_TP, SL, SL), BF16),
            V((N_SP, 2, CAP, SL), BF16),
            V((len(SECOND), 2, CAP, SL), BF16),
            V((2, N_TP, N_SP * CAP, SL), BF16),
            V((TOK, N_SP * CAP), BF16),
            V((NC, 2, NY, MAX, SL), BF16),
            V((NC, NY, MAX, SL), BF16),
            V((NC, NY, MAX, SL), BF16),
            V((NC, 6, MAX // 2, SL), BF16),
            V((NC, 2, MAX // 2, SL), BF16),
            V((N_SP, CAP, SL), BF16),
            V((N_SP, CAP, SL), BF16),
            V((N_SP * CAP, SL), BF16),
            V((N_SP * CAP, SL), BF16),
            V((N_SP * CAP, SL), BF16),
            V((CH, TOK), BF16),
            V((CH, TOK), BF16),
            V((KW, CH), F32),
            V((N_TP, CH, TOK), BF16),
            V((N_TP, CH, SL), BF16),
            V((N_TP, CH, TOK), F32),
            V((N_TP, CH, TOK), F32),
            V((N_TP, CH, TOK), BF16),
            V((8, TOK), F32),
            V((2, NY, CH, TOK), BF16),
            V((NY, CH, TOK), BF16),
            V((NY - 1, CH, TOK), BF16),
            V((NY - 1, CH, TOK), BF16),
            V((8, TOK), F32),
            V((N_TP - 1, 8, TOK), F32),
            V((CH, TOK + 128), F32),
            V((N_TP, NX, CH // 2, 128), BF16),
            V((N_SP, CH // 2, 128), BF16),
            V((CH // 2, 128), F32),
            V((CH // 2, 128), F32),
            pltpu.SemaphoreType.REGULAR((3,)),
            D((14,)),
            D((7,)),
            D((2,)),
            D((NC,)),
            D((NC,)),
            D((2,)),
            D((NC, 4)),
            D,
            D((NC, 4)),
            D,
            D((NC,)),
            D,
            D((7,)),
            D,
            D,
            D,
            D,
            D,
            D((NY,)),
            D,
            D,
            D,
            D,
            D,
            D,
            D,
            D,
        ],
        compiler_params=pltpu.CompilerParams(
            collective_id=0, has_side_effects=True, vmem_limit_bytes=54 * 1024 * 1024
        ),
        cost_estimate=pl.CostEstimate(flops=flops, bytes_accessed=16 << 20, transcendentals=0),
        name="routed_experts",
    )(*operands)


def on_device(
    upstream,
    stream,
    routes,
    route_weights,
    glu_value,
    glu_gate,
    conv_taps,
    conv_saved,
    out_proj,
    expert_gate,
    expert_up,
    expert_down,
):
    grad_stream, grad_value, grad_gate, grad_out_proj, grad_gate_w, grad_up_w, grad_down_w = store_call(*main_call(
        upstream, stream, routes.T, route_weights.T,
        expert_gate.reshape(N_TP, SL, SL), expert_up.reshape(N_TP, SL, SL), expert_down[0],
        glu_value.T, glu_gate.T, conv_taps, conv_saved.T, out_proj.T,
    ))
    return (
        grad_stream,
        grad_value.T,
        grad_gate.T,
        grad_out_proj,
        grad_gate_w.reshape(1, N_TP * SL, SL),
        grad_up_w.reshape(1, N_TP * SL, SL),
        grad_down_w[None],
    )


def solution(mesh):
    in_specs = (
        P("sp", None),
        P("sp", None),
        P("sp", None),
        P("sp", None),
        P("sp", "tp"),
        P("sp", "tp"),
        P(None, "tp"),
        P("sp", "tp"),
        P(None, "tp"),
        P("sp", None, "tp"),
        P("sp", None, "tp"),
        P("sp", "tp", None),
    )
    out_specs = (
        P("sp", "tp"),
        P("sp", "tp"),
        P("sp", "tp"),
        P("sp", "tp"),
        P("sp", None, "tp"),
        P("sp", None, "tp"),
        P("sp", "tp", None),
    )
    return jax.shard_map(
        on_device, mesh=mesh, in_specs=in_specs, out_specs=out_specs, check_vma=False
    )
```

```python
import jax
import jax.numpy as jnp
from jax import lax
from jax.experimental import pallas as pl
from jax.experimental.pallas import tpu as pltpu
from jax.sharding import PartitionSpec as P

MESH = pl.DeviceIdType.MESH
BF16 = jnp.bfloat16
F32 = jnp.float32

CW = 512
NZ, NX, NY = 8, 4, 4
N_SP = 32
N_TP = 8
CAP = 32
TOK = 256
SL = 256
CHUNKS = ((0, 4), (4, 8), (12, 8), (20, 8), (28, 4))
NC = len(CHUNKS)
MAX = 8 * CAP

clamp_limit = 7.0
glu_alpha = 1.702
norm_eps = 1e-05

OFFSETS = (
    ((0, 0), (1, 0), (7, 0), (0, 1))
    + ((0, 3), (0, 2), (1, 1), (7, 1), (1, 3), (7, 3), (2, 0), (6, 0))
    + ((4, 0), (4, 1), (4, 2), (4, 3), (1, 2), (7, 2), (2, 2), (6, 2))
    + ((3, 0), (5, 0), (3, 1), (5, 1), (3, 2), (5, 2), (3, 3), (5, 3))
    + ((2, 1), (6, 1), (2, 3), (6, 3))
)
DIRECT = (0, 3, 4)
SECOND = {p: i for i, p in enumerate(p for k in DIRECT for p in range(CHUNKS[k][0], sum(CHUNKS[k])))}
OWN = 0


def far_first(positions):
    hops = lambda p: min(OFFSETS[p][0], 8 - OFFSETS[p][0]) + min(OFFSETS[p][1], 4 - OFFSETS[p][1])
    return sorted(positions, key=lambda p: (-hops(p), p))


G_SLOT = (0, 1, 3, 1, 0, 3, 2, 2, 3, 3, 3, 3, 3, 3)
CH = 64
KW = 31


def dot_tn(left, right):
    return lax.dot_general(left, right, (((0,), (0,)), ((), ())), preferred_element_type=F32)


def dot_nt(left, right):
    return lax.dot_general(left, right, (((1,), (1,)), ((), ())), preferred_element_type=F32)


def dot_nn(left, right):
    return lax.dot_general(left, right, (((1,), (0,)), ((), ())), preferred_element_type=F32)


def main_kernel(
    up_hbm, st_hbm, routes_hbm, weights_hbm, wg_hbm, wu_hbm, wd_hbm,
    value_hbm, gate_hbm, taps_hbm, conv_hbm, proj_hbm,
    gs_out, gv_out, gq_out, go_out, gg_out, gu_out, gd_out,
    gs_ref, gv_ref, gq_ref, go_ref, acc_g, acc_u, acc_d,
    up_v, st_v, up_o, st_o, routes_v, weights_v, wg, wu, wd, send, send_o, xs, onehot, part, part_in, comb, ring_in, relay,
    row_out, ret, ggp, gup, act,
    value_v, gate_v, taps_v, conv_all, proj_all, hh, hn, mix, stat,
    pm, pm_in, pm_out, pm_got, sums, sums_in, conv_grad, gt, gt_in, gt_out, gt_got,
    far_sem, load_sem, out_sem, a_snd, a_rcv, ao_rcv, g_snd, g_rcv, r_snd, r_rcv, b_snd, b_rcv,
    e_snd, e_rcv, j_snd, j_rcv, k_snd, k_rcv, p_snd, p_rcv, s_snd, s_rcv, h_snd, h_rcv, o_snd, o_rcv, f_snd, f_rcv,
):
    sp = lax.axis_index("sp")
    tp = lax.axis_index("tp")
    z, x = sp // NX, sp % NX
    y, c = tp // 2, tp % 2
    fwd, bwd = ((y + 1) % NY) * 2 + c, ((y + 3) % NY) * 2 + c
    opp = ((y + 2) % NY) * 2 + c
    other = y * 2 + (1 - c)
    up_dev, down_dev, mate = (sp, fwd), (sp, bwd), (sp, other)
    oc = 1 - c
    fwd_o, bwd_o, opp_o = ((y + 1) % NY) * 2 + oc, ((y + 3) % NY) * 2 + oc, ((y + 2) % NY) * 2 + oc

    def sp_dev(p, sign):
        dz, dx = OFFSETS[p]
        if sign < 0:
            dz, dx = (NZ - dz) % NZ, (NX - dx) % NX
        return (((z + dz) % NZ) * NX + (x + dx) % NX, tp)

    def whole(ref, sem):
        pltpu.make_async_copy(ref, ref, sem).wait()

    chunk_of = [k for k, (_, count) in enumerate(CHUNKS) for _ in range(count)]
    column = pl.multiple_of(tp * SL, SL)
    column_o = pl.multiple_of(opp * SL, SL)
    quarter = pl.ds(pl.multiple_of(x * (CH // NX), CH // NX), CH // NX)
    loads = [
        pltpu.make_async_copy(st_hbm.at[:, pl.ds(column, SL)], st_v, load_sem.at[0]),
        pltpu.make_async_copy(up_hbm.at[:, pl.ds(column, SL)], up_v, load_sem.at[1]),
        pltpu.make_async_copy(st_hbm.at[:, pl.ds(column_o, SL)], st_o, load_sem.at[12]),
        pltpu.make_async_copy(up_hbm.at[:, pl.ds(column_o, SL)], up_o, load_sem.at[13]),
        pltpu.make_async_copy(routes_hbm, routes_v, load_sem.at[2]),
        pltpu.make_async_copy(weights_hbm, weights_v, load_sem.at[3]),
    ]
    late = [
        pltpu.make_async_copy(wg_hbm, wg, load_sem.at[4]),
        pltpu.make_async_copy(wu_hbm, wu, load_sem.at[5]),
    ]
    for j in range(N_TP):
        late.append(
            pltpu.make_async_copy(wd_hbm.at[:, pl.ds(j * SL, SL)], wd.at[j], load_sem.at[6])
        )
    tail_loads = [
        pltpu.make_async_copy(value_hbm, value_v, load_sem.at[7]),
        pltpu.make_async_copy(gate_hbm, gate_v, load_sem.at[8]),
        pltpu.make_async_copy(taps_hbm, taps_v, load_sem.at[9]),
        pltpu.make_async_copy(conv_hbm, conv_all.at[tp], load_sem.at[10]),
        pltpu.make_async_copy(
            proj_hbm.at[quarter, pl.ds(column, SL)], proj_all.at[tp, quarter], load_sem.at[11]
        ),
    ]
    barrier = pltpu.get_barrier_semaphore()
    peers = [(sp, (tp + r) % N_TP) for r in range(1, N_TP)]
    near = [p for p in range(N_SP) if p != OWN and OFFSETS[p][0] in (0, 1, NZ - 1)]
    for dev in [sp_dev(p, 1) for p in near] + peers:
        pl.semaphore_signal(barrier, inc=1, device_id=dev, device_id_type=MESH)
    for copy in loads:
        copy.start()
    for copy in late + tail_loads:
        copy.start()
    above, below = (((z + 1) % NZ) * NX + x, tp), (((z + NZ - 1) % NZ) * NX + x, tp)

    for copy in loads:
        copy.wait()
    packed = jnp.concatenate(
        [routes_v[...].astype(F32), weights_v[...], jnp.zeros((4, TOK), F32)], axis=0
    ).T
    r0, r1 = packed[:, 0:1].astype(jnp.int32), packed[:, 1:2].astype(jnp.int32)
    experts = lax.broadcasted_iota(jnp.int32, (TOK, N_SP), 1)
    c0 = jnp.where(r0 == experts, 1.0, 0.0).astype(F32)
    c1 = jnp.where(r1 == experts, 1.0, 0.0).astype(F32)
    tri = jnp.where(
        lax.broadcasted_iota(jnp.int32, (TOK, TOK), 1) < lax.broadcasted_iota(jnp.int32, (TOK, TOK), 0),
        1.0, 0.0,
    ).astype(BF16)
    expert = lax.broadcasted_iota(jnp.int32, (8, N_SP), 1)
    offset_of = (((expert >> 2) - z) & (NZ - 1)) * NX + (((expert & 3) - x) & (NX - 1))
    first_slot = jnp.zeros((8, N_SP), F32)
    for p, (dz, dx) in enumerate(OFFSETS):
        first_slot = first_slot + jnp.where(offset_of == dz * NX + dx, float(p * CAP), 0.0)
    slots = dot_nn(tri, (c0 + c1).astype(BF16)) + first_slot[0:1, :]
    pos0 = jnp.sum(slots * c0, axis=1, keepdims=True).astype(jnp.int32)
    pos1 = jnp.sum(slots * c1, axis=1, keepdims=True).astype(jnp.int32)
    stream = st_v[...]
    ups = up_v[...].astype(F32)
    cot0 = (packed[:, 2:3] * ups).astype(BF16)
    cot1 = (packed[:, 3:4] * ups).astype(BF16)
    stream_o = st_o[...]
    ups_o = up_o[...].astype(F32)
    cot0_o = (packed[:, 2:3] * ups_o).astype(BF16)
    cot1_o = (packed[:, 3:4] * ups_o).astype(BF16)

    def a2a(p):
        return pltpu.make_async_remote_copy(
            src_ref=send.at[p],
            dst_ref=xs.at[:, tp, pl.ds(p * CAP, CAP), :],
            send_sem=a_snd.at[0],
            recv_sem=a_rcv.at[chunk_of[p]],
            device_id=sp_dev(p, 1),
            device_id_type=MESH,
        )

    def a2a_o(p):
        return pltpu.make_async_remote_copy(
            src_ref=send_o.at[SECOND[p]],
            dst_ref=xs.at[:, opp, pl.ds(p * CAP, CAP), :],
            send_sem=a_snd.at[1],
            recv_sem=ao_rcv.at[chunk_of[p]],
            device_id=sp_dev(p, 1),
            device_id_type=MESH,
        )

    conv_plan = ((tp, up_dev), (tp, down_dev), (tp, (sp, opp)), (tp, mate), (bwd, mate), (fwd, mate), (opp, mate))
    conv_arrives = (bwd, fwd, opp, other, bwd_o, fwd_o, opp_o)

    def conv_copy(kind, arriving=False):
        at, dev = conv_plan[kind]
        if arriving:
            at = conv_arrives[kind]
        return pltpu.make_async_remote_copy(
            src_ref=conv_hbm if kind < 4 else conv_all.at[at], dst_ref=conv_all.at[at],
            send_sem=e_snd, recv_sem=e_rcv.at[kind], device_id=dev, device_id_type=MESH,
        )

    def proj_copy(r):
        at = pl.multiple_of(((tp + r) % N_TP) * SL, SL)
        return pltpu.make_async_remote_copy(
            src_ref=proj_hbm.at[quarter, pl.ds(at, SL)], dst_ref=proj_all.at[tp, quarter],
            send_sem=j_snd, recv_sem=j_rcv, device_id=peers[r - 1], device_id_type=MESH,
        )

    def quarter_copy(d):
        return pltpu.make_async_remote_copy(
            src_ref=proj_all.at[:, quarter, :], dst_ref=proj_all.at[:, quarter, :],
            send_sem=k_snd, recv_sem=k_rcv,
            device_id=(z * NX + (x + d) % NX, tp), device_id_type=MESH,
        )

    def stage_s(k):
        start, count = CHUNKS[k]
        width = count * CAP
        lanes = lax.broadcasted_iota(jnp.int32, (TOK, width), 1) + start * CAP
        s0 = jnp.where(pos0 == lanes, 1.0, 0.0).astype(BF16)
        s1 = jnp.where(pos1 == lanes, 1.0, 0.0).astype(BF16)
        both = s0 + s1
        onehot[:, start * CAP:start * CAP + width] = both
        rows = dot_tn(both, stream).astype(BF16)
        cots = (dot_tn(s0, cot0) + dot_tn(s1, cot1)).astype(BF16)
        send[start:start + count, 0] = rows.reshape(count, CAP, SL)
        send[start:start + count, 1] = cots.reshape(count, CAP, SL)
        if k in DIRECT:
            at = SECOND[start]
            rows = dot_tn(both, stream_o).astype(BF16)
            cots = (dot_tn(s0, cot0_o) + dot_tn(s1, cot1_o)).astype(BF16)
            send_o[at:at + count, 0] = rows.reshape(count, CAP, SL)
            send_o[at:at + count, 1] = cots.reshape(count, CAP, SL)

    def stage_go(k):
        start, count = CHUNKS[k]
        for p in range(start, start + count):
            if p == OWN:
                xs[:, tp, pl.ds(p * CAP, CAP), :] = send[p]
                xs[:, opp, pl.ds(p * CAP, CAP), :] = send_o[SECOND[p]]
            else:
                a2a(p).start()

    def stage_ox(k):
        start, count = CHUNKS[k]
        for p in range(max(start, 1), start + count):
            a2a_o(p).start()

    def farther(step):
        for dev in (above, below):
            pl.semaphore_signal(far_sem.at[step], inc=1, device_id=dev, device_id_type=MESH)

    def stage_f(step):
        pl.semaphore_wait(far_sem.at[step], 2)
        if step < 2:
            farther(step + 1)

    stage_s(0)
    stage_s(1)
    pl.semaphore_wait(barrier, len(near) + N_TP - 1)
    farther(0)
    stage_go(0)
    stage_ox(0)
    for kind in range(4):
        conv_copy(kind).start()
    for r in range(1, N_TP):
        proj_copy(r).start()
    stage_f(0)
    stage_go(1)
    stage_s(2)
    stage_f(1)
    stage_f(2)

    @pl.when(c == 0)
    def _():
        stage_go(2)


    def gather(k, kind, rc, slice_at, dev):
        start, count = CHUNKS[k]
        ref = xs.at[rc, slice_at, pl.ds(start * CAP, count * CAP), :]
        return pltpu.make_async_remote_copy(
            src_ref=ref, dst_ref=ref, send_sem=g_snd.at[1 if k in DIRECT else 0], recv_sem=g_rcv.at[k, G_SLOT[kind]],
            device_id=dev, device_id_type=MESH,
        )

    plan = (
        (0, tp, up_dev), (0, tp, down_dev), (0, tp, mate),
        (1, tp, up_dev), (1, tp, down_dev), (1, tp, mate),
        (0, bwd, up_dev), (1, fwd, down_dev),
        (0, bwd, mate), (0, fwd, mate), (0, opp, mate),
        (1, fwd, mate), (1, bwd, mate), (1, opp, mate),
    )

    def spread(k, kind):
        rc, slice_at, dev = plan[kind]
        return gather(k, kind, rc, slice_at, dev)

    def both(k, slot):
        start, count = CHUNKS[k]
        whole(xs.at[:, tp, pl.ds(start * CAP, count * CAP), :], g_rcv.at[k, slot])

    def stage_a(k):
        start, count = CHUNKS[k]
        begin = max(start, 1)
        whole(xs.at[:, tp, pl.ds(begin * CAP, (start + count - begin) * CAP), :], a_rcv.at[k])
        for kind in (0, 4, 3, 1, 2, 5):
            spread(k, kind).start()

    def opposite(k):
        start, count = CHUNKS[k]
        begin = max(start, 1)
        whole(xs.at[:, opp, pl.ds(begin * CAP, (start + count - begin) * CAP), :], ao_rcv.at[k])
        spread(k, 10).start()
        spread(k, 13).start()

    def stage_b1(k):
        both(k, 0)
        for kind in (8, 11) if k in DIRECT else (6, 7, 8, 11):
            spread(k, kind).start()

    def stage_b2(k):
        both(k, 1)
        spread(k, 9).start()
        spread(k, 12).start()
        if k in DIRECT:
            opposite(k)
        else:
            both(k, 2)
            spread(k, 10).start()
            spread(k, 13).start()

    def stage_b3(k):
        start, count = CHUNKS[k]
        whole(xs.at[:, pl.ds(0, NY), pl.ds(start * CAP, count * CAP), :], g_rcv.at[k, 3])

    def swap(k):
        return pltpu.make_async_remote_copy(
            src_ref=part.at[k, 1 - c, :, pl.ds(0, CHUNKS[k][1] * CAP), :],
            dst_ref=part_in.at[k, :, pl.ds(0, CHUNKS[k][1] * CAP), :],
            send_sem=r_snd, recv_sem=r_rcv.at[k, 0], device_id=mate, device_id_type=MESH,
        )

    def stage_c(k):
        start, count = CHUNKS[k]
        size = count * CAP
        rows = pl.ds(start * CAP, size)
        gate_pre = jnp.zeros((size, SL), F32)
        up_pre = jnp.zeros((size, SL), F32)
        grad_act = jnp.zeros((size, SL), F32)
        for j in range(N_TP):
            r = xs[0, j, rows, :]
            gate_pre = gate_pre + dot_nn(r, wg[j])
            up_pre = up_pre + dot_nn(r, wu[j])
            grad_act = grad_act + dot_nt(xs[1, j, rows, :], wd[j])
        capped = jnp.minimum(gate_pre, clamp_limit)
        clipped = jnp.clip(up_pre, -clamp_limit, clamp_limit)
        sig = jax.nn.sigmoid(glu_alpha * capped)
        act[rows, :] = (capped * sig * (clipped + 1.0)).astype(BF16)
        slope = sig + glu_alpha * capped * sig * (1.0 - sig)
        g_gate = jnp.where(gate_pre < clamp_limit, grad_act * (clipped + 1.0) * slope, 0.0).astype(BF16)
        g_up = jnp.where(jnp.abs(up_pre) < clamp_limit, grad_act * capped * sig, 0.0).astype(BF16)
        ggp[rows, :] = g_gate
        gup[rows, :] = g_up
        for i in range(N_TP):
            core, at = (1 - c, i) if i < NY else (c, i - NY)
            total = dot_nt(g_gate, wg[2 * at + core]) + dot_nt(g_up, wu[2 * at + core])
            part[k, core, at, 0:size] = total.astype(BF16)
            if i == NY - 1:
                swap(k).start()

    def stage_w(start, stop):
        rows = pl.ds(start, stop - start)

        def grads(j, carry):
            r = xs[0, j, rows, :]
            at = pl.ds(pl.multiple_of(j * SL, SL), SL)
            g, u = dot_tn(r, ggp[rows, :]), dot_tn(r, gup[rows, :])
            d = dot_tn(act[rows, :], xs[1, j, rows, :])
            if start == 0:
                acc_g[j], acc_u[j], acc_d[:, at] = g, u, d
            else:
                acc_g[j] += g
                acc_u[j] += u
                acc_d[:, at] += d
            return carry

        lax.fori_loop(0, N_TP, grads, 0)

    def halves(k):
        half = CHUNKS[k][1] * CAP // 2
        return pl.ds(0, half), pl.ds(half, half)

    def ring(k, kind, src, slot, dev):
        return pltpu.make_async_remote_copy(
            src_ref=src, dst_ref=ring_in.at[k, slot, halves(k)[0], :],
            send_sem=r_snd, recv_sem=r_rcv.at[k, min(kind, 3)], device_id=dev, device_id_type=MESH,
        )

    def rings(k, kind):
        lo, hi = halves(k)
        if kind == 0:
            return swap(k)
        if kind == 1:
            return ring(k, 1, comb.at[k, 2, lo, :], 0, down_dev)
        if kind == 2:
            return ring(k, 2, comb.at[k, 2, hi, :], 1, up_dev)
        if kind == 3:
            return ring(k, 3, comb.at[k, 1, lo, :], 2, up_dev)
        if kind == 4:
            return ring(k, 4, comb.at[k, 3, hi, :], 3, down_dev)
        if kind == 5:
            return ring(k, 5, relay.at[k, 0, lo, :], 4, down_dev)
        return ring(k, 6, relay.at[k, 1, lo, :], 5, up_dev)

    def straight(k, r):
        size = CHUNKS[k][1] * CAP
        return pltpu.make_async_remote_copy(
            src_ref=comb.at[k, r, pl.ds(0, size), :], dst_ref=ring_in.at[k, r - 1, pl.ds(0, size), :],
            send_sem=r_snd, recv_sem=r_rcv.at[k, 3],
            device_id=(sp, ((y + r) % NY) * 2 + c), device_id_type=MESH,
        )

    def stage_last():
        k = NC - 1
        size = CHUNKS[k][1] * CAP
        swap(k).wait_recv()
        for r in (2, 1, 3, 0):
            at = (y + r) % NY
            pair = part[k, c, at, 0:size].astype(F32) + part_in[k, at, 0:size].astype(F32)
            comb[k, r, 0:size] = pair.astype(BF16)
            if r > 0:
                straight(k, r).start()

    def stage_end():
        k = NC - 1
        at, count = CHUNKS[k]
        size = count * CAP
        whole(ring_in.at[k, pl.ds(0, 3), pl.ds(0, size), :], r_rcv.at[k, 3])
        total = comb[k, 0, 0:size].astype(F32)
        for r in range(1, NY):
            total = total + ring_in[k, r - 1, 0:size].astype(F32)
        row_out[at:at + count] = total.astype(BF16).reshape(count, CAP, SL)
        for p in far_first(range(at, at + count)):
            back_copy(p).start()

    def stage_d(k):
        rings(k, 0).wait_recv()
        size = CHUNKS[k][1] * CAP
        for r in (2, 1, 3, 0):
            at = (y + r) % NY
            both = part[k, c, at, 0:size].astype(F32) + part_in[k, at, 0:size].astype(F32)
            comb[k, r, 0:size] = both.astype(BF16)
            if r == 2:
                rings(k, 1).start()
                rings(k, 2).start()
        rings(k, 3).start()
        rings(k, 4).start()

    def stage_e1(k):
        rings(k, 1).wait_recv()
        lo, hi = halves(k)
        relay[k, 0, lo, :] = (ring_in[k, 0, lo, :].astype(F32) + comb[k, 3, lo, :].astype(F32)).astype(BF16)
        rings(k, 5).start()
        rings(k, 2).wait_recv()
        relay[k, 1, lo, :] = (ring_in[k, 1, lo, :].astype(F32) + comb[k, 1, hi, :].astype(F32)).astype(BF16)
        rings(k, 6).start()

    def back_copy(p):
        return pltpu.make_async_remote_copy(
            src_ref=row_out.at[p], dst_ref=ret.at[p],
            send_sem=b_snd, recv_sem=b_rcv.at[chunk_of[p]], device_id=sp_dev(p, -1), device_id_type=MESH,
        )

    def stage_e2(k):
        lo, hi = halves(k)
        whole(ring_in.at[k, pl.ds(2, 4), lo, :], r_rcv.at[k, 3])
        low = comb[k, 0, lo, :].astype(F32) + ring_in[k, 2, lo, :].astype(F32) + ring_in[k, 4, lo, :].astype(F32)
        high = comb[k, 0, hi, :].astype(F32) + ring_in[k, 3, lo, :].astype(F32) + ring_in[k, 5, lo, :].astype(F32)
        at, count = CHUNKS[k]
        row_out[at:at + count // 2] = low.astype(BF16).reshape(count // 2, CAP, SL)
        row_out[at + count // 2:at + count] = high.astype(BF16).reshape(count // 2, CAP, SL)
        for p in far_first(range(at, at + count)):
            if p == OWN:
                ret[p] = row_out[p]
            else:
                back_copy(p).start()

    def stage_m():
        for copy in tail_loads:
            copy.wait()
        for kind in range(3):
            conv_copy(kind, True).wait_recv()
            conv_copy(kind + 4).start()
        whole(proj_all.at[pl.ds(0, N_TP - 1), pl.ds(0, CH // NX), :], j_rcv)
        for d in range(1, NX):
            quarter_copy(d).start()

    def stage_n():
        for kind in range(3, 7):
            conv_copy(kind, True).wait_recv()
        total, square = jnp.zeros((1, TOK), F32), jnp.zeros((1, TOK), F32)
        for k in range(N_TP):
            v = conv_all[k].astype(F32)
            total = total + jnp.sum(v, axis=0, keepdims=True)
            square = square + jnp.sum(v * v, axis=0, keepdims=True)
        mean = total / CW
        inv = lax.rsqrt(square / CW - mean * mean + norm_eps)
        stat[0:1, :] = mean
        stat[1:2, :] = inv
        for k in range(N_TP):
            n = (conv_all[k].astype(F32) - mean) * inv
            sig = jax.nn.sigmoid(n)
            slope = sig * (1.0 + n * (1.0 - sig))
            mix[k] = (n * sig).astype(BF16)
            hh[k] = slope
            hn[k] = slope * n

    stage_a(0)
    stage_s(3)
    stage_s(4)
    stage_a(1)

    @pl.when(c == 0)
    def _():
        stage_go(3)
        stage_go(4)
        stage_ox(4)

    @pl.when(c == 1)
    def _():
        stage_go(2)

    stage_b1(0)
    stage_b2(0)
    late[0].wait()
    late[1].wait()
    whole(wd, load_sem.at[6])
    stage_b3(0)
    stage_c(0)
    stage_b1(1)
    stage_d(0)
    stage_a(2)

    @pl.when(c == 1)
    def _():
        stage_go(3)
        stage_go(4)
        stage_ox(4)

    stage_m()
    stage_b2(1)
    stage_b3(1)
    stage_c(1)
    stage_e1(0)
    stage_b1(2)
    stage_d(1)
    stage_a(3)
    stage_ox(3)
    stage_e2(0)
    stage_n()
    stage_w(0, 384)
    stage_b2(2)
    stage_b3(2)
    stage_c(2)
    stage_e1(1)
    stage_b1(3)
    stage_d(2)
    stage_a(4)
    stage_w(384, 640)
    stage_e2(1)
    stage_b2(3)
    stage_b3(3)
    stage_c(3)
    stage_b1(4)
    stage_e1(2)
    stage_d(3)
    stage_b2(4)
    stage_b3(4)
    stage_c(4)
    stage_e2(2)
    stage_e1(3)
    stage_last()
    stage_w(640, 896)
    stage_e2(3)
    stage_end()
    stage_w(896, 1024)
    outs = [
        pltpu.make_async_copy(acc_g, gg_out, out_sem.at[4]),
        pltpu.make_async_copy(acc_u, gu_out, out_sem.at[5]),
        pltpu.make_async_copy(acc_d, gd_out, out_sem.at[6]),
    ]
    for copy in outs:
        copy.start()
    total = up_v[...].astype(F32)
    for start, count in CHUNKS:
        begin = max(start, 1)
        whole(ret.at[pl.ds(begin, start + count - begin)], b_rcv.at[chunk_of[start]])
        picked = onehot[:, start * CAP:(start + count) * CAP]
        total = total + dot_nn(picked, ret[start:start + count].reshape(count * CAP, SL))
    grads = total.astype(BF16)
    gs_ref[...] = grads

    outer = dot_nn(mix[...].reshape(CW, TOK), grads).reshape(N_TP, 2, CH // 2, SL)
    low_half = lax.broadcasted_iota(jnp.int32, (CW // 2, 128), 1) < CH
    for g in range(2):
        upper = outer[:, 0, :, 128 * g:128 * g + 128].reshape(CW // 2, 128)
        lower = outer[:, 1, :, 128 * g:128 * g + 128].reshape(CW // 2, 128)
        even = jnp.where(low_half, upper, pltpu.roll(lower, CH, 1))
        odd = jnp.where(low_half, pltpu.roll(upper, CH, 1), lower)
        gt[:, 2 * g] = even.astype(BF16).reshape(N_TP, CH // 2, 128)
        gt[:, 2 * g + 1] = odd.astype(BF16).reshape(N_TP, CH // 2, 128)
    def block_at(height):
        ahead = (height - tp + NZ) % NZ
        return 2 * ((y + ahead // 2 + 2) % NY) + ahead % 2

    def gt_copy(p):
        dev = sp_dev(p, 1)
        return pltpu.make_async_remote_copy(
            src_ref=gt.at[block_at(dev[0] // NX), dev[0] % NX], dst_ref=gt_in.at[p], send_sem=o_snd, recv_sem=o_rcv,
            device_id=dev, device_id_type=MESH,
        )

    for p in far_first(range(N_SP)):
        if p != OWN:
            gt_copy(p).start()

    whole(proj_all.at[:, pl.ds(0, 3 * CH // NX), :], k_rcv)
    prod = dot_nt(proj_all[...].reshape(CW, SL), grads)
    sums[0:1, :] = jnp.sum(prod * hh[...].reshape(CW, TOK), axis=0, keepdims=True)
    sums[1:2, :] = jnp.sum(prod * hn[...].reshape(CW, TOK), axis=0, keepdims=True)
    for k in range(N_TP):
        pm[k % 2, k // 2] = prod[k * CH:(k + 1) * CH].astype(BF16)

    def pm_copy(r):
        if r == 0:
            src, dst, dev = pm.at[1 - c], pm_in, mate
        else:
            src, dst, dev = pm_out.at[r - 1], pm_got.at[r - 1], (sp, ((y + r) % NY) * 2 + c)
        return pltpu.make_async_remote_copy(
            src_ref=src, dst_ref=dst, send_sem=p_snd, recv_sem=p_rcv.at[r],
            device_id=dev, device_id_type=MESH,
        )

    def sum_copy(r):
        return pltpu.make_async_remote_copy(
            src_ref=sums, dst_ref=sums_in.at[r - 1], send_sem=s_snd, recv_sem=s_rcv,
            device_id=peers[r - 1], device_id_type=MESH,
        )

    pm_copy(0).start()
    for r in range(1, N_TP):
        sum_copy(r).start()

    pm_copy(0).wait_recv()
    for r in (2, 1, 3):
        at = (y + r) % NY
        pm_out[r - 1] = (pm[c, at].astype(F32) + pm_in[at].astype(F32)).astype(BF16)
        pm_copy(r).start()
    mixed_grad = pm[c, y].astype(F32) + pm_in[y].astype(F32)
    first, second = sums[0:1, :], sums[1:2, :]
    whole(sums_in, s_rcv)
    for r in range(1, N_TP):
        first = first + sums_in[r - 1, 0:1, :]
        second = second + sums_in[r - 1, 1:2, :]
    for r in (1, 3, 2):
        pm_copy(r).wait_recv()
        mixed_grad = mixed_grad + pm_got[r - 1].astype(F32)
    mean, inv = stat[0:1, :], stat[1:2, :]
    normed = (conv_all[tp].astype(F32) - mean) * inv
    grad_normed = mixed_grad * hh[tp]
    conv_grad[:, 0:TOK] = inv * (grad_normed - first / CW - normed * (second / CW))
    halo = pltpu.make_async_remote_copy(
        src_ref=conv_grad.at[:, pl.ds(0, 128)], dst_ref=conv_grad.at[:, pl.ds(TOK, 128)],
        send_sem=h_snd, recv_sem=h_rcv, device_id=((sp + N_SP - 1) % N_SP, tp), device_id_type=MESH,
    )
    halo.start()

    whole(gt_in.at[pl.ds(1, N_SP - 1)], o_rcv)
    owned = gt[block_at(z), x].astype(F32)
    for p in range(N_SP):
        if p != OWN:
            owned = owned + gt_in[p].astype(F32)
    gt_out[...] = owned
    owner_copy = pltpu.make_async_remote_copy(
        src_ref=gt_out, dst_ref=gt_got, send_sem=f_snd, recv_sem=f_rcv,
        device_id=(tp * NX + x, block_at(z)), device_id_type=MESH,
    )
    owner_copy.start()

    halo.wait_recv()
    tail = conv_grad[:, TOK:TOK + 128]
    wide = jnp.concatenate([conv_grad[:, 0:TOK], jnp.where(sp == N_SP - 1, 0.0, tail)], axis=1)
    taps_t = jnp.concatenate([taps_v[...], jnp.zeros((1, CH), F32)], axis=0).T
    glu = taps_t[:, 0:1] * wide[:, 0:TOK]
    for offset in range(1, KW):
        glu = glu + taps_t[:, offset:offset + 1] * pltpu.roll(wide, TOK + 128 - offset, 1)[:, 0:TOK]
    gate_sig = jax.nn.sigmoid(gate_v[...].astype(F32))
    gv_ref[...] = (glu * gate_sig).astype(BF16)
    gq_ref[...] = (glu * value_v[...].astype(F32) * gate_sig * (1.0 - gate_sig)).astype(BF16)

    owner_copy.wait_recv()
    owner_copy.wait_send()
    got_t = gt_got[...].T
    go_ref[:, 0:CH // 2] = got_t[0:CH]
    go_ref[:, CH // 2:CH] = got_t[CH:2 * CH]
    outs.extend([
        pltpu.make_async_copy(gs_ref, gs_out, out_sem.at[0]),
        pltpu.make_async_copy(gv_ref, gv_out, out_sem.at[1]),
        pltpu.make_async_copy(gq_ref, gq_out, out_sem.at[2]),
        pltpu.make_async_copy(go_ref, go_out, out_sem.at[3]),
    ])
    for copy in outs[3:]:
        copy.start()
    whole(send.at[pl.ds(1, N_SP - 1)], a_snd.at[0])
    whole(send_o.at[pl.ds(1, len(SECOND) - 1)], a_snd.at[1])
    whole(row_out.at[pl.ds(1, N_SP - 1)], b_snd)
    whole(gt_in.at[pl.ds(1, N_SP - 1)], o_snd)

    whole(xs.at[:, pl.ds(0, 7), pl.ds(0, 512), :], g_snd.at[0])
    whole(xs.at[:, pl.ds(0, 6), pl.ds(0, 512), :], g_snd.at[1])
    whole(xs.at[0, pl.ds(0, 7)], r_snd)
    whole(conv_all.at[pl.ds(0, 7)], p_snd)
    whole(sums_in, s_snd)
    whole(proj_all.at[pl.ds(0, N_TP - 1), pl.ds(0, CH // NX), :], j_snd)
    whole(proj_all.at[:, pl.ds(0, 3 * CH // NX), :], k_snd)
    whole(conv_all.at[pl.ds(0, 7)], e_snd)
    for copy in outs:
        copy.wait()
    halo.wait_send()


RESULTS = (
    ((TOK, SL), BF16),
    ((CH, TOK), BF16),
    ((CH, TOK), BF16),
    ((CH, CH), F32),
    ((N_TP, SL, SL), F32),
    ((N_TP, SL, SL), F32),
    ((SL, N_TP * SL), F32),
)


def store_kernel(*refs):
    n = len(RESULTS)
    sems = refs[-1]
    copies = [pltpu.make_async_copy(refs[i], refs[n + i], sems.at[i]) for i in range(n)]
    for copy in copies:
        copy.start()
    for copy in copies:
        copy.wait()


def store_call(*results):
    return pl.pallas_call(
        store_kernel,
        out_shape=tuple(jax.ShapeDtypeStruct(shape, dtype) for shape, dtype in RESULTS),
        in_specs=[pl.BlockSpec(memory_space=pltpu.VMEM)] * len(RESULTS),
        out_specs=(pl.BlockSpec(memory_space=pl.ANY),) * len(RESULTS),
        scratch_shapes=[pltpu.SemaphoreType.DMA((len(RESULTS),))],
        compiler_params=pltpu.CompilerParams(vmem_limit_bytes=2 * 1024 * 1024),
        name="store_results",
    )(*(pltpu.with_memory_space_constraint(r, pltpu.VMEM) for r in results))


def main_call(*operands):
    any_spec = pl.BlockSpec(memory_space=pltpu.HBM)
    flops = 2 * N_SP * CAP * 2048 * 256 * 8
    V = pltpu.VMEM
    D = pltpu.SemaphoreType.DMA
    return pl.pallas_call(
        main_kernel,
        out_shape=tuple(V(shape, dtype) for shape, dtype in RESULTS),
        in_specs=[any_spec] * 12,
        out_specs=(pl.BlockSpec(memory_space=pl.ANY),) * 7,
        scratch_shapes=[V(shape, dtype) for shape, dtype in RESULTS] + [
            V((TOK, SL), BF16),
            V((TOK, SL), BF16),
            V((TOK, SL), BF16),
            V((TOK, SL), BF16),
            V((2, TOK), jnp.int32),
            V((2, TOK), F32),
            V((N_TP, SL, SL), BF16),
            V((N_TP, SL, SL), BF16),
            V((N_TP, SL, SL), BF16),
            V((N_SP, 2, CAP, SL), BF16),
            V((len(SECOND), 2, CAP, SL), BF16),
            V((2, N_TP, N_SP * CAP, SL), BF16),
            V((TOK, N_SP * CAP), BF16),
            V((NC, 2, NY, MAX, SL), BF16),
            V((NC, NY, MAX, SL), BF16),
            V((NC, NY, MAX, SL), BF16),
            V((NC, 6, MAX // 2, SL), BF16),
            V((NC, 2, MAX // 2, SL), BF16),
            V((N_SP, CAP, SL), BF16),
            V((N_SP, CAP, SL), BF16),
            V((N_SP * CAP, SL), BF16),
            V((N_SP * CAP, SL), BF16),
            V((N_SP * CAP, SL), BF16),
            V((CH, TOK), BF16),
            V((CH, TOK), BF16),
            V((KW, CH), F32),
            V((N_TP, CH, TOK), BF16),
            V((N_TP, CH, SL), BF16),
            V((N_TP, CH, TOK), F32),
            V((N_TP, CH, TOK), F32),
            V((N_TP, CH, TOK), BF16),
            V((8, TOK), F32),
            V((2, NY, CH, TOK), BF16),
            V((NY, CH, TOK), BF16),
            V((NY - 1, CH, TOK), BF16),
            V((NY - 1, CH, TOK), BF16),
            V((8, TOK), F32),
            V((N_TP - 1, 8, TOK), F32),
            V((CH, TOK + 128), F32),
            V((N_TP, NX, CH // 2, 128), BF16),
            V((N_SP, CH // 2, 128), BF16),
            V((CH // 2, 128), F32),
            V((CH // 2, 128), F32),
            pltpu.SemaphoreType.REGULAR((3,)),
            D((14,)),
            D((7,)),
            D((2,)),
            D((NC,)),
            D((NC,)),
            D((2,)),
            D((NC, 4)),
            D,
            D((NC, 4)),
            D,
            D((NC,)),
            D,
            D((7,)),
            D,
            D,
            D,
            D,
            D,
            D((NY,)),
            D,
            D,
            D,
            D,
            D,
            D,
            D,
            D,
        ],
        compiler_params=pltpu.CompilerParams(
            collective_id=0, has_side_effects=True, vmem_limit_bytes=54 * 1024 * 1024
        ),
        cost_estimate=pl.CostEstimate(flops=flops, bytes_accessed=16 << 20, transcendentals=0),
        name="routed_experts",
    )(*operands)


def on_device(
    upstream,
    stream,
    routes,
    route_weights,
    glu_value,
    glu_gate,
    conv_taps,
    conv_saved,
    out_proj,
    expert_gate,
    expert_up,
    expert_down,
):
    grad_stream, grad_value, grad_gate, grad_out_proj, grad_gate_w, grad_up_w, grad_down_w = store_call(*main_call(
        upstream, stream, routes.T, route_weights.T,
        expert_gate.reshape(N_TP, SL, SL), expert_up.reshape(N_TP, SL, SL), expert_down[0],
        glu_value.T, glu_gate.T, conv_taps, conv_saved.T, out_proj.T,
    ))
    return (
        grad_stream,
        grad_value.T,
        grad_gate.T,
        grad_out_proj,
        grad_gate_w.reshape(1, N_TP * SL, SL),
        grad_up_w.reshape(1, N_TP * SL, SL),
        grad_down_w[None],
    )


def solution(mesh):
    in_specs = (
        P("sp", None),
        P("sp", None),
        P("sp", None),
        P("sp", None),
        P("sp", "tp"),
        P("sp", "tp"),
        P(None, "tp"),
        P("sp", "tp"),
        P(None, "tp"),
        P("sp", None, "tp"),
        P("sp", None, "tp"),
        P("sp", "tp", None),
    )
    out_specs = (
        P("sp", "tp"),
        P("sp", "tp"),
        P("sp", "tp"),
        P("sp", "tp"),
        P("sp", None, "tp"),
        P("sp", None, "tp"),
        P("sp", "tp", None),
    )
    return jax.shard_map(
        on_device, mesh=mesh, in_specs=in_specs, out_specs=out_specs, check_vma=False
    )
```

```python
import jax
import jax.numpy as jnp
from jax import lax
from jax.experimental import pallas as pl
from jax.experimental.pallas import tpu as pltpu
from jax.sharding import PartitionSpec as P

MESH = pl.DeviceIdType.MESH
BF16 = jnp.bfloat16
F32 = jnp.float32

CW = 512
NZ, NX, NY = 8, 4, 4
N_SP = 32
N_TP = 8
CAP = 32
TOK = 256
SL = 256
CHUNKS = ((0, 4), (4, 8), (12, 8), (20, 8), (28, 4))
NC = len(CHUNKS)
MAX = 8 * CAP

clamp_limit = 7.0
glu_alpha = 1.702
norm_eps = 1e-05

OFFSETS = (
    ((0, 0), (1, 0), (7, 0), (0, 1))
    + ((0, 3), (0, 2), (1, 1), (7, 1), (1, 3), (7, 3), (2, 0), (6, 0))
    + ((4, 0), (4, 1), (4, 2), (4, 3), (1, 2), (7, 2), (2, 2), (6, 2))
    + ((3, 0), (5, 0), (3, 1), (5, 1), (3, 2), (5, 2), (3, 3), (5, 3))
    + ((2, 1), (6, 1), (2, 3), (6, 3))
)
DIRECT = (0, 3, 4)
SECOND = {p: i for i, p in enumerate(p for k in DIRECT for p in range(CHUNKS[k][0], sum(CHUNKS[k])))}
OWN = 0


def far_first(positions):
    hops = lambda p: min(OFFSETS[p][0], 8 - OFFSETS[p][0]) + min(OFFSETS[p][1], 4 - OFFSETS[p][1])
    return sorted(positions, key=lambda p: (-hops(p), p))


G_SLOT = (0, 1, 3, 1, 0, 3, 2, 2, 3, 3, 3, 3, 3, 3)
CH = 64
KW = 31


def dot_tn(left, right):
    return lax.dot_general(left, right, (((0,), (0,)), ((), ())), preferred_element_type=F32)


def dot_nt(left, right):
    return lax.dot_general(left, right, (((1,), (1,)), ((), ())), preferred_element_type=F32)


def dot_nn(left, right):
    return lax.dot_general(left, right, (((1,), (0,)), ((), ())), preferred_element_type=F32)


def main_kernel(
    up_hbm, st_hbm, routes_hbm, weights_hbm, wg_hbm, wu_hbm, wd_hbm,
    value_hbm, gate_hbm, taps_hbm, conv_hbm, proj_hbm,
    gs_out, gv_out, gq_out, go_out, gg_out, gu_out, gd_out,
    gs_ref, gv_ref, gq_ref, go_ref, acc_g, acc_u, acc_d,
    up_v, st_v, up_o, st_o, routes_v, weights_v, wg, wu, wd, send, send_o, xs, onehot, part, part_in, comb, ring_in, relay,
    row_out, ret, ggp, gup, act,
    value_v, gate_v, taps_v, conv_all, proj_all, hh, hn, mix, stat,
    pm, pm_in, pm_out, pm_got, sums, sums_in, conv_grad, gt, gt_in, gt_out, gt_got,
    far_sem, load_sem, out_sem, a_snd, a_rcv, ao_rcv, g_snd, g_rcv, r_snd, r_rcv, b_snd, b_rcv,
    e_snd, e_rcv, j_snd, j_rcv, k_snd, k_rcv, p_snd, p_rcv, s_snd, s_rcv, h_snd, h_rcv, o_snd, o_rcv, f_snd, f_rcv,
):
    sp = lax.axis_index("sp")
    tp = lax.axis_index("tp")
    z, x = sp // NX, sp % NX
    y, c = tp // 2, tp % 2
    fwd, bwd = ((y + 1) % NY) * 2 + c, ((y + 3) % NY) * 2 + c
    opp = ((y + 2) % NY) * 2 + c
    other = y * 2 + (1 - c)
    up_dev, down_dev, mate = (sp, fwd), (sp, bwd), (sp, other)
    oc = 1 - c
    fwd_o, bwd_o, opp_o = ((y + 1) % NY) * 2 + oc, ((y + 3) % NY) * 2 + oc, ((y + 2) % NY) * 2 + oc

    def sp_dev(p, sign):
        dz, dx = OFFSETS[p]
        if sign < 0:
            dz, dx = (NZ - dz) % NZ, (NX - dx) % NX
        return (((z + dz) % NZ) * NX + (x + dx) % NX, tp)

    def whole(ref, sem):
        pltpu.make_async_copy(ref, ref, sem).wait()

    chunk_of = [k for k, (_, count) in enumerate(CHUNKS) for _ in range(count)]
    column = pl.multiple_of(tp * SL, SL)
    column_o = pl.multiple_of(opp * SL, SL)
    quarter = pl.ds(pl.multiple_of(x * (CH // NX), CH // NX), CH // NX)
    loads = [
        pltpu.make_async_copy(st_hbm.at[:, pl.ds(column, SL)], st_v, load_sem.at[0]),
        pltpu.make_async_copy(up_hbm.at[:, pl.ds(column, SL)], up_v, load_sem.at[1]),
        pltpu.make_async_copy(st_hbm.at[:, pl.ds(column_o, SL)], st_o, load_sem.at[12]),
        pltpu.make_async_copy(up_hbm.at[:, pl.ds(column_o, SL)], up_o, load_sem.at[13]),
        pltpu.make_async_copy(routes_hbm, routes_v, load_sem.at[2]),
        pltpu.make_async_copy(weights_hbm, weights_v, load_sem.at[3]),
    ]
    late = [
        pltpu.make_async_copy(wg_hbm, wg, load_sem.at[4]),
        pltpu.make_async_copy(wu_hbm, wu, load_sem.at[5]),
    ]
    for j in range(N_TP):
        late.append(
            pltpu.make_async_copy(wd_hbm.at[:, pl.ds(j * SL, SL)], wd.at[j], load_sem.at[6])
        )
    tail_loads = [
        pltpu.make_async_copy(value_hbm, value_v, load_sem.at[7]),
        pltpu.make_async_copy(gate_hbm, gate_v, load_sem.at[8]),
        pltpu.make_async_copy(taps_hbm, taps_v, load_sem.at[9]),
        pltpu.make_async_copy(conv_hbm, conv_all.at[tp], load_sem.at[10]),
        pltpu.make_async_copy(
            proj_hbm.at[quarter, pl.ds(column, SL)], proj_all.at[tp, quarter], load_sem.at[11]
        ),
    ]
    barrier = pltpu.get_barrier_semaphore()
    peers = [(sp, (tp + r) % N_TP) for r in range(1, N_TP)]
    near = [p for p in range(N_SP) if p != OWN and OFFSETS[p][0] in (0, 1, NZ - 1)]
    for dev in [sp_dev(p, 1) for p in near] + peers:
        pl.semaphore_signal(barrier, inc=1, device_id=dev, device_id_type=MESH)
    for copy in loads:
        copy.start()
    for copy in late + tail_loads:
        copy.start()
    above, below = (((z + 1) % NZ) * NX + x, tp), (((z + NZ - 1) % NZ) * NX + x, tp)

    for copy in loads:
        copy.wait()
    packed = jnp.concatenate(
        [routes_v[...].astype(F32), weights_v[...], jnp.zeros((4, TOK), F32)], axis=0
    ).T
    r0, r1 = packed[:, 0:1].astype(jnp.int32), packed[:, 1:2].astype(jnp.int32)
    experts = lax.broadcasted_iota(jnp.int32, (TOK, N_SP), 1)
    c0 = jnp.where(r0 == experts, 1.0, 0.0).astype(F32)
    c1 = jnp.where(r1 == experts, 1.0, 0.0).astype(F32)
    tri = jnp.where(
        lax.broadcasted_iota(jnp.int32, (TOK, TOK), 1) < lax.broadcasted_iota(jnp.int32, (TOK, TOK), 0),
        1.0, 0.0,
    ).astype(BF16)
    expert = lax.broadcasted_iota(jnp.int32, (8, N_SP), 1)
    offset_of = (((expert >> 2) - z) & (NZ - 1)) * NX + (((expert & 3) - x) & (NX - 1))
    first_slot = jnp.zeros((8, N_SP), F32)
    for p, (dz, dx) in enumerate(OFFSETS):
        first_slot = first_slot + jnp.where(offset_of == dz * NX + dx, float(p * CAP), 0.0)
    slots = dot_nn(tri, (c0 + c1).astype(BF16)) + first_slot[0:1, :]
    pos0 = jnp.sum(slots * c0, axis=1, keepdims=True).astype(jnp.int32)
    pos1 = jnp.sum(slots * c1, axis=1, keepdims=True).astype(jnp.int32)
    stream = st_v[...]
    ups = up_v[...].astype(F32)
    cot0 = (packed[:, 2:3] * ups).astype(BF16)
    cot1 = (packed[:, 3:4] * ups).astype(BF16)
    stream_o = st_o[...]
    ups_o = up_o[...].astype(F32)
    cot0_o = (packed[:, 2:3] * ups_o).astype(BF16)
    cot1_o = (packed[:, 3:4] * ups_o).astype(BF16)

    def a2a(p):
        return pltpu.make_async_remote_copy(
            src_ref=send.at[p],
            dst_ref=xs.at[:, tp, pl.ds(p * CAP, CAP), :],
            send_sem=a_snd.at[0],
            recv_sem=a_rcv.at[chunk_of[p]],
            device_id=sp_dev(p, 1),
            device_id_type=MESH,
        )

    def a2a_o(p):
        return pltpu.make_async_remote_copy(
            src_ref=send_o.at[SECOND[p]],
            dst_ref=xs.at[:, opp, pl.ds(p * CAP, CAP), :],
            send_sem=a_snd.at[1],
            recv_sem=ao_rcv.at[chunk_of[p]],
            device_id=sp_dev(p, 1),
            device_id_type=MESH,
        )

    conv_plan = ((tp, up_dev), (tp, down_dev), (tp, (sp, opp)), (tp, mate), (bwd, mate), (fwd, mate), (opp, mate))
    conv_arrives = (bwd, fwd, opp, other, bwd_o, fwd_o, opp_o)

    def conv_copy(kind, arriving=False):
        at, dev = conv_plan[kind]
        if arriving:
            at = conv_arrives[kind]
        return pltpu.make_async_remote_copy(
            src_ref=conv_hbm if kind < 4 else conv_all.at[at], dst_ref=conv_all.at[at],
            send_sem=e_snd, recv_sem=e_rcv.at[kind], device_id=dev, device_id_type=MESH,
        )

    def proj_copy(r):
        at = pl.multiple_of(((tp + r) % N_TP) * SL, SL)
        return pltpu.make_async_remote_copy(
            src_ref=proj_hbm.at[quarter, pl.ds(at, SL)], dst_ref=proj_all.at[tp, quarter],
            send_sem=j_snd, recv_sem=j_rcv, device_id=peers[r - 1], device_id_type=MESH,
        )

    def quarter_copy(d):
        return pltpu.make_async_remote_copy(
            src_ref=proj_all.at[:, quarter, :], dst_ref=proj_all.at[:, quarter, :],
            send_sem=k_snd, recv_sem=k_rcv,
            device_id=(z * NX + (x + d) % NX, tp), device_id_type=MESH,
        )

    def stage_s(k):
        start, count = CHUNKS[k]
        width = count * CAP
        lanes = lax.broadcasted_iota(jnp.int32, (TOK, width), 1) + start * CAP
        s0 = jnp.where(pos0 == lanes, 1.0, 0.0).astype(BF16)
        s1 = jnp.where(pos1 == lanes, 1.0, 0.0).astype(BF16)
        both = s0 + s1
        onehot[:, start * CAP:start * CAP + width] = both
        rows = dot_tn(both, stream).astype(BF16)
        cots = (dot_tn(s0, cot0) + dot_tn(s1, cot1)).astype(BF16)
        send[start:start + count, 0] = rows.reshape(count, CAP, SL)
        send[start:start + count, 1] = cots.reshape(count, CAP, SL)
        if k in DIRECT:
            at = SECOND[start]
            rows = dot_tn(both, stream_o).astype(BF16)
            cots = (dot_tn(s0, cot0_o) + dot_tn(s1, cot1_o)).astype(BF16)
            send_o[at:at + count, 0] = rows.reshape(count, CAP, SL)
            send_o[at:at + count, 1] = cots.reshape(count, CAP, SL)

    def stage_go(k):
        start, count = CHUNKS[k]
        for p in range(start, start + count):
            if p == OWN:
                xs[:, tp, pl.ds(p * CAP, CAP), :] = send[p]
                xs[:, opp, pl.ds(p * CAP, CAP), :] = send_o[SECOND[p]]
            else:
                a2a(p).start()

    def stage_ox(k):
        start, count = CHUNKS[k]
        for p in range(max(start, 1), start + count):
            a2a_o(p).start()

    def farther(step):
        for dev in (above, below):
            pl.semaphore_signal(far_sem.at[step], inc=1, device_id=dev, device_id_type=MESH)

    def stage_f(step):
        pl.semaphore_wait(far_sem.at[step], 2)
        if step < 2:
            farther(step + 1)

    stage_s(0)
    stage_s(1)
    pl.semaphore_wait(barrier, len(near) + N_TP - 1)
    farther(0)
    stage_go(0)
    stage_ox(0)
    for kind in range(4):
        conv_copy(kind).start()
    for r in range(1, N_TP):
        proj_copy(r).start()
    stage_f(0)
    stage_go(1)
    stage_s(2)
    def gather(k, kind, rc, slice_at, dev):
        start, count = CHUNKS[k]
        ref = xs.at[rc, slice_at, pl.ds(start * CAP, count * CAP), :]
        return pltpu.make_async_remote_copy(
            src_ref=ref, dst_ref=ref, send_sem=g_snd.at[1 if k in DIRECT else 0], recv_sem=g_rcv.at[k, G_SLOT[kind]],
            device_id=dev, device_id_type=MESH,
        )

    plan = (
        (0, tp, up_dev), (0, tp, down_dev), (0, tp, mate),
        (1, tp, up_dev), (1, tp, down_dev), (1, tp, mate),
        (0, bwd, up_dev), (1, fwd, down_dev),
        (0, bwd, mate), (0, fwd, mate), (0, opp, mate),
        (1, fwd, mate), (1, bwd, mate), (1, opp, mate),
    )

    def spread(k, kind):
        rc, slice_at, dev = plan[kind]
        return gather(k, kind, rc, slice_at, dev)

    def both(k, slot):
        start, count = CHUNKS[k]
        whole(xs.at[:, tp, pl.ds(start * CAP, count * CAP), :], g_rcv.at[k, slot])

    def stage_a(k):
        start, count = CHUNKS[k]
        begin = max(start, 1)
        whole(xs.at[:, tp, pl.ds(begin * CAP, (start + count - begin) * CAP), :], a_rcv.at[k])
        for kind in (0, 4, 3, 1, 2, 5):
            spread(k, kind).start()

    def opposite(k):
        start, count = CHUNKS[k]
        begin = max(start, 1)
        whole(xs.at[:, opp, pl.ds(begin * CAP, (start + count - begin) * CAP), :], ao_rcv.at[k])
        spread(k, 10).start()
        spread(k, 13).start()

    def stage_b1(k):
        both(k, 0)
        for kind in (8, 11) if k in DIRECT else (6, 7, 8, 11):
            spread(k, kind).start()

    def stage_b2(k):
        both(k, 1)
        spread(k, 9).start()
        spread(k, 12).start()
        if k in DIRECT:
            opposite(k)
        else:
            both(k, 2)
            spread(k, 10).start()
            spread(k, 13).start()

    def stage_b3(k):
        start, count = CHUNKS[k]
        whole(xs.at[:, pl.ds(0, NY), pl.ds(start * CAP, count * CAP), :], g_rcv.at[k, 3])

    def swap(k):
        return pltpu.make_async_remote_copy(
            src_ref=part.at[k, 1 - c, :, pl.ds(0, CHUNKS[k][1] * CAP), :],
            dst_ref=part_in.at[k, :, pl.ds(0, CHUNKS[k][1] * CAP), :],
            send_sem=r_snd, recv_sem=r_rcv.at[k, 0], device_id=mate, device_id_type=MESH,
        )

    def stage_c(k):
        start, count = CHUNKS[k]
        size = count * CAP
        rows = pl.ds(start * CAP, size)
        gate_pre = jnp.zeros((size, SL), F32)
        up_pre = jnp.zeros((size, SL), F32)
        grad_act = jnp.zeros((size, SL), F32)
        for j in range(N_TP):
            r = xs[0, j, rows, :]
            gate_pre = gate_pre + dot_nn(r, wg[j])
            up_pre = up_pre + dot_nn(r, wu[j])
            grad_act = grad_act + dot_nt(xs[1, j, rows, :], wd[j])
        capped = jnp.minimum(gate_pre, clamp_limit)
        clipped = jnp.clip(up_pre, -clamp_limit, clamp_limit)
        sig = jax.nn.sigmoid(glu_alpha * capped)
        act[rows, :] = (capped * sig * (clipped + 1.0)).astype(BF16)
        slope = sig + glu_alpha * capped * sig * (1.0 - sig)
        g_gate = jnp.where(gate_pre < clamp_limit, grad_act * (clipped + 1.0) * slope, 0.0).astype(BF16)
        g_up = jnp.where(jnp.abs(up_pre) < clamp_limit, grad_act * capped * sig, 0.0).astype(BF16)
        ggp[rows, :] = g_gate
        gup[rows, :] = g_up
        for i in range(N_TP):
            core, at = (1 - c, i) if i < NY else (c, i - NY)
            total = dot_nt(g_gate, wg[2 * at + core]) + dot_nt(g_up, wu[2 * at + core])
            part[k, core, at, 0:size] = total.astype(BF16)
            if i == NY - 1:
                swap(k).start()

    def stage_w(start, stop):
        rows = pl.ds(start, stop - start)

        def grads(j, carry):
            r = xs[0, j, rows, :]
            at = pl.ds(pl.multiple_of(j * SL, SL), SL)
            g, u = dot_tn(r, ggp[rows, :]), dot_tn(r, gup[rows, :])
            d = dot_tn(act[rows, :], xs[1, j, rows, :])
            if start == 0:
                acc_g[j], acc_u[j], acc_d[:, at] = g, u, d
            else:
                acc_g[j] += g
                acc_u[j] += u
                acc_d[:, at] += d
            return carry

        lax.fori_loop(0, N_TP, grads, 0)

    def halves(k):
        half = CHUNKS[k][1] * CAP // 2
        return pl.ds(0, half), pl.ds(half, half)

    def ring(k, kind, src, slot, dev):
        return pltpu.make_async_remote_copy(
            src_ref=src, dst_ref=ring_in.at[k, slot, halves(k)[0], :],
            send_sem=r_snd, recv_sem=r_rcv.at[k, min(kind, 3)], device_id=dev, device_id_type=MESH,
        )

    def rings(k, kind):
        lo, hi = halves(k)
        if kind == 0:
            return swap(k)
        if kind == 1:
            return ring(k, 1, comb.at[k, 2, lo, :], 0, down_dev)
        if kind == 2:
            return ring(k, 2, comb.at[k, 2, hi, :], 1, up_dev)
        if kind == 3:
            return ring(k, 3, comb.at[k, 1, lo, :], 2, up_dev)
        if kind == 4:
            return ring(k, 4, comb.at[k, 3, hi, :], 3, down_dev)
        if kind == 5:
            return ring(k, 5, relay.at[k, 0, lo, :], 4, down_dev)
        return ring(k, 6, relay.at[k, 1, lo, :], 5, up_dev)

    def straight(k, r):
        size = CHUNKS[k][1] * CAP
        return pltpu.make_async_remote_copy(
            src_ref=comb.at[k, r, pl.ds(0, size), :], dst_ref=ring_in.at[k, r - 1, pl.ds(0, size), :],
            send_sem=r_snd, recv_sem=r_rcv.at[k, 3],
            device_id=(sp, ((y + r) % NY) * 2 + c), device_id_type=MESH,
        )

    def stage_last():
        k = NC - 1
        size = CHUNKS[k][1] * CAP
        swap(k).wait_recv()
        for r in (2, 1, 3, 0):
            at = (y + r) % NY
            pair = part[k, c, at, 0:size].astype(F32) + part_in[k, at, 0:size].astype(F32)
            comb[k, r, 0:size] = pair.astype(BF16)
            if r > 0:
                straight(k, r).start()

    def stage_end():
        k = NC - 1
        at, count = CHUNKS[k]
        size = count * CAP
        whole(ring_in.at[k, pl.ds(0, 3), pl.ds(0, size), :], r_rcv.at[k, 3])
        total = comb[k, 0, 0:size].astype(F32)
        for r in range(1, NY):
            total = total + ring_in[k, r - 1, 0:size].astype(F32)
        row_out[at:at + count] = total.astype(BF16).reshape(count, CAP, SL)
        for p in far_first(range(at, at + count)):
            back_copy(p).start()

    def stage_d(k):
        rings(k, 0).wait_recv()
        size = CHUNKS[k][1] * CAP
        for r in (2, 1, 3, 0):
            at = (y + r) % NY
            both = part[k, c, at, 0:size].astype(F32) + part_in[k, at, 0:size].astype(F32)
            comb[k, r, 0:size] = both.astype(BF16)
            if r == 2:
                rings(k, 1).start()
                rings(k, 2).start()
        rings(k, 3).start()
        rings(k, 4).start()

    def stage_e1(k):
        rings(k, 1).wait_recv()
        lo, hi = halves(k)
        relay[k, 0, lo, :] = (ring_in[k, 0, lo, :].astype(F32) + comb[k, 3, lo, :].astype(F32)).astype(BF16)
        rings(k, 5).start()
        rings(k, 2).wait_recv()
        relay[k, 1, lo, :] = (ring_in[k, 1, lo, :].astype(F32) + comb[k, 1, hi, :].astype(F32)).astype(BF16)
        rings(k, 6).start()

    def back_copy(p):
        return pltpu.make_async_remote_copy(
            src_ref=row_out.at[p], dst_ref=ret.at[p],
            send_sem=b_snd, recv_sem=b_rcv.at[chunk_of[p]], device_id=sp_dev(p, -1), device_id_type=MESH,
        )

    def stage_e2(k):
        lo, hi = halves(k)
        whole(ring_in.at[k, pl.ds(2, 4), lo, :], r_rcv.at[k, 3])
        low = comb[k, 0, lo, :].astype(F32) + ring_in[k, 2, lo, :].astype(F32) + ring_in[k, 4, lo, :].astype(F32)
        high = comb[k, 0, hi, :].astype(F32) + ring_in[k, 3, lo, :].astype(F32) + ring_in[k, 5, lo, :].astype(F32)
        at, count = CHUNKS[k]
        row_out[at:at + count // 2] = low.astype(BF16).reshape(count // 2, CAP, SL)
        row_out[at + count // 2:at + count] = high.astype(BF16).reshape(count // 2, CAP, SL)
        for p in far_first(range(at, at + count)):
            if p == OWN:
                ret[p] = row_out[p]
            else:
                back_copy(p).start()

    def stage_m():
        for copy in tail_loads:
            copy.wait()
        for kind in range(3):
            conv_copy(kind, True).wait_recv()
            conv_copy(kind + 4).start()
        whole(proj_all.at[pl.ds(0, N_TP - 1), pl.ds(0, CH // NX), :], j_rcv)
        for d in range(1, NX):
            quarter_copy(d).start()

    def stage_n():
        for kind in range(3, 7):
            conv_copy(kind, True).wait_recv()
        total, square = jnp.zeros((1, TOK), F32), jnp.zeros((1, TOK), F32)
        for k in range(N_TP):
            v = conv_all[k].astype(F32)
            total = total + jnp.sum(v, axis=0, keepdims=True)
            square = square + jnp.sum(v * v, axis=0, keepdims=True)
        mean = total / CW
        inv = lax.rsqrt(square / CW - mean * mean + norm_eps)
        stat[0:1, :] = mean
        stat[1:2, :] = inv
        for k in range(N_TP):
            n = (conv_all[k].astype(F32) - mean) * inv
            sig = jax.nn.sigmoid(n)
            slope = sig * (1.0 + n * (1.0 - sig))
            mix[k] = (n * sig).astype(BF16)
            hh[k] = slope
            hn[k] = slope * n

    stage_f(1)
    stage_a(0)
    stage_f(2)

    @pl.when(c == 0)
    def _():
        stage_go(2)

    stage_s(3)
    stage_s(4)
    stage_a(1)

    @pl.when(c == 0)
    def _():
        stage_go(3)
        stage_go(4)
        stage_ox(4)

    @pl.when(c == 1)
    def _():
        stage_go(2)

    stage_b1(0)
    stage_b2(0)
    late[0].wait()
    late[1].wait()
    whole(wd, load_sem.at[6])
    stage_b3(0)
    stage_c(0)
    stage_b1(1)
    stage_d(0)
    stage_a(2)

    @pl.when(c == 1)
    def _():
        stage_go(3)
        stage_go(4)
        stage_ox(4)

    stage_m()
    stage_b2(1)
    stage_b3(1)
    stage_c(1)
    stage_e1(0)
    stage_b1(2)
    stage_d(1)
    stage_a(3)
    stage_ox(3)
    stage_n()
    stage_w(0, 384)
    stage_b2(2)
    stage_b3(2)
    stage_c(2)
    stage_e1(1)
    stage_e2(0)
    stage_b1(3)
    stage_d(2)
    stage_a(4)
    stage_w(384, 640)
    stage_e2(1)
    stage_b2(3)
    stage_b3(3)
    stage_c(3)
    stage_b1(4)
    stage_e1(2)
    stage_d(3)
    stage_b2(4)
    stage_b3(4)
    stage_c(4)
    stage_e2(2)
    stage_e1(3)
    stage_last()
    stage_w(640, 896)
    stage_e2(3)
    stage_end()
    stage_w(896, 1024)
    outs = [
        pltpu.make_async_copy(acc_g, gg_out, out_sem.at[4]),
        pltpu.make_async_copy(acc_u, gu_out, out_sem.at[5]),
        pltpu.make_async_copy(acc_d, gd_out, out_sem.at[6]),
    ]
    for copy in outs:
        copy.start()
    total = up_v[...].astype(F32)
    for start, count in CHUNKS:
        begin = max(start, 1)
        whole(ret.at[pl.ds(begin, start + count - begin)], b_rcv.at[chunk_of[start]])
        picked = onehot[:, start * CAP:(start + count) * CAP]
        total = total + dot_nn(picked, ret[start:start + count].reshape(count * CAP, SL))
    grads = total.astype(BF16)
    gs_ref[...] = grads

    outer = dot_nn(mix[...].reshape(CW, TOK), grads).reshape(N_TP, 2, CH // 2, SL)
    low_half = lax.broadcasted_iota(jnp.int32, (CW // 2, 128), 1) < CH
    for g in range(2):
        upper = outer[:, 0, :, 128 * g:128 * g + 128].reshape(CW // 2, 128)
        lower = outer[:, 1, :, 128 * g:128 * g + 128].reshape(CW // 2, 128)
        even = jnp.where(low_half, upper, pltpu.roll(lower, CH, 1))
        odd = jnp.where(low_half, pltpu.roll(upper, CH, 1), lower)
        gt[:, 2 * g] = even.astype(BF16).reshape(N_TP, CH // 2, 128)
        gt[:, 2 * g + 1] = odd.astype(BF16).reshape(N_TP, CH // 2, 128)
    def block_at(height):
        ahead = (height - tp + NZ) % NZ
        return 2 * ((y + ahead // 2 + 2) % NY) + ahead % 2

    def gt_copy(p):
        dev = sp_dev(p, 1)
        return pltpu.make_async_remote_copy(
            src_ref=gt.at[block_at(dev[0] // NX), dev[0] % NX], dst_ref=gt_in.at[p], send_sem=o_snd, recv_sem=o_rcv,
            device_id=dev, device_id_type=MESH,
        )

    for p in far_first(range(N_SP)):
        if p != OWN:
            gt_copy(p).start()

    whole(proj_all.at[:, pl.ds(0, 3 * CH // NX), :], k_rcv)
    prod = dot_nt(proj_all[...].reshape(CW, SL), grads)
    sums[0:1, :] = jnp.sum(prod * hh[...].reshape(CW, TOK), axis=0, keepdims=True)
    sums[1:2, :] = jnp.sum(prod * hn[...].reshape(CW, TOK), axis=0, keepdims=True)
    for k in range(N_TP):
        pm[k % 2, k // 2] = prod[k * CH:(k + 1) * CH].astype(BF16)

    def pm_copy(r):
        if r == 0:
            src, dst, dev = pm.at[1 - c], pm_in, mate
        else:
            src, dst, dev = pm_out.at[r - 1], pm_got.at[r - 1], (sp, ((y + r) % NY) * 2 + c)
        return pltpu.make_async_remote_copy(
            src_ref=src, dst_ref=dst, send_sem=p_snd, recv_sem=p_rcv.at[r],
            device_id=dev, device_id_type=MESH,
        )

    def sum_copy(r):
        return pltpu.make_async_remote_copy(
            src_ref=sums, dst_ref=sums_in.at[r - 1], send_sem=s_snd, recv_sem=s_rcv,
            device_id=peers[r - 1], device_id_type=MESH,
        )

    pm_copy(0).start()
    for r in range(1, N_TP):
        sum_copy(r).start()

    pm_copy(0).wait_recv()
    for r in (2, 1, 3):
        at = (y + r) % NY
        pm_out[r - 1] = (pm[c, at].astype(F32) + pm_in[at].astype(F32)).astype(BF16)
        pm_copy(r).start()
    mixed_grad = pm[c, y].astype(F32) + pm_in[y].astype(F32)
    first, second = sums[0:1, :], sums[1:2, :]
    whole(sums_in, s_rcv)
    for r in range(1, N_TP):
        first = first + sums_in[r - 1, 0:1, :]
        second = second + sums_in[r - 1, 1:2, :]
    for r in (1, 3, 2):
        pm_copy(r).wait_recv()
        mixed_grad = mixed_grad + pm_got[r - 1].astype(F32)
    mean, inv = stat[0:1, :], stat[1:2, :]
    normed = (conv_all[tp].astype(F32) - mean) * inv
    grad_normed = mixed_grad * hh[tp]
    conv_grad[:, 0:TOK] = inv * (grad_normed - first / CW - normed * (second / CW))
    halo = pltpu.make_async_remote_copy(
        src_ref=conv_grad.at[:, pl.ds(0, 128)], dst_ref=conv_grad.at[:, pl.ds(TOK, 128)],
        send_sem=h_snd, recv_sem=h_rcv, device_id=((sp + N_SP - 1) % N_SP, tp), device_id_type=MESH,
    )
    halo.start()

    whole(gt_in.at[pl.ds(1, N_SP - 1)], o_rcv)
    owned = gt[block_at(z), x].astype(F32)
    for p in range(N_SP):
        if p != OWN:
            owned = owned + gt_in[p].astype(F32)
    gt_out[...] = owned
    owner_copy = pltpu.make_async_remote_copy(
        src_ref=gt_out, dst_ref=gt_got, send_sem=f_snd, recv_sem=f_rcv,
        device_id=(tp * NX + x, block_at(z)), device_id_type=MESH,
    )
    owner_copy.start()

    halo.wait_recv()
    tail = conv_grad[:, TOK:TOK + 128]
    wide = jnp.concatenate([conv_grad[:, 0:TOK], jnp.where(sp == N_SP - 1, 0.0, tail)], axis=1)
    taps_t = jnp.concatenate([taps_v[...], jnp.zeros((1, CH), F32)], axis=0).T
    glu = taps_t[:, 0:1] * wide[:, 0:TOK]
    for offset in range(1, KW):
        glu = glu + taps_t[:, offset:offset + 1] * pltpu.roll(wide, TOK + 128 - offset, 1)[:, 0:TOK]
    gate_sig = jax.nn.sigmoid(gate_v[...].astype(F32))
    gv_ref[...] = (glu * gate_sig).astype(BF16)
    gq_ref[...] = (glu * value_v[...].astype(F32) * gate_sig * (1.0 - gate_sig)).astype(BF16)

    owner_copy.wait_recv()
    owner_copy.wait_send()
    got_t = gt_got[...].T
    go_ref[:, 0:CH // 2] = got_t[0:CH]
    go_ref[:, CH // 2:CH] = got_t[CH:2 * CH]
    outs.extend([
        pltpu.make_async_copy(gs_ref, gs_out, out_sem.at[0]),
        pltpu.make_async_copy(gv_ref, gv_out, out_sem.at[1]),
        pltpu.make_async_copy(gq_ref, gq_out, out_sem.at[2]),
        pltpu.make_async_copy(go_ref, go_out, out_sem.at[3]),
    ])
    for copy in outs[3:]:
        copy.start()
    whole(send.at[pl.ds(1, N_SP - 1)], a_snd.at[0])
    whole(send_o.at[pl.ds(1, len(SECOND) - 1)], a_snd.at[1])
    whole(row_out.at[pl.ds(1, N_SP - 1)], b_snd)
    whole(gt_in.at[pl.ds(1, N_SP - 1)], o_snd)

    whole(xs.at[:, pl.ds(0, 7), pl.ds(0, 512), :], g_snd.at[0])
    whole(xs.at[:, pl.ds(0, 6), pl.ds(0, 512), :], g_snd.at[1])
    whole(xs.at[0, pl.ds(0, 7)], r_snd)
    whole(conv_all.at[pl.ds(0, 7)], p_snd)
    whole(sums_in, s_snd)
    whole(proj_all.at[pl.ds(0, N_TP - 1), pl.ds(0, CH // NX), :], j_snd)
    whole(proj_all.at[:, pl.ds(0, 3 * CH // NX), :], k_snd)
    whole(conv_all.at[pl.ds(0, 7)], e_snd)
    for copy in outs:
        copy.wait()
    halo.wait_send()


RESULTS = (
    ((TOK, SL), BF16),
    ((CH, TOK), BF16),
    ((CH, TOK), BF16),
    ((CH, CH), F32),
    ((N_TP, SL, SL), F32),
    ((N_TP, SL, SL), F32),
    ((SL, N_TP * SL), F32),
)


def store_kernel(*refs):
    n = len(RESULTS)
    sems = refs[-1]
    copies = [pltpu.make_async_copy(refs[i], refs[n + i], sems.at[i]) for i in range(n)]
    for copy in copies:
        copy.start()
    for copy in copies:
        copy.wait()


def store_call(*results):
    return pl.pallas_call(
        store_kernel,
        out_shape=tuple(jax.ShapeDtypeStruct(shape, dtype) for shape, dtype in RESULTS),
        in_specs=[pl.BlockSpec(memory_space=pltpu.VMEM)] * len(RESULTS),
        out_specs=(pl.BlockSpec(memory_space=pl.ANY),) * len(RESULTS),
        scratch_shapes=[pltpu.SemaphoreType.DMA((len(RESULTS),))],
        compiler_params=pltpu.CompilerParams(vmem_limit_bytes=2 * 1024 * 1024),
        name="store_results",
    )(*(pltpu.with_memory_space_constraint(r, pltpu.VMEM) for r in results))


def main_call(*operands):
    any_spec = pl.BlockSpec(memory_space=pltpu.HBM)
    flops = 2 * N_SP * CAP * 2048 * 256 * 8
    V = pltpu.VMEM
    D = pltpu.SemaphoreType.DMA
    return pl.pallas_call(
        main_kernel,
        out_shape=tuple(V(shape, dtype) for shape, dtype in RESULTS),
        in_specs=[any_spec] * 12,
        out_specs=(pl.BlockSpec(memory_space=pl.ANY),) * 7,
        scratch_shapes=[V(shape, dtype) for shape, dtype in RESULTS] + [
            V((TOK, SL), BF16),
            V((TOK, SL), BF16),
            V((TOK, SL), BF16),
            V((TOK, SL), BF16),
            V((2, TOK), jnp.int32),
            V((2, TOK), F32),
            V((N_TP, SL, SL), BF16),
            V((N_TP, SL, SL), BF16),
            V((N_TP, SL, SL), BF16),
            V((N_SP, 2, CAP, SL), BF16),
            V((len(SECOND), 2, CAP, SL), BF16),
            V((2, N_TP, N_SP * CAP, SL), BF16),
            V((TOK, N_SP * CAP), BF16),
            V((NC, 2, NY, MAX, SL), BF16),
            V((NC, NY, MAX, SL), BF16),
            V((NC, NY, MAX, SL), BF16),
            V((NC, 6, MAX // 2, SL), BF16),
            V((NC, 2, MAX // 2, SL), BF16),
            V((N_SP, CAP, SL), BF16),
            V((N_SP, CAP, SL), BF16),
            V((N_SP * CAP, SL), BF16),
            V((N_SP * CAP, SL), BF16),
            V((N_SP * CAP, SL), BF16),
            V((CH, TOK), BF16),
            V((CH, TOK), BF16),
            V((KW, CH), F32),
            V((N_TP, CH, TOK), BF16),
            V((N_TP, CH, SL), BF16),
            V((N_TP, CH, TOK), F32),
            V((N_TP, CH, TOK), F32),
            V((N_TP, CH, TOK), BF16),
            V((8, TOK), F32),
            V((2, NY, CH, TOK), BF16),
            V((NY, CH, TOK), BF16),
            V((NY - 1, CH, TOK), BF16),
            V((NY - 1, CH, TOK), BF16),
            V((8, TOK), F32),
            V((N_TP - 1, 8, TOK), F32),
            V((CH, TOK + 128), F32),
            V((N_TP, NX, CH // 2, 128), BF16),
            V((N_SP, CH // 2, 128), BF16),
            V((CH // 2, 128), F32),
            V((CH // 2, 128), F32),
            pltpu.SemaphoreType.REGULAR((3,)),
            D((14,)),
            D((7,)),
            D((2,)),
            D((NC,)),
            D((NC,)),
            D((2,)),
            D((NC, 4)),
            D,
            D((NC, 4)),
            D,
            D((NC,)),
            D,
            D((7,)),
            D,
            D,
            D,
            D,
            D,
            D((NY,)),
            D,
            D,
            D,
            D,
            D,
            D,
            D,
            D,
        ],
        compiler_params=pltpu.CompilerParams(
            collective_id=0, has_side_effects=True, vmem_limit_bytes=54 * 1024 * 1024
        ),
        cost_estimate=pl.CostEstimate(flops=flops, bytes_accessed=16 << 20, transcendentals=0),
        name="routed_experts",
    )(*operands)


def on_device(
    upstream,
    stream,
    routes,
    route_weights,
    glu_value,
    glu_gate,
    conv_taps,
    conv_saved,
    out_proj,
    expert_gate,
    expert_up,
    expert_down,
):
    grad_stream, grad_value, grad_gate, grad_out_proj, grad_gate_w, grad_up_w, grad_down_w = store_call(*main_call(
        upstream, stream, routes.T, route_weights.T,
        expert_gate.reshape(N_TP, SL, SL), expert_up.reshape(N_TP, SL, SL), expert_down[0],
        glu_value.T, glu_gate.T, conv_taps, conv_saved.T, out_proj.T,
    ))
    return (
        grad_stream,
        grad_value.T,
        grad_gate.T,
        grad_out_proj,
        grad_gate_w.reshape(1, N_TP * SL, SL),
        grad_up_w.reshape(1, N_TP * SL, SL),
        grad_down_w[None],
    )


def solution(mesh):
    in_specs = (
        P("sp", None),
        P("sp", None),
        P("sp", None),
        P("sp", None),
        P("sp", "tp"),
        P("sp", "tp"),
        P(None, "tp"),
        P("sp", "tp"),
        P(None, "tp"),
        P("sp", None, "tp"),
        P("sp", None, "tp"),
        P("sp", "tp", None),
    )
    out_specs = (
        P("sp", "tp"),
        P("sp", "tp"),
        P("sp", "tp"),
        P("sp", "tp"),
        P("sp", None, "tp"),
        P("sp", None, "tp"),
        P("sp", "tp", None),
    )
    return jax.shard_map(
        on_device, mesh=mesh, in_specs=in_specs, out_specs=out_specs, check_vma=False
    )
```
